512 devices in a mesh: sp: 64 (over z, y), tp: 8 (over x, core).
Axes of the slice: x: 4, y: 4, z: 16, core: 2. Of those that a mesh axis runs over, the one named last changes fastest.
Arguments:
- tokens: bfloat16 [16384, 2048], P('sp', 'tp'), may hold values from -6 to 6
- norm_gain: float32 [2048], replicated, may hold values from 0.1 to 1.9
- recv_weight: bfloat16 [2048, 1024], P(None, 'tp'), may hold values from -0.125 to 0.125
- lin_key_weight: bfloat16 [2048, 1024], P(None, 'tp'), may hold values from -0.125 to 0.125
- lin_value_weight: bfloat16 [2048, 1024], P(None, 'tp'), may hold values from -0.125 to 0.125
- decay_down: bfloat16 [2048, 64], replicated, may hold values from -0.125 to 0.125
- decay_up: bfloat16 [64, 1024], P(None, 'tp'), may hold values from -0.75 to 0.75
- decay_log_bias: float32 [1024], P('tp'), may hold values from -13 to -3
- decay_shift: float32 [16384, 1024], P('sp', 'tp'), may hold values from -1 to 13
- learn_rate: float32 [1024], P('tp'), may hold values from 0 to 1
- group_gain: float32 [1024], P('tp'), may hold values from 0.1 to 1.9
- initial_state: float32 [16, 64, 64], P('tp'), may hold values from -768 to 768
- query_weight: bfloat16 [2048, 1024], P(None, 'tp'), may hold values from -8 to 8
- att_key_weight: bfloat16 [2048, 1024], P(None, 'tp'), may hold values from -1 to 1
- att_value_weight: bfloat16 [2048, 1024], P(None, 'tp'), may hold values from -0.125 to 0.125
- gate_cache: float32 [16384, 8], P('sp', 'tp'), may hold values from -16384 to 0, as said below
- att_gain: float32 [1024], P('tp'), may hold values from 0.1 to 1.9
- out_lin_weight: bfloat16 [1024, 2048], P('tp'), may hold values from -0.125 to 0.125
- out_att_weight: bfloat16 [1024, 2048], P('tp'), may hold values from -0.125 to 0.125
Outputs:
- mixed_out: bfloat16 [16384, 2048], P('sp', 'tp')
The draws below stay inside these ranges and needn't reach their ends.
Inputs may be any that keep to these rules, and one draw needn't show every extreme that they name: `gate_cache`: never rises along the sequence.
All inputs are finite; a program needn't handle non-finite values.
Results may differ from the reference program's by a relative error of at most 0.025.
Values may be sent and summed in bfloat16 or wider, within the bound.
No kernel may reach another device: no remote copies, remote signals or barrier semaphores. Data moves between devices by JAX's collectives and lax.ppermute only.
A program may use at most 64 MiB of HBM per device.

```python
import math
import jax
import jax.numpy as jnp
from jax import lax

D = 2048
HEAD_LIN = 64
HEAD_ATT = 128
RANK = 64
TOK_DEV = 256
SEQUENCE_LENGTH = 16384
LIN_W = 1024
ATT_W = 1024
LIN_HEADS = 16
ATT_HEADS = 8
N_SP = 64
N_TP = 8


def lin_plan(key):
    order = jax.random.permutation(jax.random.fold_in(key, 21), LIN_HEADS)
    cut = LIN_HEADS // 2
    return jnp.repeat(order >= cut, HEAD_LIN)


def draw_decay_log_bias(key, part):
    slow_rows = lin_plan(key)
    slow_log = jax.random.uniform(jax.random.fold_in(key, 22), (LIN_W,), jnp.float32, jnp.log(0.1), jnp.log(0.4)) - jnp.log(float(SEQUENCE_LENGTH))
    fast_log = jax.random.uniform(jax.random.fold_in(key, 23), (LIN_W,), jnp.float32, jnp.log(0.01), jnp.log(1.0 / 30.0))
    return jnp.where(slow_rows, slow_log, fast_log)


def draw_learn_rate(key, part):
    slow_rows = lin_plan(key)
    slow_rate = jnp.exp(jax.random.uniform(jax.random.fold_in(key, 24), (LIN_W,), jnp.float32, jnp.log(0.3), 0.0)) * HEAD_LIN / SEQUENCE_LENGTH
    slow_rate = jnp.minimum(slow_rate, 0.5)
    fast_rate = jax.random.uniform(jax.random.fold_in(key, 25), (LIN_W,), jnp.float32, 0.2, 0.8)
    return jnp.where(slow_rows, slow_rate, fast_rate)


def draw_decay_shift(key, part):
    blocks = SEQUENCE_LENGTH // TOK_DEV
    shift_amounts = jax.random.uniform(jax.random.fold_in(key, 31), (blocks, 1), jnp.float32, -0.7, 0.7)
    shift_amounts = jnp.repeat(shift_amounts, TOK_DEV, axis=0)
    spike_events = jax.random.randint(jax.random.fold_in(key, 32), (4,), 0, SEQUENCE_LENGTH)
    spike_rows = jnp.any(jnp.arange(SEQUENCE_LENGTH)[:, None] == spike_events[None, :], axis=1).astype(jnp.float32)[:, None]
    random_noise = jax.random.uniform(jax.random.fold_in(key, 33), (SEQUENCE_LENGTH, LIN_W), jnp.float32, -0.3, 0.3)
    return shift_amounts + random_noise + spike_rows * (jnp.log(float(SEQUENCE_LENGTH)) + 0.6)


def draw_gate_cache(key, part):
    order = jax.random.permutation(jax.random.fold_in(key, 41), ATT_HEADS)
    cut = ATT_HEADS // 2
    slow_heads = order >= cut
    fast_rate = jnp.exp(jax.random.uniform(jax.random.fold_in(key, 42), (ATT_HEADS,), jnp.float32, jnp.log(1.0 / 80.0), jnp.log(1.0 / 30.0)))
    rates = jnp.where(slow_heads, 1.0 / SEQUENCE_LENGTH, fast_rate)
    blocks = SEQUENCE_LENGTH // TOK_DEV
    factors = jnp.exp(jax.random.uniform(jax.random.fold_in(key, 43), (blocks, ATT_HEADS), jnp.float32, -0.7, 0.7))
    factors = jnp.repeat(factors, TOK_DEV, axis=0)
    random_noise = jax.random.uniform(jax.random.fold_in(key, 44), (SEQUENCE_LENGTH, ATT_HEADS), jnp.float32, 0.5, 1.5)
    return jnp.cumsum(-random_noise * factors * rates[None, :], axis=0)


def att_pair(key):
    key_part = jax.random.normal(jax.random.fold_in(key, 51), (D, ATT_W), jnp.float32) * D ** (-0.5)
    query_part = jax.random.normal(jax.random.fold_in(key, 52), (D, ATT_W), jnp.float32) * D ** (-0.5)
    return (query_part, jnp.clip(key_part, -1.0, 1.0))


def draw_query_weight(key, part):
    return jnp.clip(att_pair(key)[0], -8.0, 8.0).astype(jnp.bfloat16)


def draw_att_key_weight(key, part):
    return att_pair(key)[1].astype(jnp.bfloat16)


def steps_of(rng, shape, pieces, low, largest):
    level = 1.0
    for axis_at, shards_of in pieces:
        heights = jax.random.uniform(jax.random.fold_in(jax.random.fold_in(rng, 6), axis_at), (shards_of,), jnp.float32, low / len(pieces), largest / len(pieces))
        level = level * jnp.repeat(jnp.exp(heights), shape[axis_at] // shards_of).reshape((-1,) + (1,) * (len(shape) - 1 - axis_at))
    return level


def normal_values(rng, dims, spread, reach, cuts=(), kind=jnp.bfloat16):
    values = spread * jax.random.normal(rng, dims, jnp.float32)
    if cuts:
        values = values * steps_of(rng, dims, cuts, -0.22, 0.18)
    return jnp.clip(values, -reach, reach).astype(kind)


def setup_inputs(seed: int = 0) -> dict:
    splits = jax.random.split(jax.random.key(seed), 20)
    return {
        "tokens": normal_values(splits[0], (SEQUENCE_LENGTH, D), 1.0, 6.0, ((0, 64), (1, 8))),
        "norm_gain": jnp.clip(1.0 + 0.18 * jax.random.normal(splits[1], (D,), jnp.float32), 0.1, 1.9),
        "recv_weight": normal_values(splits[2], (D, LIN_W), D ** -0.5, 0.125, ((1, 8),)),
        "lin_key_weight": normal_values(splits[3], (D, LIN_W), D ** -0.5, 0.125, ((1, 8),)),
        "lin_value_weight": normal_values(splits[4], (D, LIN_W), D ** -0.5, 0.125, ((1, 8),)),
        "decay_down": normal_values(splits[5], (D, RANK), D ** -0.5, 0.125),
        "decay_up": normal_values(splits[6], (RANK, LIN_W), RANK ** -0.5, 0.75, ((1, 8),)),
        "decay_log_bias": draw_decay_log_bias(jax.random.fold_in(splits[19], 71), 0),
        "decay_shift": draw_decay_shift(jax.random.fold_in(splits[19], 71), 0),
        "learn_rate": draw_learn_rate(jax.random.fold_in(splits[19], 71), 0),
        "group_gain": jnp.clip(1.0 + 0.18 * jax.random.normal(splits[10], (LIN_W,), jnp.float32), 0.1, 1.9),
        "initial_state": normal_values(splits[11], (LIN_HEADS, HEAD_LIN, HEAD_LIN), ((TOK_DEV * N_SP) ** 0.5), 768.0, ((0, 8),), jnp.float32),
        "query_weight": draw_query_weight(jax.random.fold_in(splits[19], 71), 0),
        "att_key_weight": draw_att_key_weight(jax.random.fold_in(splits[19], 71), 0),
        "att_value_weight": normal_values(splits[14], (D, ATT_W), D ** -0.5, 0.125, ((1, 8),)),
        "gate_cache": draw_gate_cache(jax.random.fold_in(splits[19], 71), 0),
        "att_gain": jnp.clip(1.0 + 0.18 * jax.random.normal(splits[16], (ATT_W,), jnp.float32), 0.1, 1.9),
        "out_lin_weight": normal_values(splits[17], (LIN_W, D), D ** -0.5, 0.125, ((0, 8),)),
        "out_att_weight": normal_values(splits[18], (ATT_W, D), D ** -0.5, 0.125, ((0, 8),)),
    }


highest = lax.Precision.HIGHEST

def lin_advance(memory, inputs):
    decays, unit_key, rate_vec, key_now, value_now, recv_now = inputs
    along = jnp.einsum('hij,hj->hi', memory, unit_key, precision=highest)
    memory = memory * decays[:, None, :] - along[:, :, None] * rate_vec[:, None, :] + value_now[:, :, None] * key_now[:, None, :]
    return (memory, jnp.einsum('hij,hj->hi', memory, recv_now, precision=highest))

def reference(tokens, norm_gain, recv_weight, lin_key_weight, lin_value_weight, decay_down, decay_up, decay_log_bias, decay_shift, learn_rate, group_gain, initial_state, query_weight, att_key_weight, att_value_weight, gate_cache, att_gain, out_lin_weight, out_att_weight):
    wide = tokens.astype(jnp.float32)
    inverse = lax.rsqrt(lax.optimization_barrier(jnp.mean(wide * wide, axis=1, keepdims=True)) + 1e-06)
    scaled = (wide * norm_gain).astype(jnp.bfloat16)

    def project(weight):
        return (jnp.dot(scaled, weight, preferred_element_type=jnp.float32) * inverse).astype(jnp.bfloat16)
    recv = project(recv_weight)
    lin_key = project(lin_key_weight)
    lin_value = project(lin_value_weight)
    queries = project(query_weight)
    att_key = project(att_key_weight)
    att_value = project(att_value_weight)
    low_rank = project(decay_down)
    exponent = decay_log_bias + decay_shift + jnp.dot(jnp.tanh(low_rank.astype(jnp.float32)).astype(jnp.bfloat16), decay_up, preferred_element_type=jnp.float32)
    decays = jnp.exp(-jnp.exp(exponent))

    def heads_of(values):
        return values.astype(jnp.float32).reshape(SEQUENCE_LENGTH, LIN_HEADS, HEAD_LIN)
    key_heads = heads_of(lin_key)
    unit_key = key_heads * lax.rsqrt(lax.optimization_barrier(jnp.sum(key_heads * key_heads, axis=-1, keepdims=True)) + 1e-06)
    rate_vec = unit_key * learn_rate.reshape(LIN_HEADS, HEAD_LIN)
    inputs = (heads_of(decays), unit_key, rate_vec, key_heads, heads_of(lin_value), heads_of(recv))
    _, lin_raw = lax.scan(lin_advance, initial_state.astype(jnp.float32), inputs)
    mean_val = lax.optimization_barrier(jnp.mean(lin_raw, axis=-1, keepdims=True))
    spread_val = lax.optimization_barrier(jnp.mean(jnp.square(lin_raw - mean_val), axis=-1, keepdims=True))
    lin_norm = (lin_raw - mean_val) * lax.rsqrt(spread_val + 0.00064) * group_gain.reshape(LIN_HEADS, HEAD_LIN)
    lin_mixed = lin_norm.reshape(SEQUENCE_LENGTH, LIN_W).astype(jnp.bfloat16)
    query_heads = queries.astype(jnp.float32).reshape(SEQUENCE_LENGTH, ATT_HEADS, HEAD_ATT)
    key_all = att_key.astype(jnp.float32).reshape(SEQUENCE_LENGTH, ATT_HEADS, HEAD_ATT)
    value_all = att_value.astype(jnp.float32).reshape(SEQUENCE_LENGTH, ATT_HEADS, HEAD_ATT)
    query_block = math.gcd(SEQUENCE_LENGTH, 512)
    key_pos = jnp.arange(SEQUENCE_LENGTH, dtype=jnp.int32)
    gate_rows = gate_cache.T

    def attend_block(block_index):
        first = (block_index * query_block).astype(jnp.int32)
        query_part = lax.dynamic_slice_in_dim(query_heads, first, query_block, 0)
        query_gate = lax.dynamic_slice_in_dim(gate_cache, first, query_block, 0)
        query_pos = first + jnp.arange(query_block, dtype=jnp.int32)
        logits = jnp.einsum('qhd,khd->hqk', query_part, key_all) * HEAD_ATT ** (-0.5)
        logits = logits + query_gate.T[:, :, None] - gate_rows[:, None, :]
        allowed = key_pos[None, :] <= query_pos[:, None]
        logits = jnp.where(allowed[None], logits, -1e+30)
        best_score = lax.optimization_barrier(jnp.max(logits, axis=-1, keepdims=True))
        raw_weights = jnp.where(allowed[None], jnp.exp(logits - best_score), 0.0)
        row_sum_total = lax.optimization_barrier(jnp.sum(raw_weights, axis=-1))
        weights = raw_weights.astype(jnp.bfloat16).astype(jnp.float32)
        summed = jnp.einsum('hqk,khd->hqd', weights, value_all)
        return jnp.swapaxes(summed / row_sum_total[..., None], 0, 1)
    att_raw = lax.map(attend_block, jnp.arange(SEQUENCE_LENGTH // query_block, dtype=jnp.int32)).reshape(SEQUENCE_LENGTH, ATT_HEADS, HEAD_ATT)
    att_norm = att_raw * lax.rsqrt(lax.optimization_barrier(jnp.mean(att_raw * att_raw, axis=-1, keepdims=True)) + 1e-06) * att_gain.reshape(ATT_HEADS, HEAD_ATT)
    att_mixed = att_norm.reshape(SEQUENCE_LENGTH, ATT_W).astype(jnp.bfloat16)
    lin_group = LIN_W // N_TP
    att_group = ATT_W // N_TP
    totals = jnp.zeros((SEQUENCE_LENGTH, D), jnp.float32)
    for group in range(N_TP):
        lin_cols = slice(group * lin_group, (group + 1) * lin_group)
        att_cols = slice(group * att_group, (group + 1) * att_group)
        partial_value = jnp.dot(lin_mixed[:, lin_cols], out_lin_weight[lin_cols], preferred_element_type=jnp.float32)
        partial_value = partial_value + jnp.dot(att_mixed[:, att_cols], out_att_weight[att_cols], preferred_element_type=jnp.float32)
        rounded = lax.optimization_barrier(partial_value.astype(jnp.bfloat16))
        totals = totals + rounded.astype(jnp.float32)
    return totals.astype(jnp.bfloat16)
```

```python
import functools
import math

import jax
import jax.numpy as jnp
from jax import lax
from jax.experimental import pallas as pl
from jax.experimental.pallas import tpu as pltpu
from jax.sharding import Mesh
from jax.sharding import PartitionSpec as P

HEAD_LIN = 64
HEAD_ATT = 128
WIDE = 128
SP = ("z", "y")
TP = ("x", "c")
LOG2E = math.log2(math.e)
NEG = -1e30
F32 = jnp.float32
BF16 = jnp.bfloat16


def params():
    return pltpu.CompilerParams(vmem_limit_bytes=48 * 1024 * 1024)


def cost(flops, size):
    return pl.CostEstimate(flops=flops, bytes_accessed=size, transcendentals=0)


def dot(a, b, dims=((1,), (0,))):
    return lax.dot_general(a, b, (dims, ((), ())), preferred_element_type=F32)


def parts_of(a):
    high = a.astype(BF16)
    return high, (a - high.astype(F32)).astype(BF16)


def dot3(a, b, dims=((1,), (0,))):
    ah, al = parts_of(a)
    bh, bl = parts_of(b)
    return dot(ah, bh, dims) + (dot(ah, bl, dims) + dot(al, bh, dims))


def dot2(a, b, dims=((1,), (0,))):
    ah, al = parts_of(a)
    return dot(ah, b, dims) + dot(al, b, dims)


def iota(shape, dim):
    return lax.broadcasted_iota(jnp.int32, shape, dim)


def by_head(a):
    left = iota(a.shape, 1) < HEAD_LIN
    first = jnp.sum(jnp.where(left, a, 0.0), axis=1, keepdims=True)
    second = jnp.sum(jnp.where(left, 0.0, a), axis=1, keepdims=True)
    return jnp.where(left, first, second)


def scaled_pieces(pieces_ref, gain_ref):
    shards, rows, depth = pieces_ref.shape
    scaled, squares = [], jnp.zeros((rows, depth), F32)
    for j in range(shards):
        wide = pieces_ref[j].astype(F32)
        scaled.append((wide * gain_ref[:, j * depth : (j + 1) * depth]).astype(BF16))
        squares = squares + wide * wide
    mean = jnp.sum(squares, axis=1, keepdims=True) / (shards * depth)
    return scaled, lax.rsqrt(mean + 1e-6)


def projected(scaled, inverse, w_ref):
    depth = scaled[0].shape[1]
    total = dot(scaled[0], w_ref[0:depth])
    for j in range(1, len(scaled)):
        total = total + dot(scaled[j], w_ref[j * depth : (j + 1) * depth])
    return (total * inverse).astype(BF16)


def kv_kernel(pieces_ref, gain_ref, wk_ref, wv_ref, out_ref):
    scaled, inverse = scaled_pieces(pieces_ref, gain_ref)
    out_ref[:, :HEAD_ATT] = projected(scaled, inverse, wk_ref)
    out_ref[:, HEAD_ATT:] = projected(scaled, inverse, wv_ref)


def spans(log_decay):
    rows = log_decay.shape[0]
    row = iota(log_decay.shape, 0)
    zero = jnp.zeros_like(log_decay)
    before = [None] + [pltpu.roll(log_decay, i, 0) for i in range(1, 8)]
    behind = [None] + [pltpu.roll(log_decay, rows - i, 0) for i in range(1, 8)]
    ahead, after = {1: zero}, {1: zero}
    for h in (2, 4, 8):
        place = row & (h - 1)
        a, b = zero, zero
        for i in range(1, h):
            a = a + jnp.where(place >= i, before[i], 0.0)
            b = b + jnp.where(place + i < h, behind[i], 0.0)
        ahead[h], after[h] = a, b
    h = 8
    while h < rows:
        shape = (rows // (2 * h), 2 * h, WIDE)
        a, b = ahead[h].reshape(shape), after[h].reshape(shape)
        step = log_decay.reshape(shape)
        left = a[:, h - 1 : h] + step[:, h - 1 : h]
        right = b[:, h : h + 1] + step[:, h : h + 1]
        a = jnp.concatenate([a[:, :h], a[:, h:] + left], axis=1)
        b = jnp.concatenate([b[:, :h] + right, b[:, h:]], axis=1)
        h *= 2
        ahead[h], after[h] = a.reshape(rows, WIDE), b.reshape(rows, WIDE)
    return ahead, after


def lin_kernel(
    pieces_ref,
    gain_ref,
    wr_ref,
    wk_ref,
    wv_ref,
    wq_ref,
    down_ref,
    up_ref,
    bias_ref,
    shift_ref,
    rate_ref,
    gate_ref,
    send_ref,
    gates_ref,
    reach_ref,
    local_ref,
    pairs_ref,
):
    scaled, inverse = scaled_pieces(pieces_ref, gain_ref)
    rows = shift_ref.shape[0]
    send_ref[0:rows] = projected(scaled, inverse, wq_ref)
    recv = projected(scaled, inverse, wr_ref).astype(F32)
    key = projected(scaled, inverse, wk_ref).astype(F32)
    value = projected(scaled, inverse, wv_ref)
    low = projected(scaled, inverse, down_ref).astype(F32)
    exponent = bias_ref[...] + shift_ref[...] + dot(jnp.tanh(low).astype(BF16), up_ref[...])
    log_decay = -jnp.exp(exponent)
    unit = key * lax.rsqrt(by_head(key * key) + 1e-6)
    rate = unit * rate_ref[...]

    ahead, after = spans(log_decay)
    lane = iota((rows, WIDE), 1)
    row = iota((rows, WIDE), 0)
    tall = iota((rows, rows), 0)
    flat = iota((rows, rows), 1)
    heads = [lane < HEAD_LIN, lane >= HEAD_LIN]

    def of_heads(a):
        return [jnp.where(mine, a, 0.0).astype(BF16) for mine in heads]

    eye = tall == flat
    right_now = jnp.concatenate([key, rate], axis=0).astype(BF16)
    for n, q_part in enumerate(of_heads(recv)):
        product = dot(q_part, right_now, ((1,), (1,)))
        for m in range(2):
            mine = slice(m * rows, (m + 1) * rows)
            pairs_ref[n, 1, :, mine] = jnp.where(eye, product[:, mine], 0.0)
            pairs_ref[n, 0, :, mine] = jnp.zeros((rows, rows), F32)
    h, level = 1, 0
    while h < rows:
        late = (row & h) != 0
        to_u = jnp.where(late, jnp.exp(ahead[h]), 0.0)
        to_q = jnp.where(late, jnp.exp(ahead[h] + log_decay), 0.0)
        from_s = jnp.where(late, 0.0, jnp.exp(after[h]))
        right = jnp.concatenate([key * from_s, rate * from_s], axis=0).astype(BF16)
        left = of_heads(unit * to_u), of_heads(recv * to_q)
        here = ((tall >> (level + 1)) == (flat >> (level + 1))) & ((tall & h) != 0) & (
            (flat & h) == 0
        )
        for n in range(2):
            for k in range(2):
                product = dot(left[k][n], right, ((1,), (1,)))
                for m in range(2):
                    mine = slice(m * rows, (m + 1) * rows)
                    pairs_ref[n, k, :, mine] = jnp.where(
                        here, product[:, mine], pairs_ref[n, k, :, mine]
                    )
        h *= 2
        level += 1

    solved = [jnp.where(eye, 1.0, 0.0) for _ in range(2)]
    h, level = 1, 0
    while h < rows:
        here = ((tall >> (level + 1)) == (flat >> (level + 1))) & ((tall & h) != 0) & (
            (flat & h) == 0
        )
        for n in range(2):
            links = jnp.where(here, pairs_ref[n, 0, :, rows:], 0.0)
            if h == 1:
                solved[n] = solved[n] - links
            else:
                step = dot3(links, solved[n])
                solved[n] = solved[n] - dot3(solved[n], step)
        h *= 2
        level += 1

    full_u = unit * jnp.exp(ahead[rows])
    full_q = recv * jnp.exp(ahead[rows] + log_decay)
    tail = jnp.exp(after[rows])
    full_k = key * tail
    full_r = rate * tail
    reach, local, moved = [], [], []
    for n in range(2):
        add = dot2(pairs_ref[n, 0, :, :rows], value)
        source = jnp.where(heads[n], full_u, pltpu.roll(add, HEAD_LIN, 1))
        along = dot3(solved[n], source)
        taken = dot3(pairs_ref[n, 1, :, rows:], along)
        reach.append(full_q - taken)
        local.append(dot2(pairs_ref[n, 1, :, :rows], value) - pltpu.roll(taken, HEAD_LIN, 1))
        moved.append(dot3(along, full_r, ((0,), (0,))))
    reach_ref[...] = jnp.where(heads[0], reach[0], reach[1])
    local_ref[...] = jnp.where(heads[0], local[0], local[1])

    lane = iota((WIDE, WIDE), 1)
    row = iota((WIDE, WIDE), 0)
    same = (lane < HEAD_LIN) == (row < HEAD_LIN)
    added = pltpu.roll(dot2(full_k, value, ((0,), (0,))).T, HEAD_LIN, 0)
    last = jnp.exp(ahead[rows][rows - 1 : rows] + log_decay[rows - 1 : rows]) - 1.0
    packed = jnp.where(same, jnp.where(lane == row, last, 0.0), added)
    packed = packed - jnp.where(lane < HEAD_LIN, moved[0], moved[1])
    send_ref[rows : rows + WIDE] = packed.astype(BF16)
    gate = gate_ref[...]
    high, mid = parts_of(gate)
    low_part = (gate - high.astype(F32) - mid.astype(F32)).astype(BF16)
    none = jnp.zeros((10, WIDE), BF16)
    gates = jnp.concatenate([high, mid, low_part, none], axis=0)
    send_ref[rows + WIDE :] = gates
    gates_ref[...] = gates


def unpacked(packed):
    packed = packed.astype(F32)
    lane = iota((WIDE, WIDE), 1)
    row = iota((WIDE, WIDE), 0)
    same = (lane < HEAD_LIN) == (row < HEAD_LIN)
    return jnp.where(same, packed, 0.0), jnp.where(same, pltpu.roll(packed, HEAD_LIN, 0), 0.0)


def row_kernel(place_ref, gathered_ref, gates_ref, send_ref, before_ref, *, rows):
    y = place_ref[1]
    count = gathered_ref.shape[0]
    shape = (WIDE, WIDE)
    total = jnp.zeros(shape, F32), jnp.zeros(shape, F32)
    mine = total
    for j in range(count):
        mine = tuple(jnp.where(y == j, t, m) for t, m in zip(total, mine))
        moved, added = unpacked(gathered_ref[j, rows : rows + WIDE])
        if j == 0:
            total = moved, added
        else:
            total = (
                total[0] + moved + dot3(total[0], moved),
                total[1] + added + dot3(total[1], moved),
            )
    before_ref[0] = mine[0]
    before_ref[1] = mine[1]
    lane = iota(shape, 1)
    row = iota(shape, 0)
    same = (lane < HEAD_LIN) == (row < HEAD_LIN)
    packed = jnp.where(same, total[0], pltpu.roll(total[1], HEAD_LIN, 0))
    send_ref[0:WIDE] = packed.astype(BF16)
    send_ref[WIDE:] = gates_ref[...]


def mix_kernel(place_ref, state_ref, gathered_ref, before_ref, reach_ref, local_ref, gain_ref, out_ref):
    z = place_ref[0]
    none = jnp.zeros((HEAD_LIN, HEAD_LIN), F32)
    state = jnp.concatenate(
        [
            jnp.concatenate([state_ref[0], none], axis=1),
            jnp.concatenate([none, state_ref[1]], axis=1),
        ],
        axis=0,
    )

    def step(k, state):
        packed = gathered_ref[k]
        moved, added = unpacked(packed[0:WIDE])
        return state + dot2(state, moved.astype(BF16)) + added

    state = lax.fori_loop(0, z, step, state)
    state = state + dot3(state, before_ref[0]) + before_ref[1]
    raw = dot3(reach_ref[...], state, ((1,), (1,))) + local_ref[...]
    off = raw - by_head(raw) * (1.0 / HEAD_LIN)
    spread = by_head(off * off) * (1.0 / HEAD_LIN)
    out_ref[...] = (off * lax.rsqrt(spread + 0.00064) * gain_ref[...]).astype(BF16)


def joined(gates):
    gates = gates.astype(F32)
    return gates[0:2] + gates[2:4] + gates[4:6]


def att_kernel(place_ref, asked_ref, held_ref, keys_ref, out_ref, best_ref, sum_ref, *, rows):
    z, y = place_ref[0], place_ref[1]
    count = asked_ref.shape[0]
    scale = HEAD_ATT ** (-0.5) * LOG2E
    best_ref[...] = jnp.full(best_ref.shape, NEG, F32)
    sum_ref[...] = jnp.zeros(sum_ref.shape, F32)
    ones = jnp.ones((rows, HEAD_ATT), BF16)
    zero_gate = [joined(asked_ref[j, rows + WIDE : rows + WIDE + 16])[0:1, 0:1] for j in range(count)]

    def block(k, masked):
        start = pl.multiple_of(k * rows, rows)
        both = keys_ref[pl.ds(start, rows)]
        key = both[:, :HEAD_ATT]
        value = jnp.concatenate([both[:, HEAD_ATT:], ones], axis=1)
        gate = joined(held_ref[k][WIDE : WIDE + 16])
        gate = jnp.concatenate([gate[0:1], gate[1:2]], axis=1)
        for j in range(count):
            logits = dot(asked_ref[j, 0:rows], key, ((1,), (1,))) * scale
            logits = logits + (zero_gate[j] - gate) * LOG2E
            if masked:
                allowed = y * rows + iota(logits.shape, 1) <= j * rows + iota(logits.shape, 0)
                logits = jnp.where(allowed, logits, NEG)
            old = best_ref[j][:, 0:1]
            new = jnp.maximum(old, jnp.max(logits, axis=1, keepdims=True))
            weights = jnp.exp2(logits - new)
            if masked:
                weights = jnp.where(allowed, weights, 0.0)
            sum_ref[j] = sum_ref[j] * jnp.exp2(old - new) + dot(weights.astype(BF16), value)
            best_ref[j] = jnp.broadcast_to(new, (rows, WIDE))

    lax.fori_loop(0, z, lambda k, c: (block(k, False), c)[1], 0)
    block(z, True)
    third = iota((rows, WIDE), 1)
    for j in range(count):
        total = sum_ref[j][:, HEAD_ATT:]
        some = total > 0.0
        safe = jnp.where(some, total, 1.0)
        out_ref[j, :, :HEAD_ATT] = (sum_ref[j][:, :HEAD_ATT] / safe).astype(BF16)
        level = jnp.where(some, best_ref[j] + jnp.log(safe) * LOG2E, NEG)
        high, mid = parts_of(level)
        last = (level - high.astype(F32) - mid.astype(F32)).astype(BF16)
        level = jnp.where(third < 40, high.astype(F32), jnp.where(third < 80, mid.astype(F32), last.astype(F32)))
        out_ref[j, :, HEAD_ATT:] = level.astype(BF16)


def out_kernel(parts_ref, lin_ref, gain_ref, wl_ref, wa_ref, out_ref):
    count, rows = parts_ref.shape[0], parts_ref.shape[1]
    levels = []
    for j in range(count):
        level = parts_ref[j, :, HEAD_ATT:].astype(F32)
        levels.append(level[:, 0:1] + level[:, 40:41] + level[:, 80:81])
    top = functools.reduce(jnp.maximum, levels)
    total, raw = jnp.zeros((rows, 1), F32), jnp.zeros((rows, HEAD_ATT), F32)
    for j in range(count):
        share = jnp.exp2(levels[j] - top)
        total = total + share
        raw = raw + share * parts_ref[j, :, :HEAD_ATT].astype(F32)
    raw = raw / total
    size = jnp.mean(raw * raw, axis=1, keepdims=True)
    att = (raw * lax.rsqrt(size + 1e-6) * gain_ref[...]).astype(BF16)
    lin = lin_ref[...]
    width = out_ref.shape[2]
    for j in range(out_ref.shape[0]):
        mine = slice(j * width, (j + 1) * width)
        out_ref[j] = (dot(lin, wl_ref[:, mine]) + dot(att, wa_ref[:, mine])).astype(BF16)


def sent_to_all(a, axis):
    size = lax.axis_size(axis)
    return lax.all_to_all(jnp.broadcast_to(a[None], (size, *a.shape)), axis, 0, 0, tiled=True)


def smem():
    return pl.BlockSpec(memory_space=pltpu.SMEM)


def vmem():
    return pl.BlockSpec(memory_space=pltpu.VMEM)


def call(kernel, name, shapes, flops, size, scratch=(), scalars=0):
    def run(*operands):
        many = isinstance(shapes, (list, tuple))
        return pl.pallas_call(
            kernel,
            name=name,
            out_shape=shapes,
            in_specs=[smem()] * scalars + [vmem()] * (len(operands) - scalars),
            out_specs=[vmem()] * len(shapes) if many else vmem(),
            scratch_shapes=list(scratch),
            compiler_params=params(),
            cost_estimate=cost(flops, size),
        )(*operands)

    return run


def body(
    tokens,
    norm_gain,
    recv_weight,
    lin_key_weight,
    lin_value_weight,
    decay_down,
    decay_up,
    decay_log_bias,
    decay_shift,
    learn_rate,
    group_gain,
    initial_state,
    query_weight,
    att_key_weight,
    att_value_weight,
    gate_cache,
    att_gain,
    out_lin_weight,
    out_att_weight,
):
    rows = tokens.shape[0]
    nz, ny = lax.axis_size("z"), lax.axis_size("y")
    ntp = lax.axis_size(TP)
    model_width = norm_gain.shape[0]
    shape = jax.ShapeDtypeStruct
    place = jnp.stack([lax.axis_index("z"), lax.axis_index("y")]).astype(jnp.int32)
    gain = norm_gain.reshape(1, -1)

    pieces = sent_to_all(tokens, TP)
    kv = call(kv_kernel, "kv", shape((rows, 256), BF16), 2 * rows * model_width * 256, 1 << 21)(
        pieces, gain, att_key_weight, att_value_weight
    )
    keys = lax.all_gather(kv, "z", axis=0, tiled=True)

    extra = 16
    send, gates, reach, local = call(
        lin_kernel,
        "lin",
        (
            shape((rows + WIDE + extra, WIDE), BF16),
            shape((extra, WIDE), BF16),
            shape((rows, WIDE), F32),
            shape((rows, WIDE), F32),
        ),
        4 * 10**9,
        1 << 22,
        scratch=[pltpu.VMEM((2, 2, rows, 2 * rows), F32)],
    )(
        pieces,
        gain,
        recv_weight,
        lin_key_weight,
        lin_value_weight,
        query_weight,
        decay_down,
        decay_up,
        decay_log_bias.reshape(1, -1),
        decay_shift,
        learn_rate.reshape(1, -1),
        gate_cache.reshape(rows // WIDE, WIDE),
    )
    asked = sent_to_all(send, "y")
    row_send, before = call(
        functools.partial(row_kernel, rows=rows),
        "row",
        (shape((WIDE + extra, WIDE), BF16), shape((2, WIDE, WIDE), F32)),
        10**8,
        1 << 20,
        scalars=1,
    )(place, asked, gates)
    held = sent_to_all(row_send, "z")
    lin_mixed = call(
        mix_kernel, "mix", shape((rows, WIDE), BF16), 10**9, 1 << 20, scalars=1
    )(place, initial_state, held, before, reach, local, group_gain.reshape(1, -1))
    found = call(
        functools.partial(att_kernel, rows=rows),
        "att",
        shape((ny, rows, 256), BF16),
        ny * rows * nz * rows * 512,
        1 << 22,
        scratch=[
            pltpu.VMEM((ny, rows, WIDE), F32),
            pltpu.VMEM((ny, rows, 256), F32),
        ],
        scalars=1,
    )(place, asked, held, keys)
    parts = lax.all_to_all(found, "y", 0, 0, tiled=True)
    width = model_width // ntp
    partial = call(
        out_kernel, "out", shape((ntp, rows, width), BF16), 2 * rows * 256 * model_width, 1 << 21
    )(parts, lin_mixed, att_gain.reshape(1, -1), out_lin_weight, out_att_weight)
    tiles = lax.all_to_all(partial, TP, 0, 0, tiled=True)
    return jnp.sum(tiles.astype(F32), axis=0).astype(BF16)


def solution(mesh):
    sp, tp = mesh.shape["sp"], mesh.shape["tp"]
    cores = 2
    ny = math.isqrt(sp) // 2 if sp > 16 else 2
    torus = Mesh(mesh.devices.reshape(sp // ny, ny, tp // cores, cores), SP + TP)
    return jax.shard_map(
        body,
        mesh=torus,
        in_specs=(
            P(SP, TP),
            P(),
            P(None, TP),
            P(None, TP),
            P(None, TP),
            P(),
            P(None, TP),
            P(TP),
            P(SP, TP),
            P(TP),
            P(TP),
            P(TP, None, None),
            P(None, TP),
            P(None, TP),
            P(None, TP),
            P(SP, TP),
            P(TP),
            P(TP, None),
            P(TP, None),
        ),
        out_specs=P(SP, TP),
        check_vma=False,
    )
```

```python
import functools
import math

import jax
import jax.numpy as jnp
from jax import lax
from jax.experimental import pallas as pl
from jax.experimental.pallas import tpu as pltpu
from jax.sharding import Mesh
from jax.sharding import PartitionSpec as P

HEAD_LIN = 64
HEAD_ATT = 128
WIDE = 128
SP = ("z", "y")
TP = ("x", "c")
LOG2E = math.log2(math.e)
NEG = -1e30
F32 = jnp.float32
BF16 = jnp.bfloat16


def params(mib):
    return pltpu.CompilerParams(vmem_limit_bytes=mib * 1024 * 1024)


def cost(flops, size):
    return pl.CostEstimate(flops=flops, bytes_accessed=size, transcendentals=0)


def dot(a, b, dims=((1,), (0,))):
    return lax.dot_general(a, b, (dims, ((), ())), preferred_element_type=F32)


def parts_of(a):
    high = a.astype(BF16)
    return high, (a - high.astype(F32)).astype(BF16)


def dot3(a, b, dims=((1,), (0,))):
    ah, al = parts_of(a)
    bh, bl = parts_of(b)
    return dot(ah, bh, dims) + (dot(ah, bl, dims) + dot(al, bh, dims))


def dot2(a, b, dims=((1,), (0,))):
    ah, al = parts_of(a)
    return dot(ah, b, dims) + dot(al, b, dims)


def iota(shape, dim):
    return lax.broadcasted_iota(jnp.int32, shape, dim)


def by_head(a):
    left = iota(a.shape, 1) < HEAD_LIN
    first = jnp.sum(jnp.where(left, a, 0.0), axis=1, keepdims=True)
    second = jnp.sum(jnp.where(left, 0.0, a), axis=1, keepdims=True)
    return jnp.where(left, first, second)


def scaled_pieces(place_ref, own_ref, other_ref, gain_ref):
    shards, rows, depth = own_ref.shape
    core = place_ref[2]
    scaled, squares = [], jnp.zeros((rows, depth), F32)
    for c, ref in enumerate((own_ref, other_ref)):
        for j in range(shards):
            start = pl.multiple_of((2 * j + (core if c == 0 else 1 - core)) * depth, depth)
            wide = ref[j].astype(F32)
            scaled.append(((wide * gain_ref[:, pl.ds(start, depth)]).astype(BF16), start))
            squares = squares + wide * wide
    mean = jnp.sum(squares, axis=1, keepdims=True) / (2 * shards * depth)
    return scaled, lax.rsqrt(mean + 1e-6)


def projected(scaled, inverse, w_ref):
    total = 0.0
    for piece, start in scaled:
        total = total + dot(piece, w_ref[pl.ds(start, piece.shape[1])])
    return total * inverse


def stacked(a):
    return jnp.concatenate([a[:, :WIDE], a[:, WIDE:]], axis=0)


def kv_kernel(place_ref, own_ref, other_ref, gain_ref, wk_ref, wv_ref, out_ref):
    scaled, inverse = scaled_pieces(place_ref, own_ref, other_ref, gain_ref)
    rows = own_ref.shape[1]
    out_ref[0:rows] = projected(scaled, inverse, wk_ref).astype(BF16)
    out_ref[rows:] = stacked(projected(scaled, inverse, wv_ref).T.astype(BF16))


def spans(log_decay):
    rows = log_decay.shape[0]
    row = iota(log_decay.shape, 0)
    zero = jnp.zeros_like(log_decay)
    before = [None] + [pltpu.roll(log_decay, i, 0) for i in range(1, 8)]
    behind = [None] + [pltpu.roll(log_decay, rows - i, 0) for i in range(1, 8)]
    ahead, after = {1: zero}, {1: zero}
    for h in (2, 4, 8):
        place = row & (h - 1)
        a, b = zero, zero
        for i in range(1, h):
            a = a + jnp.where(place >= i, before[i], 0.0)
            b = b + jnp.where(place + i < h, behind[i], 0.0)
        ahead[h], after[h] = a, b
    h = 8
    while h < rows:
        shape = (rows // (2 * h), 2 * h, WIDE)
        a, b = ahead[h].reshape(shape), after[h].reshape(shape)
        step = log_decay.reshape(shape)
        left = a[:, h - 1 : h] + step[:, h - 1 : h]
        right = b[:, h : h + 1] + step[:, h : h + 1]
        a = jnp.concatenate([a[:, :h], a[:, h:] + left], axis=1)
        b = jnp.concatenate([b[:, :h] + right, b[:, h:]], axis=1)
        h *= 2
        ahead[h], after[h] = a.reshape(rows, WIDE), b.reshape(rows, WIDE)
    return ahead, after


def lin_kernel(
    place_ref,
    own_ref,
    other_ref,
    gain_ref,
    wr_ref,
    wk_ref,
    wv_ref,
    wq_ref,
    down_ref,
    up_ref,
    bias_ref,
    shift_ref,
    rate_ref,
    gate_ref,
    send_ref,
    gates_ref,
    reach_ref,
    local_ref,
    pairs_ref,
):
    scaled, inverse = scaled_pieces(place_ref, own_ref, other_ref, gain_ref)
    rows = shift_ref.shape[0]
    send_ref[0:rows] = stacked(projected(scaled, inverse, wq_ref).T.astype(BF16))
    recv = projected(scaled, inverse, wr_ref).astype(BF16).astype(F32)
    key = projected(scaled, inverse, wk_ref).astype(BF16).astype(F32)
    value = projected(scaled, inverse, wv_ref).astype(BF16)
    low = 0.0
    for piece, start in scaled:
        low = low + dot(piece, down_ref[:, pl.ds(start, piece.shape[1])], ((1,), (1,)))
    low = (low * inverse).astype(BF16).astype(F32)
    exponent = bias_ref[...] + shift_ref[...] + dot(jnp.tanh(low).astype(BF16), up_ref[...])
    log_decay = -jnp.exp(exponent)
    unit = key * lax.rsqrt(by_head(key * key) + 1e-6)
    rate = unit * rate_ref[...]

    ahead, after = spans(log_decay)
    half = rows // 2
    lane = iota((rows, WIDE), 1)
    row = iota((rows, WIDE), 0)
    tall = iota((half, half), 0)
    flat = iota((half, half), 1)
    heads = [lane < HEAD_LIN, lane >= HEAD_LIN]
    eye = tall == flat
    blocks = slice(0, half), slice(half, rows)

    def of_heads(a):
        return [jnp.where(mine, a, 0.0).astype(BF16) for mine in heads]

    def below(h):
        level = h.bit_length()
        near = (tall >> level) == (flat >> level)
        return near & ((tall & h) != 0) & ((flat & h) == 0)

    for m, source in enumerate((key, rate)):
        now = by_head(recv * source)
        for n in range(2):
            for b in range(2):
                cols = slice(m * rows + b * half, m * rows + (b + 1) * half)
                same_row = now[blocks[b], n * HEAD_LIN : n * HEAD_LIN + 1]
                pairs_ref[n, 1, blocks[b], cols] = jnp.where(eye, same_row, 0.0)
                pairs_ref[n, 0, blocks[b], cols] = jnp.zeros((half, half), F32)
            cols = slice(m * rows + half, (m + 1) * rows)
            for k in range(2):
                pairs_ref[n, k, blocks[0], cols] = jnp.zeros((half, half), F32)
    h = 1
    while h < rows:
        late = (row & h) != 0
        to_u = jnp.where(late, jnp.exp(ahead[h]), 0.0)
        to_q = jnp.where(late, jnp.exp(ahead[h] + log_decay), 0.0)
        from_s = jnp.where(late, 0.0, jnp.exp(after[h]))
        right = (key * from_s).astype(BF16), (rate * from_s).astype(BF16)
        left = of_heads(unit * to_u) + of_heads(recv * to_q)
        for b in range(2) if h < half else (1,):
            c = b if h < half else 0
            product = dot(
                jnp.concatenate([a[blocks[b]] for a in left], axis=0),
                jnp.concatenate([a[blocks[c]] for a in right], axis=0),
                ((1,), (1,)),
            )
            for k in range(2):
                for n in range(2):
                    for m in range(2):
                        cols = slice(m * rows + c * half, m * rows + (c + 1) * half)
                        new = product[
                            (2 * k + n) * half : (2 * k + n + 1) * half,
                            m * half : (m + 1) * half,
                        ]
                        if h < half:
                            new = jnp.where(below(h), new, pairs_ref[n, k, blocks[b], cols])
                        pairs_ref[n, k, blocks[b], cols] = new
        h *= 2

    solved = {}
    h = 1
    while h < half:
        here = below(h)
        for n in range(2):
            for b in range(2):
                cols = slice(rows + b * half, rows + (b + 1) * half)
                links = jnp.where(here, pairs_ref[n, 0, blocks[b], cols], 0.0)
                if h == 1:
                    solved[n, b] = jnp.where(eye, 1.0, 0.0) - links
                else:
                    step = dot3(links, solved[n, b])
                    solved[n, b] = solved[n, b] - dot3(solved[n, b], step)
        h *= 2

    full_u = unit * jnp.exp(ahead[rows])
    full_q = recv * jnp.exp(ahead[rows] + log_decay)
    tail = jnp.exp(after[rows])
    full_k = key * tail
    full_r = rate * tail
    reach, local, moved = [], [], []
    for n in range(2):
        add = dot2(pairs_ref[n, 0, :, :rows], value)
        source = jnp.where(heads[n], full_u, pltpu.roll(add, HEAD_LIN, 1))
        first = dot3(solved[n, 0], source[:half])
        later = source[half:] - dot3(pairs_ref[n, 0, half:, rows : rows + half], first)
        along = jnp.concatenate([first, dot3(solved[n, 1], later)], axis=0)
        taken = dot3(pairs_ref[n, 1, :, rows:], along)
        reach.append(full_q - taken)
        local.append(dot2(pairs_ref[n, 1, :, :rows], value) - pltpu.roll(taken, HEAD_LIN, 1))
        moved.append(dot3(along, full_r, ((0,), (0,))))
    reach_ref[...] = jnp.where(heads[0], reach[0], reach[1])
    local_ref[...] = jnp.where(heads[0], local[0], local[1])

    lane = iota((WIDE, WIDE), 1)
    row = iota((WIDE, WIDE), 0)
    same = (lane < HEAD_LIN) == (row < HEAD_LIN)
    added = pltpu.roll(dot2(full_k, value, ((0,), (0,))).T, HEAD_LIN, 0)
    last = jnp.exp(ahead[rows][rows - 1 : rows] + log_decay[rows - 1 : rows]) - 1.0
    packed = jnp.where(same, jnp.where(lane == row, last, 0.0), added)
    packed = packed - jnp.where(lane < HEAD_LIN, moved[0], moved[1])
    send_ref[rows : rows + WIDE] = packed.astype(BF16)
    gate = gate_ref[...]
    high, mid = parts_of(gate)
    low_part = (gate - high.astype(F32) - mid.astype(F32)).astype(BF16)
    none = jnp.zeros((10, WIDE), BF16)
    gates = jnp.concatenate([high, mid, low_part, none], axis=0)
    send_ref[rows + WIDE :] = gates
    gates_ref[...] = gates


def unpacked(packed):
    packed = packed.astype(F32)
    lane = iota((WIDE, WIDE), 1)
    row = iota((WIDE, WIDE), 0)
    same = (lane < HEAD_LIN) == (row < HEAD_LIN)
    return jnp.where(same, packed, 0.0), jnp.where(same, pltpu.roll(packed, HEAD_LIN, 0), 0.0)


def row_kernel(place_ref, gathered_ref, gates_ref, send_ref, before_ref, *, rows):
    y = place_ref[1]
    count = gathered_ref.shape[0]
    shape = (WIDE, WIDE)
    total = jnp.zeros(shape, F32), jnp.zeros(shape, F32)
    mine = total
    for j in range(count):
        mine = tuple(jnp.where(y == j, t, m) for t, m in zip(total, mine))
        moved, added = unpacked(gathered_ref[j, rows : rows + WIDE])
        if j == 0:
            total = moved, added
        else:
            total = (
                total[0] + moved + dot3(total[0], moved),
                total[1] + added + dot3(total[1], moved),
            )
    before_ref[0] = mine[0]
    before_ref[1] = mine[1]
    lane = iota(shape, 1)
    row = iota(shape, 0)
    same = (lane < HEAD_LIN) == (row < HEAD_LIN)
    packed = jnp.where(same, total[0], pltpu.roll(total[1], HEAD_LIN, 0))
    send_ref[0:WIDE] = packed.astype(BF16)
    send_ref[WIDE:] = gates_ref[...]


def mix_kernel(place_ref, state_ref, gathered_ref, before_ref, reach_ref, local_ref, gain_ref, out_ref):
    z = place_ref[0]
    none = jnp.zeros((HEAD_LIN, HEAD_LIN), F32)
    state = jnp.concatenate(
        [
            jnp.concatenate([state_ref[0], none], axis=1),
            jnp.concatenate([none, state_ref[1]], axis=1),
        ],
        axis=0,
    )

    def step(k, state):
        packed = gathered_ref[k]
        moved, added = unpacked(packed[0:WIDE])
        return state + dot2(state, moved.astype(BF16)) + added

    state = lax.fori_loop(0, z, step, state)
    state = state + dot3(state, before_ref[0]) + before_ref[1]
    raw = dot3(reach_ref[...], state, ((1,), (1,))) + local_ref[...]
    off = raw - by_head(raw) * (1.0 / HEAD_LIN)
    spread = by_head(off * off) * (1.0 / HEAD_LIN)
    out_ref[...] = (off * lax.rsqrt(spread + 0.00064) * gain_ref[...]).astype(BF16)


def joined(gates):
    gates = gates.astype(F32)
    return gates[0:2] + gates[2:4] + gates[4:6]


def att_kernel(
    place_ref, asked_ref, held_ref, keys_ref, out_ref, best_ref, sum_ref, block_ref, sems, *, rows
):
    z, y = place_ref[0], place_ref[1]
    count = asked_ref.shape[0]
    scale = HEAD_ATT ** (-0.5) * LOG2E

    def fetch(k):
        start = pl.multiple_of(k * 2 * rows, 2 * rows)
        return pltpu.make_async_copy(
            keys_ref.at[pl.ds(start, 2 * rows)], block_ref.at[k], sems.at[k]
        )

    lax.fori_loop(0, z + 1, lambda k, c: (fetch(k).start(), c)[1], 0)
    best_ref[...] = jnp.full(best_ref.shape, NEG, F32)
    sum_ref[...] = jnp.zeros(sum_ref.shape, F32)
    ones = jnp.ones((16, rows), BF16)
    base = joined(asked_ref[0, rows + WIDE : rows + WIDE + 16])[0:1, 0:1]

    def block(k, masked):
        fetch(k).wait()
        key = block_ref[k, 0:rows]
        left, right = block_ref[k, rows : rows + WIDE], block_ref[k, rows + WIDE :]
        value = jnp.concatenate([jnp.concatenate([left, right], axis=1), ones], axis=0)
        drop = (base - joined(held_ref[k, WIDE : WIDE + 16])) * LOG2E
        drop = [jnp.broadcast_to(drop[i : i + 1], (WIDE, WIDE)).T for i in range(2)]
        drop = jnp.concatenate(drop, axis=0)
        drop = jnp.concatenate([drop, drop], axis=1)
        for j in range(count):
            asked = jnp.concatenate([asked_ref[j, 0:WIDE], asked_ref[j, WIDE:rows]], axis=1)
            logits = dot(key, asked) * scale + drop
            if masked:
                allowed = y * rows + iota(logits.shape, 0) <= j * rows + iota(logits.shape, 1)
                logits = jnp.where(allowed, logits, NEG)
            old = best_ref[j]
            new = jnp.maximum(old, jnp.max(logits, axis=0, keepdims=True))
            weights = jnp.exp2(logits - new)
            if masked:
                weights = jnp.where(allowed, weights, 0.0)
            sum_ref[j] = sum_ref[j] * jnp.exp2(old - new) + dot(value, weights.astype(BF16))
            best_ref[j] = new

    lax.fori_loop(0, z, lambda k, c: (block(k, False), c)[1], 0)
    block(z, True)
    third = iota((16, rows), 0)
    for j in range(count):
        total = sum_ref[j, HEAD_ATT : HEAD_ATT + 1]
        some = total > 0.0
        safe = jnp.where(some, total, 1.0)
        out_ref[j, 0:HEAD_ATT] = (sum_ref[j, 0:HEAD_ATT] / safe).astype(BF16)
        level = jnp.where(some, best_ref[j] + jnp.log(safe) * LOG2E, NEG)
        high, mid = parts_of(level)
        high, mid = high.astype(F32), mid.astype(F32)
        last = level - high - mid
        level = jnp.where(third == 0, high, jnp.where(third == 1, mid, last))
        out_ref[j, HEAD_ATT:] = level.astype(BF16)


def out_kernel(place_ref, parts_ref, lin_ref, gain_ref, wl_ref, wa_ref, own_ref, other_ref):
    count, rows = parts_ref.shape[0], parts_ref.shape[2]
    core = place_ref[2]
    levels = []
    for j in range(count):
        level = parts_ref[j, HEAD_ATT:].astype(F32)
        levels.append(level[0:1] + level[1:2] + level[2:3])
    top = functools.reduce(jnp.maximum, levels)
    total, raw = jnp.zeros((1, rows), F32), jnp.zeros((HEAD_ATT, rows), F32)
    for j in range(count):
        share = jnp.exp2(levels[j] - top)
        total = total + share
        raw = raw + share * parts_ref[j, 0:HEAD_ATT].astype(F32)
    raw = raw / total
    size = jnp.mean(raw * raw, axis=0, keepdims=True)
    att = ((raw * lax.rsqrt(size + 1e-6)).T * gain_ref[...]).astype(BF16)
    lin = lin_ref[...]
    width = own_ref.shape[2]
    for c, ref in enumerate((own_ref, other_ref)):
        for j in range(ref.shape[0]):
            start = pl.multiple_of((2 * j + (core if c == 0 else 1 - core)) * width, width)
            mine = pl.ds(start, width)
            ref[j] = (dot(lin, wl_ref[:, mine]) + dot(att, wa_ref[:, mine])).astype(BF16)


def sent_to_all(a, axis):
    size = lax.axis_size(axis)
    return lax.all_to_all(jnp.broadcast_to(a[None], (size, *a.shape)), axis, 0, 0, tiled=True)


def to_other_core(a):
    return lax.ppermute(a, "c", [(0, 1), (1, 0)])


def smem():
    return pl.BlockSpec(memory_space=pltpu.SMEM)


def vmem():
    return pl.BlockSpec(memory_space=pltpu.VMEM)


def hbm():
    return pl.BlockSpec(memory_space=pltpu.HBM)


def call(kernel, name, shapes, flops, size, mib, scratch=(), outside=0):
    def run(*operands):
        many = isinstance(shapes, (list, tuple))
        inside = len(operands) - 1 - outside
        return pl.pallas_call(
            kernel,
            name=name,
            out_shape=shapes,
            in_specs=[smem()] + [vmem()] * inside + [hbm()] * outside,
            out_specs=[vmem()] * len(shapes) if many else vmem(),
            scratch_shapes=list(scratch),
            compiler_params=params(mib),
            cost_estimate=cost(flops, size),
        )(*operands)

    return run


def body(
    tokens,
    norm_gain,
    recv_weight,
    lin_key_weight,
    lin_value_weight,
    decay_down,
    decay_up,
    decay_log_bias,
    decay_shift,
    learn_rate,
    group_gain,
    initial_state,
    query_weight,
    att_key_weight,
    att_value_weight,
    gate_cache,
    att_gain,
    out_lin_weight,
    out_att_weight,
):
    rows = tokens.shape[0]
    nz, ny, nx = (lax.axis_size(axis) for axis in ("z", "y", "x"))
    model_width = norm_gain.shape[0]
    shape = jax.ShapeDtypeStruct
    place = jnp.stack([lax.axis_index(axis) for axis in ("z", "y", "c")]).astype(jnp.int32)
    gain = norm_gain.reshape(1, -1)

    own = sent_to_all(tokens, "x")
    other = to_other_core(own)
    kv = call(
        kv_kernel, "kv", shape((2 * rows, WIDE), BF16), 2 * rows * model_width * 256, 1 << 21, 12
    )(place, own, other, gain, att_key_weight, att_value_weight)
    keys = lax.all_gather(kv, "z", axis=0, tiled=True)

    extra = 16
    send, gates, reach, local = call(
        lin_kernel,
        "lin",
        (
            shape((rows + WIDE + extra, WIDE), BF16),
            shape((extra, WIDE), BF16),
            shape((rows, WIDE), F32),
            shape((rows, WIDE), F32),
        ),
        4 * 10**9,
        1 << 22,
        24,
        scratch=[pltpu.VMEM((2, 2, rows, 2 * rows), F32)],
    )(
        place,
        own,
        other,
        gain,
        recv_weight,
        lin_key_weight,
        lin_value_weight,
        query_weight,
        decay_down.T,
        decay_up,
        decay_log_bias.reshape(1, -1),
        decay_shift,
        learn_rate.reshape(1, -1),
        gate_cache.reshape(rows // WIDE, WIDE),
    )
    asked = sent_to_all(send, "y")
    row_send, before = call(
        functools.partial(row_kernel, rows=rows),
        "row",
        (shape((WIDE + extra, WIDE), BF16), shape((2, WIDE, WIDE), F32)),
        10**8,
        1 << 20,
        12,
    )(place, asked, gates)
    held = lax.all_gather(row_send, "z")
    lin_mixed = call(mix_kernel, "mix", shape((rows, WIDE), BF16), 10**9, 1 << 20, 12)(
        place, initial_state, held, before, reach, local, group_gain.reshape(1, -1)
    )
    asked, lin_mixed = lax.optimization_barrier((asked, lin_mixed))
    found = call(
        functools.partial(att_kernel, rows=rows),
        "att",
        shape((ny, HEAD_ATT + 16, rows), BF16),
        ny * rows * nz * rows * 512,
        1 << 22,
        24,
        scratch=[
            pltpu.VMEM((ny, 1, rows), F32),
            pltpu.VMEM((ny, HEAD_ATT + 16, rows), F32),
            pltpu.VMEM((nz, 2 * rows, WIDE), BF16),
            pltpu.SemaphoreType.DMA((nz,)),
        ],
        outside=1,
    )(place, asked, held, keys)
    parts = lax.all_to_all(found, "y", 0, 0, tiled=True)
    width = model_width // (2 * nx)
    tile = shape((nx, rows, width), BF16)
    mine, theirs = call(
        out_kernel, "out", (tile, tile), 2 * rows * 256 * model_width, 1 << 21, 12
    )(place, parts, lin_mixed, att_gain.reshape(1, -1), out_lin_weight, out_att_weight)
    pair = (mine.astype(F32) + to_other_core(theirs).astype(F32)).astype(BF16)
    tiles = lax.all_to_all(pair, "x", 0, 0, tiled=True)
    return jnp.sum(tiles.astype(F32), axis=0).astype(BF16)


def solution(mesh):
    sp, tp = mesh.shape["sp"], mesh.shape["tp"]
    cores = 2
    ny = math.isqrt(sp) // 2 if sp > 16 else 2
    torus = Mesh(mesh.devices.reshape(sp // ny, ny, tp // cores, cores), SP + TP)
    return jax.shard_map(
        body,
        mesh=torus,
        in_specs=(
            P(SP, TP),
            P(),
            P(None, TP),
            P(None, TP),
            P(None, TP),
            P(),
            P(None, TP),
            P(TP),
            P(SP, TP),
            P(TP),
            P(TP),
            P(TP, None, None),
            P(None, TP),
            P(None, TP),
            P(None, TP),
            P(SP, TP),
            P(TP),
            P(TP, None),
            P(TP, None),
        ),
        out_specs=P(SP, TP),
        check_vma=False,
    )
```

```python
import functools
import math

import jax
import jax.numpy as jnp
from jax import lax
from jax.experimental import pallas as pl
from jax.experimental.pallas import tpu as pltpu
from jax.sharding import Mesh
from jax.sharding import PartitionSpec as P

HEAD_LIN = 64
HEAD_ATT = 128
WIDE = 128
SP = ("z", "y")
TP = ("x", "c")
LOG2E = math.log2(math.e)
NEG = -1e30
F32 = jnp.float32
BF16 = jnp.bfloat16


def params(mib):
    return pltpu.CompilerParams(vmem_limit_bytes=mib * 1024 * 1024)


def cost(flops, size):
    return pl.CostEstimate(flops=flops, bytes_accessed=size, transcendentals=0)


def dot(a, b, dims=((1,), (0,))):
    return lax.dot_general(a, b, (dims, ((), ())), preferred_element_type=F32)


def parts_of(a):
    high = a.astype(BF16)
    return high, (a - high.astype(F32)).astype(BF16)


def dot3(a, b, dims=((1,), (0,))):
    ah, al = parts_of(a)
    bh, bl = parts_of(b)
    return dot(ah, bh, dims) + (dot(ah, bl, dims) + dot(al, bh, dims))


def dot2(a, b, dims=((1,), (0,))):
    ah, al = parts_of(a)
    return dot(ah, b, dims) + dot(al, b, dims)


def iota(shape, dim):
    return lax.broadcasted_iota(jnp.int32, shape, dim)


def by_head(a):
    left = iota(a.shape, 1) < HEAD_LIN
    first = jnp.sum(jnp.where(left, a, 0.0), axis=1, keepdims=True)
    second = jnp.sum(jnp.where(left, 0.0, a), axis=1, keepdims=True)
    return jnp.where(left, first, second)


def scaled_pieces(place_ref, own_ref, other_ref, gain_ref):
    shards, rows, depth = own_ref.shape
    core = place_ref[2]
    scaled, squares = [], jnp.zeros((rows, depth), F32)
    for c, ref in enumerate((own_ref, other_ref)):
        for j in range(shards):
            start = pl.multiple_of((2 * j + (core if c == 0 else 1 - core)) * depth, depth)
            wide = ref[j].astype(F32)
            scaled.append(((wide * gain_ref[:, pl.ds(start, depth)]).astype(BF16), start))
            squares = squares + wide * wide
    mean = jnp.sum(squares, axis=1, keepdims=True) / (2 * shards * depth)
    return scaled, lax.rsqrt(mean + 1e-6)


def projected(scaled, inverse, w_ref):
    total = 0.0
    for piece, start in scaled:
        total = total + dot(piece, w_ref[pl.ds(start, piece.shape[1])])
    return total * inverse


def stacked(a):
    return jnp.concatenate([a[:, :WIDE], a[:, WIDE:]], axis=0)


def spread_kernel(place_ref, tokens_ref, out_ref):
    tokens = tokens_ref[...]
    for j in range(out_ref.shape[0]):
        out_ref[j] = tokens


def kv_kernel(place_ref, own_ref, other_ref, gain_ref, wk_ref, wv_ref, out_ref):
    scaled, inverse = scaled_pieces(place_ref, own_ref, other_ref, gain_ref)
    rows = own_ref.shape[1]
    out_ref[0:rows] = projected(scaled, inverse, wk_ref).astype(BF16)
    out_ref[rows:] = stacked(projected(scaled, inverse, wv_ref).T.astype(BF16))


def spans(log_decay):
    rows = log_decay.shape[0]
    row = iota(log_decay.shape, 0)
    zero = jnp.zeros_like(log_decay)
    before = [None] + [pltpu.roll(log_decay, i, 0) for i in range(1, 8)]
    behind = [None] + [pltpu.roll(log_decay, rows - i, 0) for i in range(1, 8)]
    ahead, after = {1: zero}, {1: zero}
    for h in (2, 4, 8):
        place = row & (h - 1)
        a, b = zero, zero
        for i in range(1, h):
            a = a + jnp.where(place >= i, before[i], 0.0)
            b = b + jnp.where(place + i < h, behind[i], 0.0)
        ahead[h], after[h] = a, b
    h = 8
    while h < rows:
        shape = (rows // (2 * h), 2 * h, WIDE)
        a, b = ahead[h].reshape(shape), after[h].reshape(shape)
        step = log_decay.reshape(shape)
        left = a[:, h - 1 : h] + step[:, h - 1 : h]
        right = b[:, h : h + 1] + step[:, h : h + 1]
        a = jnp.concatenate([a[:, :h], a[:, h:] + left], axis=1)
        b = jnp.concatenate([b[:, :h] + right, b[:, h:]], axis=1)
        h *= 2
        ahead[h], after[h] = a.reshape(rows, WIDE), b.reshape(rows, WIDE)
    return ahead, after


def lin_kernel(
    place_ref,
    own_ref,
    other_ref,
    gain_ref,
    wr_ref,
    wk_ref,
    wv_ref,
    wq_ref,
    down_ref,
    up_ref,
    bias_ref,
    shift_ref,
    rate_ref,
    gate_ref,
    send_ref,
    gates_ref,
    reach_ref,
    local_ref,
    pairs_ref,
):
    scaled, inverse = scaled_pieces(place_ref, own_ref, other_ref, gain_ref)
    rows = shift_ref.shape[0]
    send_ref[0:rows] = stacked(projected(scaled, inverse, wq_ref).T.astype(BF16))
    recv = projected(scaled, inverse, wr_ref).astype(BF16).astype(F32)
    key = projected(scaled, inverse, wk_ref).astype(BF16).astype(F32)
    value = projected(scaled, inverse, wv_ref).astype(BF16)
    low = 0.0
    for piece, start in scaled:
        low = low + dot(piece, down_ref[:, pl.ds(start, piece.shape[1])], ((1,), (1,)))
    low = (low * inverse).astype(BF16).astype(F32)
    exponent = bias_ref[...] + shift_ref[...] + dot(jnp.tanh(low).astype(BF16), up_ref[...])
    log_decay = -jnp.exp(exponent)
    unit = key * lax.rsqrt(by_head(key * key) + 1e-6)
    rate = unit * rate_ref[...]

    ahead, after = spans(log_decay)
    half = rows // 2
    lane = iota((rows, WIDE), 1)
    row = iota((rows, WIDE), 0)
    tall = iota((half, half), 0)
    flat = iota((half, half), 1)
    heads = [lane < HEAD_LIN, lane >= HEAD_LIN]
    eye = tall == flat
    blocks = slice(0, half), slice(half, rows)

    def of_heads(a):
        return [jnp.where(mine, a, 0.0).astype(BF16) for mine in heads]

    def below(h):
        level = h.bit_length()
        near = (tall >> level) == (flat >> level)
        return near & ((tall & h) != 0) & ((flat & h) == 0)

    for m, source in enumerate((key, rate)):
        now = by_head(recv * source)
        for n in range(2):
            for b in range(2):
                cols = slice(m * rows + b * half, m * rows + (b + 1) * half)
                same_row = now[blocks[b], n * HEAD_LIN : n * HEAD_LIN + 1]
                pairs_ref[n, 1, blocks[b], cols] = jnp.where(eye, same_row, 0.0)
                pairs_ref[n, 0, blocks[b], cols] = jnp.zeros((half, half), F32)
            cols = slice(m * rows + half, (m + 1) * rows)
            for k in range(2):
                pairs_ref[n, k, blocks[0], cols] = jnp.zeros((half, half), F32)
    h = 1
    while h < rows:
        late = (row & h) != 0
        to_u = jnp.where(late, jnp.exp(ahead[h]), 0.0)
        to_q = jnp.where(late, jnp.exp(ahead[h] + log_decay), 0.0)
        from_s = jnp.where(late, 0.0, jnp.exp(after[h]))
        right = (key * from_s).astype(BF16), (rate * from_s).astype(BF16)
        left = of_heads(unit * to_u) + of_heads(recv * to_q)
        for b in range(2) if h < half else (1,):
            c = b if h < half else 0
            product = dot(
                jnp.concatenate([a[blocks[b]] for a in left], axis=0),
                jnp.concatenate([a[blocks[c]] for a in right], axis=0),
                ((1,), (1,)),
            )
            for k in range(2):
                for n in range(2):
                    for m in range(2):
                        cols = slice(m * rows + c * half, m * rows + (c + 1) * half)
                        new = product[
                            (2 * k + n) * half : (2 * k + n + 1) * half,
                            m * half : (m + 1) * half,
                        ]
                        if h < half:
                            new = jnp.where(below(h), new, pairs_ref[n, k, blocks[b], cols])
                        pairs_ref[n, k, blocks[b], cols] = new
        h *= 2

    solved = {}
    h = 1
    while h < half:
        here = below(h)
        for n in range(2):
            for b in range(2):
                cols = slice(rows + b * half, rows + (b + 1) * half)
                links = jnp.where(here, pairs_ref[n, 0, blocks[b], cols], 0.0)
                if h == 1:
                    solved[n, b] = jnp.where(eye, 1.0, 0.0) - links
                else:
                    step = dot3(links, solved[n, b])
                    solved[n, b] = solved[n, b] - dot3(solved[n, b], step)
        h *= 2

    full_u = unit * jnp.exp(ahead[rows])
    full_q = recv * jnp.exp(ahead[rows] + log_decay)
    tail = jnp.exp(after[rows])
    full_k = key * tail
    full_r = rate * tail
    reach, local, moved = [], [], []
    for n in range(2):
        add = dot2(pairs_ref[n, 0, :, :rows], value)
        source = jnp.where(heads[n], full_u, pltpu.roll(add, HEAD_LIN, 1))
        first = dot3(solved[n, 0], source[:half])
        later = source[half:] - dot3(pairs_ref[n, 0, half:, rows : rows + half], first)
        along = jnp.concatenate([first, dot3(solved[n, 1], later)], axis=0)
        taken = dot3(pairs_ref[n, 1, :, rows:], along)
        reach.append(full_q - taken)
        local.append(dot2(pairs_ref[n, 1, :, :rows], value) - pltpu.roll(taken, HEAD_LIN, 1))
        moved.append(dot3(along, full_r, ((0,), (0,))))
    reach_ref[...] = jnp.where(heads[0], reach[0], reach[1])
    local_ref[...] = jnp.where(heads[0], local[0], local[1])

    lane = iota((WIDE, WIDE), 1)
    row = iota((WIDE, WIDE), 0)
    same = (lane < HEAD_LIN) == (row < HEAD_LIN)
    added = pltpu.roll(dot2(full_k, value, ((0,), (0,))).T, HEAD_LIN, 0)
    last = jnp.exp(ahead[rows][rows - 1 : rows] + log_decay[rows - 1 : rows]) - 1.0
    packed = jnp.where(same, jnp.where(lane == row, last, 0.0), added)
    packed = packed - jnp.where(lane < HEAD_LIN, moved[0], moved[1])
    send_ref[rows : rows + WIDE] = packed.astype(BF16)
    gate = gate_ref[...]
    high, mid = parts_of(gate)
    low_part = (gate - high.astype(F32) - mid.astype(F32)).astype(BF16)
    none = jnp.zeros((10, WIDE), BF16)
    gates = jnp.concatenate([high, mid, low_part, none], axis=0)
    send_ref[rows + WIDE :] = gates
    gates_ref[...] = gates


def unpacked(packed):
    packed = packed.astype(F32)
    lane = iota((WIDE, WIDE), 1)
    row = iota((WIDE, WIDE), 0)
    same = (lane < HEAD_LIN) == (row < HEAD_LIN)
    return jnp.where(same, packed, 0.0), jnp.where(same, pltpu.roll(packed, HEAD_LIN, 0), 0.0)


def row_kernel(place_ref, gathered_ref, gates_ref, send_ref, before_ref, *, rows):
    y = place_ref[1]
    count = gathered_ref.shape[0]
    shape = (WIDE, WIDE)
    total = jnp.zeros(shape, F32), jnp.zeros(shape, F32)
    mine = total
    for j in range(count):
        mine = tuple(jnp.where(y == j, t, m) for t, m in zip(total, mine))
        moved, added = unpacked(gathered_ref[j, rows : rows + WIDE])
        if j == 0:
            total = moved, added
        else:
            total = (
                total[0] + moved + dot3(total[0], moved),
                total[1] + added + dot3(total[1], moved),
            )
    before_ref[0] = mine[0]
    before_ref[1] = mine[1]
    lane = iota(shape, 1)
    row = iota(shape, 0)
    same = (lane < HEAD_LIN) == (row < HEAD_LIN)
    packed = jnp.where(same, total[0], pltpu.roll(total[1], HEAD_LIN, 0))
    send_ref[0:WIDE] = packed.astype(BF16)
    send_ref[WIDE:] = gates_ref[...]


def mix_kernel(place_ref, state_ref, gathered_ref, before_ref, reach_ref, local_ref, gain_ref, out_ref):
    z = place_ref[0]
    none = jnp.zeros((HEAD_LIN, HEAD_LIN), F32)
    state = jnp.concatenate(
        [
            jnp.concatenate([state_ref[0], none], axis=1),
            jnp.concatenate([none, state_ref[1]], axis=1),
        ],
        axis=0,
    )

    def step(k, state):
        packed = gathered_ref[k]
        moved, added = unpacked(packed[0:WIDE])
        return state + dot2(state, moved.astype(BF16)) + added

    state = lax.fori_loop(0, z, step, state)
    state = state + dot3(state, before_ref[0]) + before_ref[1]
    raw = dot3(reach_ref[...], state, ((1,), (1,))) + local_ref[...]
    off = raw - by_head(raw) * (1.0 / HEAD_LIN)
    spread = by_head(off * off) * (1.0 / HEAD_LIN)
    out_ref[...] = (off * lax.rsqrt(spread + 0.00064) * gain_ref[...]).astype(BF16)


def joined(gates):
    gates = gates.astype(F32)
    return gates[0:2] + gates[2:4] + gates[4:6]


def att_kernel(
    place_ref, asked_ref, held_ref, keys_ref, out_ref, best_ref, sum_ref, *, rows
):
    z, y = place_ref[0], place_ref[1]
    count = asked_ref.shape[0]
    scale = HEAD_ATT ** (-0.5) * LOG2E

    best_ref[...] = jnp.full(best_ref.shape, NEG, F32)
    sum_ref[...] = jnp.zeros(sum_ref.shape, F32)
    ones = jnp.ones((16, rows), BF16)
    base = joined(asked_ref[0, rows + WIDE : rows + WIDE + 16])[0:1, 0:1]

    def block(k, masked):
        both = keys_ref[k]
        key, left, right = both[:rows], both[rows : rows + WIDE], both[rows + WIDE :]
        value = jnp.concatenate([jnp.concatenate([left, right], axis=1), ones], axis=0)
        drop = (base - joined(held_ref[k, WIDE : WIDE + 16])) * LOG2E
        drop = [jnp.broadcast_to(drop[i : i + 1], (WIDE, WIDE)).T for i in range(2)]
        drop = jnp.concatenate(drop, axis=0)
        drop = jnp.concatenate([drop, drop], axis=1)
        for j in range(count):
            asked = jnp.concatenate([asked_ref[j, 0:WIDE], asked_ref[j, WIDE:rows]], axis=1)
            logits = dot(key, asked) * scale + drop
            if masked:
                allowed = y * rows + iota(logits.shape, 0) <= j * rows + iota(logits.shape, 1)
                logits = jnp.where(allowed, logits, NEG)
            old = best_ref[j]
            new = jnp.maximum(old, jnp.max(logits, axis=0, keepdims=True))
            weights = jnp.exp2(logits - new)
            if masked:
                weights = jnp.where(allowed, weights, 0.0)
            sum_ref[j] = sum_ref[j] * jnp.exp2(old - new) + dot(value, weights.astype(BF16))
            best_ref[j] = new

    lax.fori_loop(0, z, lambda k, c: (block(k, False), c)[1], 0)
    block(z, True)
    third = iota((16, rows), 0)
    for j in range(count):
        total = sum_ref[j, HEAD_ATT : HEAD_ATT + 1]
        some = total > 0.0
        safe = jnp.where(some, total, 1.0)
        out_ref[j, 0:HEAD_ATT] = (sum_ref[j, 0:HEAD_ATT] / safe).astype(BF16)
        level = jnp.where(some, best_ref[j] + jnp.log(safe) * LOG2E, NEG)
        high, mid = parts_of(level)
        high, mid = high.astype(F32), mid.astype(F32)
        last = level - high - mid
        level = jnp.where(third == 0, high, jnp.where(third == 1, mid, last))
        out_ref[j, HEAD_ATT:] = level.astype(BF16)


def out_kernel(place_ref, parts_ref, lin_ref, gain_ref, wl_ref, wa_ref, own_ref, other_ref):
    count, rows = parts_ref.shape[0], parts_ref.shape[2]
    core = place_ref[2]
    levels = []
    for j in range(count):
        level = parts_ref[j, HEAD_ATT:].astype(F32)
        levels.append(level[0:1] + level[1:2] + level[2:3])
    top = functools.reduce(jnp.maximum, levels)
    total, raw = jnp.zeros((1, rows), F32), jnp.zeros((HEAD_ATT, rows), F32)
    for j in range(count):
        share = jnp.exp2(levels[j] - top)
        total = total + share
        raw = raw + share * parts_ref[j, 0:HEAD_ATT].astype(F32)
    raw = raw / total
    size = jnp.mean(raw * raw, axis=0, keepdims=True)
    att = ((raw * lax.rsqrt(size + 1e-6)).T * gain_ref[...]).astype(BF16)
    lin = lin_ref[...]
    width = own_ref.shape[2]
    for c, ref in enumerate((own_ref, other_ref)):
        for j in range(ref.shape[0]):
            start = pl.multiple_of((2 * j + (core if c == 0 else 1 - core)) * width, width)
            mine = pl.ds(start, width)
            ref[j] = (dot(lin, wl_ref[:, mine]) + dot(att, wa_ref[:, mine])).astype(BF16)


def sent_to_all(a, axis):
    size = lax.axis_size(axis)
    return lax.all_to_all(jnp.broadcast_to(a[None], (size, *a.shape)), axis, 0, 0, tiled=True)


def to_other_core(a):
    return lax.ppermute(a, "c", [(0, 1), (1, 0)])


def smem():
    return pl.BlockSpec(memory_space=pltpu.SMEM)


def vmem():
    return pl.BlockSpec(memory_space=pltpu.VMEM)


def call(kernel, name, shapes, flops, size, mib, scratch=()):
    def run(*operands):
        many = isinstance(shapes, (list, tuple))
        return pl.pallas_call(
            kernel,
            name=name,
            out_shape=shapes,
            in_specs=[smem()] + [vmem()] * (len(operands) - 1),
            out_specs=[vmem()] * len(shapes) if many else vmem(),
            scratch_shapes=list(scratch),
            compiler_params=params(mib),
            cost_estimate=cost(flops, size),
        )(*operands)

    return run


def body(
    tokens,
    norm_gain,
    recv_weight,
    lin_key_weight,
    lin_value_weight,
    decay_down,
    decay_up,
    decay_log_bias,
    decay_shift,
    learn_rate,
    group_gain,
    initial_state,
    query_weight,
    att_key_weight,
    att_value_weight,
    gate_cache,
    att_gain,
    out_lin_weight,
    out_att_weight,
):
    rows = tokens.shape[0]
    nz, ny, nx = (lax.axis_size(axis) for axis in ("z", "y", "x"))
    model_width = norm_gain.shape[0]
    shape = jax.ShapeDtypeStruct
    place = jnp.stack([lax.axis_index(axis) for axis in ("z", "y", "c")]).astype(jnp.int32)
    gain = norm_gain.reshape(1, -1)

    copies = call(spread_kernel, "spread", shape((nx, *tokens.shape), BF16), 10**10, 1 << 24, 4)(
        place, tokens
    )
    own = lax.all_to_all(copies, "x", 0, 0, tiled=True)
    other = to_other_core(own)
    kv = call(
        kv_kernel, "kv", shape((2 * rows, WIDE), BF16), 2 * rows * model_width * 256, 1 << 21, 12
    )(place, own, other, gain, att_key_weight, att_value_weight)
    keys = lax.all_gather(kv, "z")

    extra = 16
    send, gates, reach, local = call(
        lin_kernel,
        "lin",
        (
            shape((rows + WIDE + extra, WIDE), BF16),
            shape((extra, WIDE), BF16),
            shape((rows, WIDE), F32),
            shape((rows, WIDE), F32),
        ),
        4 * 10**9,
        1 << 22,
        24,
        scratch=[pltpu.VMEM((2, 2, rows, 2 * rows), F32)],
    )(
        place,
        own,
        other,
        gain,
        recv_weight,
        lin_key_weight,
        lin_value_weight,
        query_weight,
        decay_down.T,
        decay_up,
        decay_log_bias.reshape(1, -1),
        decay_shift,
        learn_rate.reshape(1, -1),
        gate_cache.reshape(rows // WIDE, WIDE),
    )
    asked = sent_to_all(send, "y")
    row_send, before = call(
        functools.partial(row_kernel, rows=rows),
        "row",
        (shape((WIDE + extra, WIDE), BF16), shape((2, WIDE, WIDE), F32)),
        10**8,
        1 << 20,
        12,
    )(place, asked, gates)
    held = lax.all_gather(row_send, "z")
    lin_mixed = call(mix_kernel, "mix", shape((rows, WIDE), BF16), 10**9, 1 << 20, 12)(
        place, initial_state, held, before, reach, local, group_gain.reshape(1, -1)
    )
    asked, lin_mixed = lax.optimization_barrier((asked, lin_mixed))
    found = call(
        functools.partial(att_kernel, rows=rows),
        "att",
        shape((ny, HEAD_ATT + 16, rows), BF16),
        ny * rows * nz * rows * 512,
        1 << 22,
        24,
        scratch=[
            pltpu.VMEM((ny, 1, rows), F32),
            pltpu.VMEM((ny, HEAD_ATT + 16, rows), F32),
        ],
    )(place, asked, held, keys)
    parts = lax.all_to_all(found, "y", 0, 0, tiled=True)
    width = model_width // (2 * nx)
    tile = shape((nx, rows, width), BF16)
    mine, theirs = call(
        out_kernel, "out", (tile, tile), 2 * rows * 256 * model_width, 1 << 21, 12
    )(place, parts, lin_mixed, att_gain.reshape(1, -1), out_lin_weight, out_att_weight)
    pair = (mine.astype(F32) + to_other_core(theirs).astype(F32)).astype(BF16)
    tiles = lax.all_to_all(pair, "x", 0, 0, tiled=True)
    return jnp.sum(tiles.astype(F32), axis=0).astype(BF16)


def solution(mesh):
    sp, tp = mesh.shape["sp"], mesh.shape["tp"]
    cores = 2
    ny = math.isqrt(sp) // 2 if sp > 16 else 2
    torus = Mesh(mesh.devices.reshape(sp // ny, ny, tp // cores, cores), SP + TP)
    return jax.shard_map(
        body,
        mesh=torus,
        in_specs=(
            P(SP, TP),
            P(),
            P(None, TP),
            P(None, TP),
            P(None, TP),
            P(),
            P(None, TP),
            P(TP),
            P(SP, TP),
            P(TP),
            P(TP),
            P(TP, None, None),
            P(None, TP),
            P(None, TP),
            P(None, TP),
            P(SP, TP),
            P(TP),
            P(TP, None),
            P(TP, None),
        ),
        out_specs=P(SP, TP),
        check_vma=False,
    )
```

```python
import functools
import math

import jax
import jax.numpy as jnp
from jax import lax
from jax.experimental import pallas as pl
from jax.experimental.pallas import tpu as pltpu
from jax.sharding import Mesh
from jax.sharding import PartitionSpec as P

HEAD_LIN = 64
HEAD_ATT = 128
WIDE = 128
SP = ("z", "y")
TP = ("x", "c")
LOG2E = math.log2(math.e)
NEG = -1e30
F32 = jnp.float32
BF16 = jnp.bfloat16


def params(mib):
    return pltpu.CompilerParams(vmem_limit_bytes=mib * 1024 * 1024)


def cost(flops, size):
    return pl.CostEstimate(flops=flops, bytes_accessed=size, transcendentals=0)


def dot(a, b, dims=((1,), (0,))):
    return lax.dot_general(a, b, (dims, ((), ())), preferred_element_type=F32)


def parts_of(a):
    high = a.astype(BF16)
    return high, (a - high.astype(F32)).astype(BF16)


def dot3(a, b, dims=((1,), (0,))):
    ah, al = parts_of(a)
    bh, bl = parts_of(b)
    return dot(ah, bh, dims) + (dot(ah, bl, dims) + dot(al, bh, dims))


def dot2(a, b, dims=((1,), (0,))):
    ah, al = parts_of(a)
    return dot(ah, b, dims) + dot(al, b, dims)


def iota(shape, dim):
    return lax.broadcasted_iota(jnp.int32, shape, dim)


def by_head(a):
    left = iota(a.shape, 1) < HEAD_LIN
    first = jnp.sum(jnp.where(left, a, 0.0), axis=1, keepdims=True)
    second = jnp.sum(jnp.where(left, 0.0, a), axis=1, keepdims=True)
    return jnp.where(left, first, second)


def scaled_pieces(place_ref, own_ref, other_ref, gain_ref):
    shards, rows, depth = own_ref.shape
    core = place_ref[2]
    scaled, squares = [], jnp.zeros((rows, depth), F32)
    for c, ref in enumerate((own_ref, other_ref)):
        for j in range(shards):
            start = pl.multiple_of((2 * j + (core if c == 0 else 1 - core)) * depth, depth)
            wide = ref[j].astype(F32)
            scaled.append(((wide * gain_ref[:, pl.ds(start, depth)]).astype(BF16), start))
            squares = squares + wide * wide
    mean = jnp.sum(squares, axis=1, keepdims=True) / (2 * shards * depth)
    return scaled, lax.rsqrt(mean + 1e-6)


def projected(scaled, inverse, *w_refs):
    total = 0.0
    for piece, start in scaled:
        weight = [w_ref[pl.ds(start, piece.shape[1])] for w_ref in w_refs]
        total = total + dot(piece, jnp.concatenate(weight, axis=1))
    return total * inverse


def spread_kernel(place_ref, tokens_ref, out_ref):
    tokens = tokens_ref[...]
    for j in range(out_ref.shape[0]):
        out_ref[j] = tokens


def kv_kernel(place_ref, own_ref, other_ref, gain_ref, wk_ref, wv_ref, out_ref):
    scaled, inverse = scaled_pieces(place_ref, own_ref, other_ref, gain_ref)
    rows = own_ref.shape[1]
    both = projected(scaled, inverse, wk_ref, wv_ref).astype(BF16)
    out_ref[0:rows] = both[:, :HEAD_ATT]
    out_ref[rows:] = both[:, HEAD_ATT:]


def spans(log_decay):
    rows = log_decay.shape[0]
    row = iota(log_decay.shape, 0)
    zero = jnp.zeros_like(log_decay)
    before = [None] + [pltpu.roll(log_decay, i, 0) for i in range(1, 8)]
    behind = [None] + [pltpu.roll(log_decay, rows - i, 0) for i in range(1, 8)]
    ahead, after = {1: zero}, {1: zero}
    for h in (2, 4, 8):
        place = row & (h - 1)
        a, b = zero, zero
        for i in range(1, h):
            a = a + jnp.where(place >= i, before[i], 0.0)
            b = b + jnp.where(place + i < h, behind[i], 0.0)
        ahead[h], after[h] = a, b
    h = 8
    while h < rows:
        shape = (rows // (2 * h), 2 * h, WIDE)
        a, b = ahead[h].reshape(shape), after[h].reshape(shape)
        step = log_decay.reshape(shape)
        left = a[:, h - 1 : h] + step[:, h - 1 : h]
        right = b[:, h : h + 1] + step[:, h : h + 1]
        a = jnp.concatenate([a[:, :h], a[:, h:] + left], axis=1)
        b = jnp.concatenate([b[:, :h] + right, b[:, h:]], axis=1)
        h *= 2
        ahead[h], after[h] = a.reshape(rows, WIDE), b.reshape(rows, WIDE)
    return ahead, after


def lin_kernel(
    place_ref,
    own_ref,
    other_ref,
    gain_ref,
    wr_ref,
    wk_ref,
    wv_ref,
    wq_ref,
    down_ref,
    up_ref,
    bias_ref,
    shift_ref,
    rate_ref,
    gate_ref,
    send_ref,
    gates_ref,
    reach_ref,
    local_ref,
    pairs_ref,
):
    scaled, inverse = scaled_pieces(place_ref, own_ref, other_ref, gain_ref)
    rows = shift_ref.shape[0]
    both = projected(scaled, inverse, wr_ref, wk_ref).astype(BF16)
    recv, key = both[:, :WIDE].astype(F32), both[:, WIDE:].astype(F32)
    both = projected(scaled, inverse, wv_ref, wq_ref).astype(BF16)
    value = both[:, :WIDE]
    send_ref[0:rows] = both[:, WIDE:]
    low = 0.0
    for piece, start in scaled:
        low = low + dot(piece, down_ref[:, pl.ds(start, piece.shape[1])], ((1,), (1,)))
    low = (low * inverse).astype(BF16).astype(F32)
    exponent = bias_ref[...] + shift_ref[...] + dot(jnp.tanh(low).astype(BF16), up_ref[...])
    log_decay = -jnp.exp(exponent)
    unit = key * lax.rsqrt(by_head(key * key) + 1e-6)
    rate = unit * rate_ref[...]

    ahead, after = spans(log_decay)
    half = rows // 2
    lane = iota((rows, WIDE), 1)
    row = iota((rows, WIDE), 0)
    tall = iota((half, half), 0)
    flat = iota((half, half), 1)
    heads = [lane < HEAD_LIN, lane >= HEAD_LIN]
    eye = tall == flat
    blocks = slice(0, half), slice(half, rows)

    def of_heads(a):
        return [jnp.where(mine, a, 0.0).astype(BF16) for mine in heads]

    def below(h):
        level = h.bit_length()
        near = (tall >> level) == (flat >> level)
        return near & ((tall & h) != 0) & ((flat & h) == 0)

    for m, source in enumerate((key, rate)):
        now = by_head(recv * source)
        for n in range(2):
            for b in range(2):
                cols = slice(m * rows + b * half, m * rows + (b + 1) * half)
                same_row = now[blocks[b], n * HEAD_LIN : n * HEAD_LIN + 1]
                pairs_ref[n, 1, blocks[b], cols] = jnp.where(eye, same_row, 0.0)
                pairs_ref[n, 0, blocks[b], cols] = jnp.zeros((half, half), F32)
            cols = slice(m * rows + half, (m + 1) * rows)
            for k in range(2):
                pairs_ref[n, k, blocks[0], cols] = jnp.zeros((half, half), F32)
    h = 1
    while h < rows:
        late = (row & h) != 0
        to_u = jnp.where(late, jnp.exp(ahead[h]), 0.0)
        to_q = jnp.where(late, jnp.exp(ahead[h] + log_decay), 0.0)
        from_s = jnp.where(late, 0.0, jnp.exp(after[h]))
        right = (key * from_s).astype(BF16), (rate * from_s).astype(BF16)
        left = of_heads(unit * to_u) + of_heads(recv * to_q)
        for b in range(2) if h < half else (1,):
            c = b if h < half else 0
            product = dot(
                jnp.concatenate([a[blocks[b]] for a in left], axis=0),
                jnp.concatenate([a[blocks[c]] for a in right], axis=0),
                ((1,), (1,)),
            )
            for k in range(2):
                for n in range(2):
                    for m in range(2):
                        cols = slice(m * rows + c * half, m * rows + (c + 1) * half)
                        new = product[
                            (2 * k + n) * half : (2 * k + n + 1) * half,
                            m * half : (m + 1) * half,
                        ]
                        if h < half:
                            new = jnp.where(below(h), new, pairs_ref[n, k, blocks[b], cols])
                        pairs_ref[n, k, blocks[b], cols] = new
        h *= 2

    solved = {}
    h = 1
    while h < half:
        here = below(h)
        for n in range(2):
            for b in range(2):
                cols = slice(rows + b * half, rows + (b + 1) * half)
                links = jnp.where(here, pairs_ref[n, 0, blocks[b], cols], 0.0)
                if h == 1:
                    solved[n, b] = jnp.where(eye, 1.0, 0.0) - links
                else:
                    step = dot3(links, solved[n, b])
                    solved[n, b] = solved[n, b] - dot3(solved[n, b], step)
        h *= 2

    full_u = unit * jnp.exp(ahead[rows])
    full_q = recv * jnp.exp(ahead[rows] + log_decay)
    tail = jnp.exp(after[rows])
    full_k = key * tail
    full_r = rate * tail
    reach, local, moved = [], [], []
    for n in range(2):
        add = dot2(pairs_ref[n, 0, :, :rows], value)
        source = jnp.where(heads[n], full_u, pltpu.roll(add, HEAD_LIN, 1))
        first = dot3(solved[n, 0], source[:half])
        later = source[half:] - dot3(pairs_ref[n, 0, half:, rows : rows + half], first)
        along = jnp.concatenate([first, dot3(solved[n, 1], later)], axis=0)
        taken = dot3(pairs_ref[n, 1, :, rows:], along)
        reach.append(full_q - taken)
        local.append(dot2(pairs_ref[n, 1, :, :rows], value) - pltpu.roll(taken, HEAD_LIN, 1))
        moved.append(dot3(along, full_r, ((0,), (0,))))
    reach_ref[...] = jnp.where(heads[0], reach[0], reach[1])
    local_ref[...] = jnp.where(heads[0], local[0], local[1])

    lane = iota((WIDE, WIDE), 1)
    row = iota((WIDE, WIDE), 0)
    same = (lane < HEAD_LIN) == (row < HEAD_LIN)
    added = pltpu.roll(dot2(full_k, value, ((0,), (0,))).T, HEAD_LIN, 0)
    last = jnp.exp(ahead[rows][rows - 1 : rows] + log_decay[rows - 1 : rows]) - 1.0
    packed = jnp.where(same, jnp.where(lane == row, last, 0.0), added)
    packed = packed - jnp.where(lane < HEAD_LIN, moved[0], moved[1])
    send_ref[rows : rows + WIDE] = packed.astype(BF16)
    gate = gate_ref[...]
    high, mid = parts_of(gate)
    low_part = (gate - high.astype(F32) - mid.astype(F32)).astype(BF16)
    none = jnp.zeros((10, WIDE), BF16)
    gates = jnp.concatenate([high, mid, low_part, none], axis=0)
    send_ref[rows + WIDE :] = gates
    gates_ref[...] = gates


def unpacked(packed):
    packed = packed.astype(F32)
    lane = iota((WIDE, WIDE), 1)
    row = iota((WIDE, WIDE), 0)
    same = (lane < HEAD_LIN) == (row < HEAD_LIN)
    return jnp.where(same, packed, 0.0), jnp.where(same, pltpu.roll(packed, HEAD_LIN, 0), 0.0)


def row_kernel(place_ref, gathered_ref, gates_ref, send_ref, before_ref, *, rows):
    y = place_ref[1]
    count = gathered_ref.shape[0]
    shape = (WIDE, WIDE)
    total = jnp.zeros(shape, F32), jnp.zeros(shape, F32)
    mine = total
    for j in range(count):
        mine = tuple(jnp.where(y == j, t, m) for t, m in zip(total, mine))
        moved, added = unpacked(gathered_ref[j, rows : rows + WIDE])
        if j == 0:
            total = moved, added
        else:
            total = (
                total[0] + moved + dot3(total[0], moved),
                total[1] + added + dot3(total[1], moved),
            )
    before_ref[0] = mine[0]
    before_ref[1] = mine[1]
    lane = iota(shape, 1)
    row = iota(shape, 0)
    same = (lane < HEAD_LIN) == (row < HEAD_LIN)
    packed = jnp.where(same, total[0], pltpu.roll(total[1], HEAD_LIN, 0))
    send_ref[0:WIDE] = packed.astype(BF16)
    send_ref[WIDE:] = gates_ref[...]


def mix_kernel(place_ref, state_ref, gathered_ref, before_ref, reach_ref, local_ref, gain_ref, out_ref):
    z = place_ref[0]
    none = jnp.zeros((HEAD_LIN, HEAD_LIN), F32)
    state = jnp.concatenate(
        [
            jnp.concatenate([state_ref[0], none], axis=1),
            jnp.concatenate([none, state_ref[1]], axis=1),
        ],
        axis=0,
    )

    def step(k, state):
        packed = gathered_ref[k]
        moved, added = unpacked(packed[0:WIDE])
        return state + dot2(state, moved.astype(BF16)) + added

    state = lax.fori_loop(0, z, step, state)
    state = state + dot3(state, before_ref[0]) + before_ref[1]
    raw = dot3(reach_ref[...], state, ((1,), (1,))) + local_ref[...]
    off = raw - by_head(raw) * (1.0 / HEAD_LIN)
    spread = by_head(off * off) * (1.0 / HEAD_LIN)
    out_ref[...] = (off * lax.rsqrt(spread + 0.00064) * gain_ref[...]).astype(BF16)


def joined(gates):
    gates = gates.astype(F32)
    return gates[0:2] + gates[2:4] + gates[4:6]


def att_kernel(
    place_ref, asked_ref, held_ref, keys_ref, out_ref, logit_ref, best_ref, sum_ref, *, rows
):
    z, y = place_ref[0], place_ref[1]
    count = asked_ref.shape[0]
    scale = HEAD_ATT ** (-0.5) * LOG2E
    best_ref[...] = jnp.full(best_ref.shape, NEG, F32)
    sum_ref[...] = jnp.zeros(sum_ref.shape, F32)
    ones = jnp.ones((rows, HEAD_ATT), BF16)
    base = joined(asked_ref[0, rows + WIDE : rows + WIDE + 16])[0:1, 0:1]

    def score(k, masked):
        key = keys_ref[k, 0:rows]
        drop = (base - joined(held_ref[k, WIDE : WIDE + 16])) * LOG2E
        drop = jnp.concatenate([drop[0:1], drop[1:2]], axis=1)
        for j in range(count):
            logits = dot(asked_ref[j, 0:rows], key, ((1,), (1,))) * scale + drop
            if masked:
                allowed = y * rows + iota(logits.shape, 1) <= j * rows + iota(logits.shape, 0)
                logits = jnp.where(allowed, logits, NEG)
            logit_ref[k, j] = logits
            top = functools.reduce(
                jnp.maximum, [logits[:, i : i + WIDE] for i in range(0, rows, WIDE)]
            )
            best_ref[j] = jnp.maximum(best_ref[j], top)

    def gather(*blocks):
        value = [jnp.concatenate([keys_ref[k, rows:], ones], axis=1) for k in blocks]
        for j in range(count):
            best = jnp.concatenate([best_ref[j]] * (rows // WIDE), axis=1)
            new = 0.0
            for k, v in zip(blocks, value):
                new = new + dot(jnp.exp2(logit_ref[k, j] - best).astype(BF16), v)
            sum_ref[j] = sum_ref[j] + new

    def score_many(i, carry):
        for k in range(5):
            score(5 * i + k, False)
        return carry

    def score_one(k, carry):
        score(k, False)
        return carry

    def gather_many(i, carry):
        gather(*(8 * i + k for k in range(8)))
        return carry

    def gather_one(k, carry):
        gather(k)
        return carry

    many = z // 5
    lax.fori_loop(0, many, score_many, 0)
    lax.fori_loop(5 * many, z, score_one, 0)
    score(z, True)
    for j in range(count):
        best = jnp.max(best_ref[j], axis=1, keepdims=True)
        best = jnp.where(best > 0.5 * NEG, best, 0.0)
        best_ref[j] = jnp.broadcast_to(best, best_ref.shape[1:])
    many = (z + 1) // 8
    lax.fori_loop(0, many, gather_many, 0)
    lax.fori_loop(8 * many, z + 1, gather_one, 0)
    third = iota((rows, WIDE), 1)
    for j in range(count):
        total = sum_ref[j, :, HEAD_ATT:]
        some = total > 0.0
        safe = jnp.where(some, total, 1.0)
        out_ref[j, :, 0:HEAD_ATT] = (sum_ref[j, :, 0:HEAD_ATT] / safe).astype(BF16)
        level = jnp.where(some, best_ref[j] + jnp.log(safe) * LOG2E, NEG)
        high, mid = parts_of(level)
        high, mid = high.astype(F32), mid.astype(F32)
        last = level - high - mid
        level = jnp.where(third < 40, high, jnp.where(third < 80, mid, last))
        out_ref[j, :, HEAD_ATT:] = level.astype(BF16)


def out_kernel(place_ref, parts_ref, lin_ref, gain_ref, wl_ref, wa_ref, own_ref, other_ref):
    count, rows = parts_ref.shape[0], parts_ref.shape[1]
    core = place_ref[2]
    levels = []
    for j in range(count):
        level = parts_ref[j, :, HEAD_ATT:].astype(F32)
        levels.append(level[:, 0:1] + level[:, 40:41] + level[:, 80:81])
    top = functools.reduce(jnp.maximum, levels)
    total, raw = jnp.zeros((rows, 1), F32), jnp.zeros((rows, HEAD_ATT), F32)
    for j in range(count):
        share = jnp.exp2(levels[j] - top)
        total = total + share
        raw = raw + share * parts_ref[j, :, 0:HEAD_ATT].astype(F32)
    raw = raw / total
    size = jnp.mean(raw * raw, axis=1, keepdims=True)
    att = (raw * lax.rsqrt(size + 1e-6) * gain_ref[...]).astype(BF16)
    lin = lin_ref[...]
    width = own_ref.shape[2]
    for c, ref in enumerate((own_ref, other_ref)):
        for j in range(ref.shape[0]):
            start = pl.multiple_of((2 * j + (core if c == 0 else 1 - core)) * width, width)
            mine = pl.ds(start, width)
            ref[j] = (dot(lin, wl_ref[:, mine]) + dot(att, wa_ref[:, mine])).astype(BF16)


def sent_to_all(a, axis):
    size = lax.axis_size(axis)
    return lax.all_to_all(jnp.broadcast_to(a[None], (size, *a.shape)), axis, 0, 0, tiled=True)


def to_other_core(a):
    return lax.ppermute(a, "c", [(0, 1), (1, 0)])


def smem():
    return pl.BlockSpec(memory_space=pltpu.SMEM)


def vmem():
    return pl.BlockSpec(memory_space=pltpu.VMEM)


def call(kernel, name, shapes, flops, size, mib, scratch=()):
    def run(*operands):
        many = isinstance(shapes, (list, tuple))
        return pl.pallas_call(
            kernel,
            name=name,
            out_shape=shapes,
            in_specs=[smem()] + [vmem()] * (len(operands) - 1),
            out_specs=[vmem()] * len(shapes) if many else vmem(),
            scratch_shapes=list(scratch),
            compiler_params=params(mib),
            cost_estimate=cost(flops, size),
        )(*operands)

    return run


def body(
    tokens,
    norm_gain,
    recv_weight,
    lin_key_weight,
    lin_value_weight,
    decay_down,
    decay_up,
    decay_log_bias,
    decay_shift,
    learn_rate,
    group_gain,
    initial_state,
    query_weight,
    att_key_weight,
    att_value_weight,
    gate_cache,
    att_gain,
    out_lin_weight,
    out_att_weight,
):
    rows = tokens.shape[0]
    nz, ny, nx = (lax.axis_size(axis) for axis in ("z", "y", "x"))
    model_width = norm_gain.shape[0]
    shape = jax.ShapeDtypeStruct
    place = jnp.stack([lax.axis_index(axis) for axis in ("z", "y", "c")]).astype(jnp.int32)
    gain = norm_gain.reshape(1, -1)

    copies = call(spread_kernel, "spread", shape((nx, *tokens.shape), BF16), 10**10, 1 << 24, 4)(
        place, tokens
    )
    own = lax.all_to_all(copies, "x", 0, 0, tiled=True)
    other = to_other_core(own)
    kv = call(
        kv_kernel, "kv", shape((2 * rows, WIDE), BF16), 2 * rows * model_width * 256, 1 << 21, 12
    )(place, own, other, gain, att_key_weight, att_value_weight)
    keys = lax.all_gather(kv, "z")

    extra = 16
    send, gates, reach, local = call(
        lin_kernel,
        "lin",
        (
            shape((rows + WIDE + extra, WIDE), BF16),
            shape((extra, WIDE), BF16),
            shape((rows, WIDE), F32),
            shape((rows, WIDE), F32),
        ),
        4 * 10**9,
        1 << 22,
        24,
        scratch=[pltpu.VMEM((2, 2, rows, 2 * rows), F32)],
    )(
        place,
        own,
        other,
        gain,
        recv_weight,
        lin_key_weight,
        lin_value_weight,
        query_weight,
        decay_down.T,
        decay_up,
        decay_log_bias.reshape(1, -1),
        decay_shift,
        learn_rate.reshape(1, -1),
        gate_cache.reshape(rows // WIDE, WIDE),
    )
    asked = sent_to_all(send, "y")
    row_send, before = call(
        functools.partial(row_kernel, rows=rows),
        "row",
        (shape((WIDE + extra, WIDE), BF16), shape((2, WIDE, WIDE), F32)),
        10**8,
        1 << 20,
        12,
    )(place, asked, gates)
    held = lax.all_gather(row_send, "z")
    lin_mixed = call(mix_kernel, "mix", shape((rows, WIDE), BF16), 10**9, 1 << 20, 12)(
        place, initial_state, held, before, reach, local, group_gain.reshape(1, -1)
    )
    asked, lin_mixed = lax.optimization_barrier((asked, lin_mixed))
    found = call(
        functools.partial(att_kernel, rows=rows),
        "att",
        shape((ny, rows, HEAD_ATT + WIDE), BF16),
        ny * rows * nz * rows * 512,
        1 << 22,
        36,
        scratch=[
            pltpu.VMEM((nz, ny, rows, rows), F32),
            pltpu.VMEM((ny, rows, WIDE), F32),
            pltpu.VMEM((ny, rows, HEAD_ATT + WIDE), F32),
        ],
    )(place, asked, held, keys)
    parts = lax.all_to_all(found, "y", 0, 0, tiled=True)
    width = model_width // (2 * nx)
    tile = shape((nx, rows, width), BF16)
    mine, theirs = call(
        out_kernel, "out", (tile, tile), 2 * rows * 256 * model_width, 1 << 21, 12
    )(place, parts, lin_mixed, att_gain.reshape(1, -1), out_lin_weight, out_att_weight)
    pair = (mine.astype(F32) + to_other_core(theirs).astype(F32)).astype(BF16)
    tiles = lax.all_to_all(pair, "x", 0, 0, tiled=True)
    return jnp.sum(tiles.astype(F32), axis=0).astype(BF16)


def solution(mesh):
    sp, tp = mesh.shape["sp"], mesh.shape["tp"]
    cores = 2
    ny = math.isqrt(sp) // 2 if sp > 16 else 2
    torus = Mesh(mesh.devices.reshape(sp // ny, ny, tp // cores, cores), SP + TP)
    return jax.shard_map(
        body,
        mesh=torus,
        in_specs=(
            P(SP, TP),
            P(),
            P(None, TP),
            P(None, TP),
            P(None, TP),
            P(),
            P(None, TP),
            P(TP),
            P(SP, TP),
            P(TP),
            P(TP),
            P(TP, None, None),
            P(None, TP),
            P(None, TP),
            P(None, TP),
            P(SP, TP),
            P(TP),
            P(TP, None),
            P(TP, None),
        ),
        out_specs=P(SP, TP),
        check_vma=False,
    )
```

```python
import functools
import math

import jax
import jax.numpy as jnp
from jax import lax
from jax.experimental import pallas as pl
from jax.experimental.pallas import tpu as pltpu
from jax.sharding import Mesh
from jax.sharding import PartitionSpec as P

HEAD_LIN = 64
HEAD_ATT = 128
WIDE = 128
SP = ("z", "y")
TP = ("x", "c")
LOG2E = math.log2(math.e)
NEG = -1e30
F32 = jnp.float32
BF16 = jnp.bfloat16


def params(mib):
    return pltpu.CompilerParams(vmem_limit_bytes=mib * 1024 * 1024)


def cost(flops, size):
    return pl.CostEstimate(flops=flops, bytes_accessed=size, transcendentals=0)


def dot(a, b, dims=((1,), (0,))):
    return lax.dot_general(a, b, (dims, ((), ())), preferred_element_type=F32)


def parts_of(a):
    high = a.astype(BF16)
    return high, (a - high.astype(F32)).astype(BF16)


def dot3(a, b, dims=((1,), (0,))):
    ah, al = parts_of(a)
    bh, bl = parts_of(b)
    return dot(ah, bh, dims) + (dot(ah, bl, dims) + dot(al, bh, dims))


def dot2(a, b, dims=((1,), (0,))):
    ah, al = parts_of(a)
    return dot(ah, b, dims) + dot(al, b, dims)


def iota(shape, dim):
    return lax.broadcasted_iota(jnp.int32, shape, dim)


def by_head(a):
    left = iota(a.shape, 1) < HEAD_LIN
    first = jnp.sum(jnp.where(left, a, 0.0), axis=1, keepdims=True)
    second = jnp.sum(jnp.where(left, 0.0, a), axis=1, keepdims=True)
    return jnp.where(left, first, second)


def scaled_pieces(place_ref, own_ref, other_ref, gain_ref):
    shards, rows, depth = own_ref.shape
    core = place_ref[2]
    scaled, squares = [], jnp.zeros((rows, depth), F32)
    for c, ref in enumerate((own_ref, other_ref)):
        for j in range(shards):
            start = pl.multiple_of((2 * j + (core if c == 0 else 1 - core)) * depth, depth)
            wide = ref[j].astype(F32)
            scaled.append(((wide * gain_ref[:, pl.ds(start, depth)]).astype(BF16), start))
            squares = squares + wide * wide
    mean = jnp.sum(squares, axis=1, keepdims=True) / (2 * shards * depth)
    return scaled, lax.rsqrt(mean + 1e-6)


def projected(scaled, inverse, *w_refs):
    total = 0.0
    for piece, start in scaled:
        weight = [w_ref[pl.ds(start, piece.shape[1])] for w_ref in w_refs]
        total = total + dot(piece, jnp.concatenate(weight, axis=1))
    return total * inverse


def spread_kernel(place_ref, tokens_ref, out_ref):
    tokens = tokens_ref[...]
    for j in range(out_ref.shape[0]):
        out_ref[j] = tokens


def kv_kernel(place_ref, own_ref, other_ref, gain_ref, wk_ref, wv_ref, out_ref):
    scaled, inverse = scaled_pieces(place_ref, own_ref, other_ref, gain_ref)
    rows = own_ref.shape[1]
    both = projected(scaled, inverse, wk_ref, wv_ref).astype(BF16)
    out_ref[0:rows] = both[:, :HEAD_ATT]
    out_ref[rows:] = both[:, HEAD_ATT:]


def spans(log_decay):
    rows = log_decay.shape[0]
    row = iota(log_decay.shape, 0)
    zero = jnp.zeros_like(log_decay)
    before = [None] + [pltpu.roll(log_decay, i, 0) for i in range(1, 8)]
    behind = [None] + [pltpu.roll(log_decay, rows - i, 0) for i in range(1, 8)]
    ahead, after = {1: zero}, {1: zero}
    for h in (2, 4, 8):
        place = row & (h - 1)
        a, b = zero, zero
        for i in range(1, h):
            a = a + jnp.where(place >= i, before[i], 0.0)
            b = b + jnp.where(place + i < h, behind[i], 0.0)
        ahead[h], after[h] = a, b
    h = 8
    while h < rows:
        shape = (rows // (2 * h), 2 * h, WIDE)
        a, b = ahead[h].reshape(shape), after[h].reshape(shape)
        step = log_decay.reshape(shape)
        left = a[:, h - 1 : h] + step[:, h - 1 : h]
        right = b[:, h : h + 1] + step[:, h : h + 1]
        a = jnp.concatenate([a[:, :h], a[:, h:] + left], axis=1)
        b = jnp.concatenate([b[:, :h] + right, b[:, h:]], axis=1)
        h *= 2
        ahead[h], after[h] = a.reshape(rows, WIDE), b.reshape(rows, WIDE)
    return ahead, after


def lin_kernel(
    place_ref,
    own_ref,
    other_ref,
    gain_ref,
    wr_ref,
    wk_ref,
    wv_ref,
    wq_ref,
    down_ref,
    up_ref,
    bias_ref,
    shift_ref,
    rate_ref,
    gate_ref,
    send_ref,
    gates_ref,
    reach_ref,
    local_ref,
    pairs_ref,
):
    scaled, inverse = scaled_pieces(place_ref, own_ref, other_ref, gain_ref)
    rows = shift_ref.shape[0]
    both = projected(scaled, inverse, wr_ref, wk_ref).astype(BF16)
    recv, key = both[:, :WIDE].astype(F32), both[:, WIDE:].astype(F32)
    both = projected(scaled, inverse, wv_ref, wq_ref).astype(BF16)
    value = both[:, :WIDE]
    send_ref[0:rows] = both[:, WIDE:]
    low = 0.0
    for piece, start in scaled:
        low = low + dot(piece, down_ref[:, pl.ds(start, piece.shape[1])], ((1,), (1,)))
    low = (low * inverse).astype(BF16).astype(F32)
    exponent = bias_ref[...] + shift_ref[...] + dot(jnp.tanh(low).astype(BF16), up_ref[...])
    log_decay = -jnp.exp(exponent)
    unit = key * lax.rsqrt(by_head(key * key) + 1e-6)
    rate = unit * rate_ref[...]

    ahead, after = spans(log_decay)
    half = rows // 2
    lane = iota((rows, WIDE), 1)
    row = iota((rows, WIDE), 0)
    tall = iota((half, half), 0)
    flat = iota((half, half), 1)
    heads = [lane < HEAD_LIN, lane >= HEAD_LIN]
    eye = tall == flat
    blocks = slice(0, half), slice(half, rows)

    def of_heads(a):
        return [jnp.where(mine, a, 0.0).astype(BF16) for mine in heads]

    def below(h):
        level = h.bit_length()
        near = (tall >> level) == (flat >> level)
        return near & ((tall & h) != 0) & ((flat & h) == 0)

    for m, source in enumerate((key, rate)):
        now = by_head(recv * source)
        for n in range(2):
            for b in range(2):
                cols = slice(m * rows + b * half, m * rows + (b + 1) * half)
                same_row = now[blocks[b], n * HEAD_LIN : n * HEAD_LIN + 1]
                pairs_ref[n, 1, blocks[b], cols] = jnp.where(eye, same_row, 0.0)
                pairs_ref[n, 0, blocks[b], cols] = jnp.zeros((half, half), F32)
            cols = slice(m * rows + half, (m + 1) * rows)
            for k in range(2):
                pairs_ref[n, k, blocks[0], cols] = jnp.zeros((half, half), F32)
    h = 1
    while h < rows:
        late = (row & h) != 0
        to_u = jnp.where(late, jnp.exp(ahead[h]), 0.0)
        to_q = jnp.where(late, jnp.exp(ahead[h] + log_decay), 0.0)
        from_s = jnp.where(late, 0.0, jnp.exp(after[h]))
        right = (key * from_s).astype(BF16), (rate * from_s).astype(BF16)
        left = of_heads(unit * to_u) + of_heads(recv * to_q)
        for b in range(2) if h < half else (1,):
            c = b if h < half else 0
            product = dot(
                jnp.concatenate([a[blocks[b]] for a in left], axis=0),
                jnp.concatenate([a[blocks[c]] for a in right], axis=0),
                ((1,), (1,)),
            )
            for k in range(2):
                for n in range(2):
                    for m in range(2):
                        cols = slice(m * rows + c * half, m * rows + (c + 1) * half)
                        new = product[
                            (2 * k + n) * half : (2 * k + n + 1) * half,
                            m * half : (m + 1) * half,
                        ]
                        if h < half:
                            new = jnp.where(below(h), new, pairs_ref[n, k, blocks[b], cols])
                        pairs_ref[n, k, blocks[b], cols] = new
        h *= 2

    solved = {}
    h = 1
    while h < half:
        here = below(h)
        for n in range(2):
            for b in range(2):
                cols = slice(rows + b * half, rows + (b + 1) * half)
                links = jnp.where(here, pairs_ref[n, 0, blocks[b], cols], 0.0)
                if h == 1:
                    solved[n, b] = jnp.where(eye, 1.0, 0.0) - links
                else:
                    step = dot3(links, solved[n, b])
                    solved[n, b] = solved[n, b] - dot3(solved[n, b], step)
        h *= 2

    full_u = unit * jnp.exp(ahead[rows])
    full_q = recv * jnp.exp(ahead[rows] + log_decay)
    tail = jnp.exp(after[rows])
    full_k = key * tail
    full_r = rate * tail
    reach, local, moved = [], [], []
    for n in range(2):
        add = dot2(pairs_ref[n, 0, :, :rows], value)
        source = jnp.where(heads[n], full_u, pltpu.roll(add, HEAD_LIN, 1))
        first = dot3(solved[n, 0], source[:half])
        later = source[half:] - dot3(pairs_ref[n, 0, half:, rows : rows + half], first)
        along = jnp.concatenate([first, dot3(solved[n, 1], later)], axis=0)
        taken = dot3(pairs_ref[n, 1, :, rows:], along)
        reach.append(full_q - taken)
        local.append(dot2(pairs_ref[n, 1, :, :rows], value) - pltpu.roll(taken, HEAD_LIN, 1))
        moved.append(dot3(along, full_r, ((0,), (0,))))
    reach_ref[...] = jnp.where(heads[0], reach[0], reach[1])
    local_ref[...] = jnp.where(heads[0], local[0], local[1])

    lane = iota((WIDE, WIDE), 1)
    row = iota((WIDE, WIDE), 0)
    same = (lane < HEAD_LIN) == (row < HEAD_LIN)
    added = pltpu.roll(dot2(full_k, value, ((0,), (0,))).T, HEAD_LIN, 0)
    last = jnp.exp(ahead[rows][rows - 1 : rows] + log_decay[rows - 1 : rows]) - 1.0
    packed = jnp.where(same, jnp.where(lane == row, last, 0.0), added)
    packed = packed - jnp.where(lane < HEAD_LIN, moved[0], moved[1])
    send_ref[rows : rows + WIDE] = packed.astype(BF16)
    gate = gate_ref[...]
    high, mid = parts_of(gate)
    low_part = (gate - high.astype(F32) - mid.astype(F32)).astype(BF16)
    none = jnp.zeros((10, WIDE), BF16)
    gates = jnp.concatenate([high, mid, low_part, none], axis=0)
    send_ref[rows + WIDE :] = gates
    gates_ref[...] = gates


def unpacked(packed):
    packed = packed.astype(F32)
    lane = iota((WIDE, WIDE), 1)
    row = iota((WIDE, WIDE), 0)
    same = (lane < HEAD_LIN) == (row < HEAD_LIN)
    return jnp.where(same, packed, 0.0), jnp.where(same, pltpu.roll(packed, HEAD_LIN, 0), 0.0)


def row_kernel(place_ref, gathered_ref, gates_ref, send_ref, before_ref, *, rows):
    y = place_ref[1]
    count = gathered_ref.shape[0]
    shape = (WIDE, WIDE)
    total = jnp.zeros(shape, F32), jnp.zeros(shape, F32)
    mine = total
    for j in range(count):
        mine = tuple(jnp.where(y == j, t, m) for t, m in zip(total, mine))
        moved, added = unpacked(gathered_ref[j, rows : rows + WIDE])
        if j == 0:
            total = moved, added
        else:
            total = (
                total[0] + moved + dot3(total[0], moved),
                total[1] + added + dot3(total[1], moved),
            )
    before_ref[0] = mine[0]
    before_ref[1] = mine[1]
    lane = iota(shape, 1)
    row = iota(shape, 0)
    same = (lane < HEAD_LIN) == (row < HEAD_LIN)
    packed = jnp.where(same, total[0], pltpu.roll(total[1], HEAD_LIN, 0))
    send_ref[0:WIDE] = packed.astype(BF16)
    send_ref[WIDE:] = gates_ref[...]


def mix_kernel(place_ref, state_ref, gathered_ref, before_ref, reach_ref, local_ref, gain_ref, out_ref):
    z = place_ref[0]
    none = jnp.zeros((HEAD_LIN, HEAD_LIN), F32)
    state = jnp.concatenate(
        [
            jnp.concatenate([state_ref[0], none], axis=1),
            jnp.concatenate([none, state_ref[1]], axis=1),
        ],
        axis=0,
    )

    def step(k, state):
        packed = gathered_ref[k]
        moved, added = unpacked(packed[0:WIDE])
        return state + dot2(state, moved.astype(BF16)) + added

    state = lax.fori_loop(0, z, step, state)
    state = state + dot3(state, before_ref[0]) + before_ref[1]
    raw = dot3(reach_ref[...], state, ((1,), (1,))) + local_ref[...]
    off = raw - by_head(raw) * (1.0 / HEAD_LIN)
    spread = by_head(off * off) * (1.0 / HEAD_LIN)
    out_ref[...] = (off * lax.rsqrt(spread + 0.00064) * gain_ref[...]).astype(BF16)


def joined(gates):
    gates = gates.astype(F32)
    return gates[0:2] + gates[2:4] + gates[4:6]


def att_kernel(
    place_ref, asked_ref, held_ref, keys_ref, out_ref, logit_ref, best_ref, sum_ref, *, rows
):
    z, y = place_ref[0], place_ref[1]
    count = asked_ref.shape[0]
    scale = HEAD_ATT ** (-0.5) * LOG2E
    best_ref[...] = jnp.full(best_ref.shape, NEG, F32)
    sum_ref[...] = jnp.zeros(sum_ref.shape, F32)
    ones = jnp.ones((rows, HEAD_ATT), BF16)
    base = joined(asked_ref[0, rows + WIDE : rows + WIDE + 16])[0:1, 0:1]

    def score(k, masked):
        key = keys_ref[k, 0:rows]
        drop = (base - joined(held_ref[k, WIDE : WIDE + 16])) * LOG2E
        drop = jnp.concatenate([drop[0:1], drop[1:2]], axis=1)
        for j in range(count):
            logits = dot(asked_ref[j, 0:rows], key, ((1,), (1,))) * scale + drop
            if masked:
                allowed = y * rows + iota(logits.shape, 1) <= j * rows + iota(logits.shape, 0)
                logits = jnp.where(allowed, logits, NEG)
            logit_ref[k, j] = logits
            top = functools.reduce(
                jnp.maximum, [logits[:, i : i + WIDE] for i in range(0, rows, WIDE)]
            )
            best_ref[j] = jnp.maximum(best_ref[j], top)

    def gather(*blocks):
        value = [jnp.concatenate([keys_ref[k, rows:], ones], axis=1) for k in blocks]
        for j in range(count):
            best = jnp.concatenate([best_ref[j]] * (rows // WIDE), axis=1)
            new = 0.0
            for k, v in zip(blocks, value):
                new = new + dot(jnp.exp2(logit_ref[k, j] - best).astype(BF16), v)
            sum_ref[j] = sum_ref[j] + new

    def score_many(i, carry):
        for k in range(3):
            score(3 * i + k, False)
        return carry

    def score_one(k, carry):
        score(k, False)
        return carry

    def gather_many(i, carry):
        gather(*(4 * i + k for k in range(4)))
        return carry

    def gather_one(k, carry):
        gather(k)
        return carry

    many = z // 3
    lax.fori_loop(0, many, score_many, 0)
    lax.fori_loop(3 * many, z, score_one, 0)
    score(z, True)
    for j in range(count):
        best = jnp.max(best_ref[j], axis=1, keepdims=True)
        best = jnp.where(best > 0.5 * NEG, best, 0.0)
        best_ref[j] = jnp.broadcast_to(best, best_ref.shape[1:])
    many = (z + 1) // 4
    lax.fori_loop(0, many, gather_many, 0)
    lax.fori_loop(4 * many, z + 1, gather_one, 0)
    third = iota((rows, WIDE), 1)
    for j in range(count):
        total = sum_ref[j, :, HEAD_ATT:]
        some = total > 0.0
        safe = jnp.where(some, total, 1.0)
        out_ref[j, :, 0:HEAD_ATT] = (sum_ref[j, :, 0:HEAD_ATT] / safe).astype(BF16)
        level = jnp.where(some, best_ref[j] + jnp.log(safe) * LOG2E, NEG)
        high, mid = parts_of(level)
        high, mid = high.astype(F32), mid.astype(F32)
        last = level - high - mid
        level = jnp.where(third < 40, high, jnp.where(third < 80, mid, last))
        out_ref[j, :, HEAD_ATT:] = level.astype(BF16)


def out_kernel(place_ref, parts_ref, lin_ref, gain_ref, wl_ref, wa_ref, own_ref, other_ref):
    count, rows = parts_ref.shape[0], parts_ref.shape[1]
    core = place_ref[2]
    levels = []
    for j in range(count):
        level = parts_ref[j, :, HEAD_ATT:].astype(F32)
        levels.append(level[:, 0:1] + level[:, 40:41] + level[:, 80:81])
    top = functools.reduce(jnp.maximum, levels)
    total, raw = jnp.zeros((rows, 1), F32), jnp.zeros((rows, HEAD_ATT), F32)
    for j in range(count):
        share = jnp.exp2(levels[j] - top)
        total = total + share
        raw = raw + share * parts_ref[j, :, 0:HEAD_ATT].astype(F32)
    raw = raw / total
    size = jnp.mean(raw * raw, axis=1, keepdims=True)
    att = (raw * lax.rsqrt(size + 1e-6) * gain_ref[...]).astype(BF16)
    lin = lin_ref[...]
    width = own_ref.shape[2]
    for c, ref in enumerate((own_ref, other_ref)):
        for j in range(ref.shape[0]):
            start = pl.multiple_of((2 * j + (core if c == 0 else 1 - core)) * width, width)
            mine = pl.ds(start, width)
            ref[j] = (dot(lin, wl_ref[:, mine]) + dot(att, wa_ref[:, mine])).astype(BF16)


def sent_to_all(a, axis):
    size = lax.axis_size(axis)
    return lax.all_to_all(jnp.broadcast_to(a[None], (size, *a.shape)), axis, 0, 0, tiled=True)


def to_other_core(a):
    return lax.ppermute(a, "c", [(0, 1), (1, 0)])


def smem():
    return pl.BlockSpec(memory_space=pltpu.SMEM)


def vmem():
    return pl.BlockSpec(memory_space=pltpu.VMEM)


def call(kernel, name, shapes, flops, size, mib, scratch=()):
    def run(*operands):
        many = isinstance(shapes, (list, tuple))
        return pl.pallas_call(
            kernel,
            name=name,
            out_shape=shapes,
            in_specs=[smem()] + [vmem()] * (len(operands) - 1),
            out_specs=[vmem()] * len(shapes) if many else vmem(),
            scratch_shapes=list(scratch),
            compiler_params=params(mib),
            cost_estimate=cost(flops, size),
        )(*operands)

    return run


def body(
    tokens,
    norm_gain,
    recv_weight,
    lin_key_weight,
    lin_value_weight,
    decay_down,
    decay_up,
    decay_log_bias,
    decay_shift,
    learn_rate,
    group_gain,
    initial_state,
    query_weight,
    att_key_weight,
    att_value_weight,
    gate_cache,
    att_gain,
    out_lin_weight,
    out_att_weight,
):
    rows = tokens.shape[0]
    nz, ny, nx = (lax.axis_size(axis) for axis in ("z", "y", "x"))
    model_width = norm_gain.shape[0]
    shape = jax.ShapeDtypeStruct
    place = jnp.stack([lax.axis_index(axis) for axis in ("z", "y", "c")]).astype(jnp.int32)
    gain = norm_gain.reshape(1, -1)

    copies = call(spread_kernel, "spread", shape((nx, *tokens.shape), BF16), 10**10, 1 << 24, 4)(
        place, tokens
    )
    own = lax.all_to_all(copies, "x", 0, 0, tiled=True)
    other = to_other_core(own)
    kv = call(
        kv_kernel, "kv", shape((2 * rows, WIDE), BF16), 2 * rows * model_width * 256, 1 << 21, 12
    )(place, own, other, gain, att_key_weight, att_value_weight)
    keys = lax.all_gather(kv, "z")

    extra = 16
    send, gates, reach, local = call(
        lin_kernel,
        "lin",
        (
            shape((rows + WIDE + extra, WIDE), BF16),
            shape((extra, WIDE), BF16),
            shape((rows, WIDE), F32),
            shape((rows, WIDE), F32),
        ),
        4 * 10**9,
        1 << 22,
        24,
        scratch=[pltpu.VMEM((2, 2, rows, 2 * rows), F32)],
    )(
        place,
        own,
        other,
        gain,
        recv_weight,
        lin_key_weight,
        lin_value_weight,
        query_weight,
        decay_down.T,
        decay_up,
        decay_log_bias.reshape(1, -1),
        decay_shift,
        learn_rate.reshape(1, -1),
        gate_cache.reshape(rows // WIDE, WIDE),
    )
    asked = sent_to_all(send, "y")
    row_send, before = call(
        functools.partial(row_kernel, rows=rows),
        "row",
        (shape((WIDE + extra, WIDE), BF16), shape((2, WIDE, WIDE), F32)),
        10**8,
        1 << 20,
        12,
    )(place, asked, gates)
    held = lax.all_gather(row_send, "z")
    lin_mixed = call(mix_kernel, "mix", shape((rows, WIDE), BF16), 10**9, 1 << 20, 12)(
        place, initial_state, held, before, reach, local, group_gain.reshape(1, -1)
    )
    asked, lin_mixed = lax.optimization_barrier((asked, lin_mixed))
    found = call(
        functools.partial(att_kernel, rows=rows),
        "att",
        shape((ny, rows, HEAD_ATT + WIDE), BF16),
        ny * rows * nz * rows * 512,
        1 << 22,
        36,
        scratch=[
            pltpu.VMEM((nz, ny, rows, rows), F32),
            pltpu.VMEM((ny, rows, WIDE), F32),
            pltpu.VMEM((ny, rows, HEAD_ATT + WIDE), F32),
        ],
    )(place, asked, held, keys)
    parts = lax.all_to_all(found, "y", 0, 0, tiled=True)
    width = model_width // (2 * nx)
    tile = shape((nx, rows, width), BF16)
    mine, theirs = call(
        out_kernel, "out", (tile, tile), 2 * rows * 256 * model_width, 1 << 21, 12
    )(place, parts, lin_mixed, att_gain.reshape(1, -1), out_lin_weight, out_att_weight)
    pair = (mine.astype(F32) + to_other_core(theirs).astype(F32)).astype(BF16)
    tiles = lax.all_to_all(pair, "x", 0, 0, tiled=True)
    return jnp.sum(tiles.astype(F32), axis=0).astype(BF16)


def solution(mesh):
    sp, tp = mesh.shape["sp"], mesh.shape["tp"]
    cores = 2
    ny = math.isqrt(sp) if sp > 16 else 4
    torus = Mesh(mesh.devices.reshape(sp // ny, ny, tp // cores, cores), SP + TP)
    return jax.shard_map(
        body,
        mesh=torus,
        in_specs=(
            P(SP, TP),
            P(),
            P(None, TP),
            P(None, TP),
            P(None, TP),
            P(),
            P(None, TP),
            P(TP),
            P(SP, TP),
            P(TP),
            P(TP),
            P(TP, None, None),
            P(None, TP),
            P(None, TP),
            P(None, TP),
            P(SP, TP),
            P(TP),
            P(TP, None),
            P(TP, None),
        ),
        out_specs=P(SP, TP),
        check_vma=False,
    )
```

```python
import functools
import math

import jax
import jax.numpy as jnp
from jax import lax
from jax.experimental import pallas as pl
from jax.experimental.pallas import tpu as pltpu
from jax.sharding import Mesh
from jax.sharding import PartitionSpec as P

HEAD_LIN = 64
HEAD_ATT = 128
WIDE = 128
KEYS = ("zh", "zl")
SP = KEYS + ("near",)
TP = ("x", "c")
LOG2E = math.log2(math.e)
NEG = -1e30
F32 = jnp.float32
BF16 = jnp.bfloat16


def params(mib):
    return pltpu.CompilerParams(vmem_limit_bytes=mib * 1024 * 1024)


def cost(flops, size):
    return pl.CostEstimate(flops=flops, bytes_accessed=size, transcendentals=0)


def dot(a, b, dims=((1,), (0,))):
    return lax.dot_general(a, b, (dims, ((), ())), preferred_element_type=F32)


def parts_of(a):
    high = a.astype(BF16)
    return high, (a - high.astype(F32)).astype(BF16)


def dot3(a, b, dims=((1,), (0,))):
    ah, al = parts_of(a)
    bh, bl = parts_of(b)
    return dot(ah, bh, dims) + (dot(ah, bl, dims) + dot(al, bh, dims))


def dot2(a, b, dims=((1,), (0,))):
    ah, al = parts_of(a)
    return dot(ah, b, dims) + dot(al, b, dims)


def in_thirds(a):
    high, mid = parts_of(a)
    low = (a - high.astype(F32) - mid.astype(F32)).astype(BF16)
    return jnp.concatenate([high, mid, low, jnp.zeros((10, WIDE), BF16)], axis=0)


def iota(shape, dim):
    return lax.broadcasted_iota(jnp.int32, shape, dim)


def by_head(a):
    left = iota(a.shape, 1) < HEAD_LIN
    first = jnp.sum(jnp.where(left, a, 0.0), axis=1, keepdims=True)
    second = jnp.sum(jnp.where(left, 0.0, a), axis=1, keepdims=True)
    return jnp.where(left, first, second)


def scaled_pieces(place_ref, own_ref, other_ref, gain_ref):
    shards, rows, depth = own_ref.shape
    core = place_ref[3]
    scaled, squares = [], jnp.zeros((rows, depth), F32)
    for c, ref in enumerate((own_ref, other_ref)):
        for j in range(shards):
            start = pl.multiple_of((2 * j + (core if c == 0 else 1 - core)) * depth, depth)
            wide = ref[j].astype(F32)
            scaled.append(((wide * gain_ref[:, pl.ds(start, depth)]).astype(BF16), start))
            squares = squares + wide * wide
    mean = jnp.sum(squares, axis=1, keepdims=True) / (2 * shards * depth)
    return scaled, lax.rsqrt(mean + 1e-6)


def projected(scaled, inverse, *w_refs):
    total = 0.0
    for piece, start in scaled:
        weight = [w_ref[pl.ds(start, piece.shape[1])] for w_ref in w_refs]
        total = total + dot(piece, jnp.concatenate(weight, axis=1))
    return total * inverse


def spread_kernel(place_ref, tokens_ref, out_ref):
    tokens = tokens_ref[...]
    for j in range(out_ref.shape[0]):
        out_ref[j] = tokens


def kv_kernel(place_ref, own_ref, other_ref, gain_ref, wk_ref, wv_ref, out_ref):
    scaled, inverse = scaled_pieces(place_ref, own_ref, other_ref, gain_ref)
    rows = own_ref.shape[1]
    both = projected(scaled, inverse, wk_ref, wv_ref).astype(BF16)
    out_ref[0:rows] = both[:, :HEAD_ATT]
    out_ref[rows:] = both[:, HEAD_ATT:]


def spans(log_decay):
    rows = log_decay.shape[0]
    row = iota(log_decay.shape, 0)
    zero = jnp.zeros_like(log_decay)
    before = [None] + [pltpu.roll(log_decay, i, 0) for i in range(1, 8)]
    behind = [None] + [pltpu.roll(log_decay, rows - i, 0) for i in range(1, 8)]
    ahead, after = {1: zero}, {1: zero}
    for h in (2, 4, 8):
        place = row & (h - 1)
        a, b = zero, zero
        for i in range(1, h):
            a = a + jnp.where(place >= i, before[i], 0.0)
            b = b + jnp.where(place + i < h, behind[i], 0.0)
        ahead[h], after[h] = a, b
    h = 8
    while h < rows:
        shape = (rows // (2 * h), 2 * h, WIDE)
        a, b = ahead[h].reshape(shape), after[h].reshape(shape)
        step = log_decay.reshape(shape)
        left = a[:, h - 1 : h] + step[:, h - 1 : h]
        right = b[:, h : h + 1] + step[:, h : h + 1]
        a = jnp.concatenate([a[:, :h], a[:, h:] + left], axis=1)
        b = jnp.concatenate([b[:, :h] + right, b[:, h:]], axis=1)
        h *= 2
        ahead[h], after[h] = a.reshape(rows, WIDE), b.reshape(rows, WIDE)
    return ahead, after


def lin_kernel(
    place_ref,
    own_ref,
    other_ref,
    gain_ref,
    wr_ref,
    wk_ref,
    wv_ref,
    wq_ref,
    down_ref,
    up_ref,
    bias_ref,
    shift_ref,
    rate_ref,
    gate_ref,
    send_ref,
    gates_ref,
    reach_ref,
    local_ref,
    pairs_ref,
):
    scaled, inverse = scaled_pieces(place_ref, own_ref, other_ref, gain_ref)
    rows = shift_ref.shape[0]
    both = projected(scaled, inverse, wr_ref, wk_ref).astype(BF16)
    recv, key = both[:, :WIDE].astype(F32), both[:, WIDE:].astype(F32)
    both = projected(scaled, inverse, wv_ref, wq_ref).astype(BF16)
    value = both[:, :WIDE]
    send_ref[0, 0:rows] = both[:, WIDE:]
    low = 0.0
    for piece, start in scaled:
        low = low + dot(piece, down_ref[:, pl.ds(start, piece.shape[1])], ((1,), (1,)))
    low = (low * inverse).astype(BF16).astype(F32)
    exponent = bias_ref[...] + shift_ref[...] + dot(jnp.tanh(low).astype(BF16), up_ref[...])
    log_decay = -jnp.exp(exponent)
    unit = key * lax.rsqrt(by_head(key * key) + 1e-6)
    rate = unit * rate_ref[...]

    ahead, after = spans(log_decay)
    half = rows // 2
    lane = iota((rows, WIDE), 1)
    row = iota((rows, WIDE), 0)
    tall = iota((half, half), 0)
    flat = iota((half, half), 1)
    heads = [lane < HEAD_LIN, lane >= HEAD_LIN]
    eye = tall == flat
    blocks = slice(0, half), slice(half, rows)

    def of_heads(a):
        return [jnp.where(mine, a, 0.0).astype(BF16) for mine in heads]

    def below(h):
        level = h.bit_length()
        near = (tall >> level) == (flat >> level)
        return near & ((tall & h) != 0) & ((flat & h) == 0)

    for m, source in enumerate((key, rate)):
        now = by_head(recv * source)
        for n in range(2):
            for b in range(2):
                cols = slice(m * rows + b * half, m * rows + (b + 1) * half)
                same_row = now[blocks[b], n * HEAD_LIN : n * HEAD_LIN + 1]
                pairs_ref[n, 1, blocks[b], cols] = jnp.where(eye, same_row, 0.0)
                pairs_ref[n, 0, blocks[b], cols] = jnp.zeros((half, half), F32)
            cols = slice(m * rows + half, (m + 1) * rows)
            for k in range(2):
                pairs_ref[n, k, blocks[0], cols] = jnp.zeros((half, half), F32)
    h = 1
    while h < rows:
        late = (row & h) != 0
        to_u = jnp.where(late, jnp.exp(ahead[h]), 0.0)
        to_q = jnp.where(late, jnp.exp(ahead[h] + log_decay), 0.0)
        from_s = jnp.where(late, 0.0, jnp.exp(after[h]))
        right = (key * from_s).astype(BF16), (rate * from_s).astype(BF16)
        left = of_heads(unit * to_u) + of_heads(recv * to_q)
        for b in range(2) if h < half else (1,):
            c = b if h < half else 0
            product = dot(
                jnp.concatenate([a[blocks[b]] for a in left], axis=0),
                jnp.concatenate([a[blocks[c]] for a in right], axis=0),
                ((1,), (1,)),
            )
            for k in range(2):
                for n in range(2):
                    for m in range(2):
                        cols = slice(m * rows + c * half, m * rows + (c + 1) * half)
                        new = product[
                            (2 * k + n) * half : (2 * k + n + 1) * half,
                            m * half : (m + 1) * half,
                        ]
                        if h < half:
                            new = jnp.where(below(h), new, pairs_ref[n, k, blocks[b], cols])
                        pairs_ref[n, k, blocks[b], cols] = new
        h *= 2

    solved = {}
    h = 1
    while h < half:
        here = below(h)
        for n in range(2):
            for b in range(2):
                cols = slice(rows + b * half, rows + (b + 1) * half)
                links = jnp.where(here, pairs_ref[n, 0, blocks[b], cols], 0.0)
                if h == 1:
                    solved[n, b] = jnp.where(eye, 1.0, 0.0) - links
                else:
                    step = dot3(links, solved[n, b])
                    solved[n, b] = solved[n, b] - dot3(solved[n, b], step)
        h *= 2

    full_u = unit * jnp.exp(ahead[rows])
    full_q = recv * jnp.exp(ahead[rows] + log_decay)
    tail = jnp.exp(after[rows])
    full_k = key * tail
    full_r = rate * tail
    reach, local, moved = [], [], []
    for n in range(2):
        add = dot2(pairs_ref[n, 0, :, :rows], value)
        source = jnp.where(heads[n], full_u, pltpu.roll(add, HEAD_LIN, 1))
        first = dot3(solved[n, 0], source[:half])
        later = source[half:] - dot3(pairs_ref[n, 0, half:, rows : rows + half], first)
        along = jnp.concatenate([first, dot3(solved[n, 1], later)], axis=0)
        taken = dot3(pairs_ref[n, 1, :, rows:], along)
        reach.append(full_q - taken)
        local.append(dot2(pairs_ref[n, 1, :, :rows], value) - pltpu.roll(taken, HEAD_LIN, 1))
        moved.append(dot3(along, full_r, ((0,), (0,))))
    reach_ref[...] = jnp.where(heads[0], reach[0], reach[1])
    local_ref[...] = jnp.where(heads[0], local[0], local[1])

    lane = iota((WIDE, WIDE), 1)
    row = iota((WIDE, WIDE), 0)
    same = (lane < HEAD_LIN) == (row < HEAD_LIN)
    added = pltpu.roll(dot2(full_k, value, ((0,), (0,))).T, HEAD_LIN, 0)
    last = jnp.exp(ahead[rows][rows - 1 : rows] + log_decay[rows - 1 : rows]) - 1.0
    packed = jnp.where(same, jnp.where(lane == row, last, 0.0), added)
    packed = packed - jnp.where(lane < HEAD_LIN, moved[0], moved[1])
    send_ref[0, rows : rows + WIDE] = packed.astype(BF16)
    gates = in_thirds(gate_ref[...])
    send_ref[0, rows + WIDE :] = gates
    gates_ref[...] = gates
    whole = send_ref[0]
    for j in range(1, send_ref.shape[0]):
        send_ref[j] = whole


def unpacked(packed):
    packed = packed.astype(F32)
    lane = iota((WIDE, WIDE), 1)
    row = iota((WIDE, WIDE), 0)
    same = (lane < HEAD_LIN) == (row < HEAD_LIN)
    return jnp.where(same, packed, 0.0), jnp.where(same, pltpu.roll(packed, HEAD_LIN, 0), 0.0)


def repacked(total):
    lane = iota((WIDE, WIDE), 1)
    row = iota((WIDE, WIDE), 0)
    same = (lane < HEAD_LIN) == (row < HEAD_LIN)
    return jnp.where(same, total[0], pltpu.roll(total[1], HEAD_LIN, 0)).astype(BF16)


def chained(first, second):
    return (
        first[0] + second[0] + dot3(first[0], second[0]),
        first[1] + second[1] + dot3(first[1], second[0]),
    )


def row_kernel(place_ref, gathered_ref, gates_ref, send_ref, before_ref, *, rows):
    near = place_ref[2]
    count = gathered_ref.shape[0]
    total = mine = jnp.zeros((WIDE, WIDE), F32), jnp.zeros((WIDE, WIDE), F32)
    for j in range(count):
        mine = tuple(jnp.where(near == j, t, m) for t, m in zip(total, mine))
        here = unpacked(gathered_ref[j, rows : rows + WIDE])
        total = chained(total, here) if j else here
    before_ref[0], before_ref[1] = mine
    send_ref[0:WIDE] = repacked(total)
    send_ref[WIDE:] = gates_ref[...]


def pair_kernel(place_ref, own_ref, other_ref, before_ref, send_ref, after_ref):
    late = place_ref[1] == 1
    own, other = unpacked(own_ref[0:WIDE]), unpacked(other_ref[0:WIDE])
    first = tuple(jnp.where(late, o, m) for m, o in zip(own, other))
    second = tuple(jnp.where(late, m, o) for m, o in zip(own, other))
    send_ref[0:WIDE] = repacked(chained(first, second))
    own_gate, other_gate = own_ref[WIDE:].astype(F32), other_ref[WIDE:].astype(F32)
    send_ref[WIDE : WIDE + 16] = jnp.where(late, other_gate, own_gate).astype(BF16)
    send_ref[WIDE + 16 :] = jnp.where(late, own_gate, other_gate).astype(BF16)
    before = before_ref[0], before_ref[1]
    moved = chained(other, before)
    after_ref[0], after_ref[1] = (jnp.where(late, m, b) for m, b in zip(moved, before))


def mix_kernel(place_ref, state_ref, gathered_ref, before_ref, reach_ref, local_ref, gain_ref, out_ref):
    none = jnp.zeros((HEAD_LIN, HEAD_LIN), F32)
    state = jnp.concatenate(
        [
            jnp.concatenate([state_ref[0], none], axis=1),
            jnp.concatenate([none, state_ref[1]], axis=1),
        ],
        axis=0,
    )

    def step(k, state):
        packed = gathered_ref[k]
        moved, added = unpacked(packed[0:WIDE])
        return state + dot2(state, moved.astype(BF16)) + added

    state = lax.fori_loop(0, place_ref[0], step, state)
    state = state + dot3(state, before_ref[0]) + before_ref[1]
    raw = dot3(reach_ref[...], state, ((1,), (1,))) + local_ref[...]
    off = raw - by_head(raw) * (1.0 / HEAD_LIN)
    spread = by_head(off * off) * (1.0 / HEAD_LIN)
    out_ref[...] = (off * lax.rsqrt(spread + 0.00064) * gain_ref[...]).astype(BF16)


def joined(gates):
    gates = gates.astype(F32)
    return gates[0:2] + gates[2:4] + gates[4:6]


def att_kernel(
    place_ref, asked_ref, held_ref, keys_ref, out_ref, logit_ref, best_ref, sum_ref, *, rows
):
    z, y = place_ref[0] * 2 + place_ref[1], place_ref[2]
    count = asked_ref.shape[0]
    scale = HEAD_ATT ** (-0.5) * LOG2E
    best_ref[...] = jnp.full(best_ref.shape, NEG, F32)
    sum_ref[...] = jnp.zeros(sum_ref.shape, F32)
    ones = jnp.ones((rows, HEAD_ATT), BF16)
    base = joined(asked_ref[0, rows + WIDE : rows + WIDE + 16])[0:1, 0:1]

    def score(k, masked):
        key = keys_ref[k, 0:rows]
        gate = held_ref[k // 2, pl.ds(pl.multiple_of(WIDE + 16 * (k % 2), 16), 16)]
        drop = (base - joined(gate)) * LOG2E
        drop = jnp.concatenate([drop[0:1], drop[1:2]], axis=1)
        for j in range(count):
            logits = dot(asked_ref[j, 0:rows], key, ((1,), (1,))) * scale + drop
            if masked:
                allowed = y * rows + iota(logits.shape, 1) <= j * rows + iota(logits.shape, 0)
                logits = jnp.where(allowed, logits, NEG)
            logit_ref[k, j] = logits
            top = functools.reduce(
                jnp.maximum, [logits[:, i : i + WIDE] for i in range(0, rows, WIDE)]
            )
            best_ref[j] = jnp.maximum(best_ref[j], top)

    def gather(*blocks):
        value = [jnp.concatenate([keys_ref[k, rows:], ones], axis=1) for k in blocks]
        for j in range(count):
            best = jnp.concatenate([best_ref[j]] * (rows // WIDE), axis=1)
            new = 0.0
            for k, v in zip(blocks, value):
                new = new + dot(jnp.exp2(logit_ref[k, j] - best).astype(BF16), v)
            sum_ref[j] = sum_ref[j] + new

    def score_many(i, carry):
        for k in range(3):
            score(3 * i + k, False)
        return carry

    def score_one(k, carry):
        score(k, False)
        return carry

    def gather_many(i, carry):
        gather(*(4 * i + k for k in range(4)))
        return carry

    def gather_one(k, carry):
        gather(k)
        return carry

    many = z // 3
    lax.fori_loop(0, many, score_many, 0)
    lax.fori_loop(3 * many, z, score_one, 0)
    score(z, True)
    for j in range(count):
        best = jnp.max(best_ref[j], axis=1, keepdims=True)
        best = jnp.where(best > 0.5 * NEG, best, 0.0)
        best_ref[j] = jnp.broadcast_to(best, best_ref.shape[1:])
    many = (z + 1) // 4
    lax.fori_loop(0, many, gather_many, 0)
    lax.fori_loop(4 * many, z + 1, gather_one, 0)
    eye = iota((WIDE, WIDE), 0) == iota((WIDE, WIDE), 1)
    for j in range(count):
        total = sum_ref[j, :, HEAD_ATT:]
        some = total > 0.0
        safe = jnp.where(some, total, 1.0)
        out_ref[j, 0:rows] = (sum_ref[j, :, 0:HEAD_ATT] / safe).astype(BF16)
        level = jnp.where(some, best_ref[j] + jnp.log(safe) * LOG2E, NEG)
        level = [
            jnp.sum(jnp.where(eye, level[i : i + WIDE], 0.0), axis=0, keepdims=True)
            for i in range(0, rows, WIDE)
        ]
        out_ref[j, rows:] = in_thirds(jnp.concatenate(level, axis=0))


def out_kernel(place_ref, parts_ref, lin_ref, gain_ref, wl_ref, wa_ref, own_ref, other_ref):
    count, rows = parts_ref.shape[0], lin_ref.shape[0]
    core = place_ref[3]
    levels = [joined(parts_ref[j, rows:]) for j in range(count)]
    top = functools.reduce(jnp.maximum, levels)
    shares = [jnp.exp2(level - top) for level in levels]
    total = functools.reduce(jnp.add, shares)
    shares = jnp.concatenate([share / total for share in shares], axis=0).T
    raw = []
    for i in range(rows // WIDE):
        mine = slice(i * WIDE, (i + 1) * WIDE)
        raw.append(
            functools.reduce(
                jnp.add,
                [
                    shares[:, 2 * j + i : 2 * j + i + 1] * parts_ref[j, mine].astype(F32)
                    for j in range(count)
                ],
            )
        )
    raw = jnp.concatenate(raw, axis=0)
    size = jnp.mean(raw * raw, axis=1, keepdims=True)
    att = (raw * lax.rsqrt(size + 1e-6) * gain_ref[...]).astype(BF16)
    lin = lin_ref[...]
    width = own_ref.shape[2]
    for c, ref in enumerate((own_ref, other_ref)):
        for j in range(ref.shape[0]):
            start = pl.multiple_of((2 * j + (core if c == 0 else 1 - core)) * width, width)
            mine = pl.ds(start, width)
            ref[j] = (dot(lin, wl_ref[:, mine]) + dot(att, wa_ref[:, mine])).astype(BF16)


def to_partner(a, axis):
    return lax.ppermute(a, axis, [(0, 1), (1, 0)])


def smem():
    return pl.BlockSpec(memory_space=pltpu.SMEM)


def vmem():
    return pl.BlockSpec(memory_space=pltpu.VMEM)


def call(kernel, name, shapes, flops, size, mib, scratch=()):
    def run(*operands):
        many = isinstance(shapes, (list, tuple))
        return pl.pallas_call(
            kernel,
            name=name,
            out_shape=shapes,
            in_specs=[smem()] + [vmem()] * (len(operands) - 1),
            out_specs=[vmem()] * len(shapes) if many else vmem(),
            scratch_shapes=list(scratch),
            compiler_params=params(mib),
            cost_estimate=cost(flops, size),
        )(*operands)

    return run


def body(
    tokens,
    norm_gain,
    recv_weight,
    lin_key_weight,
    lin_value_weight,
    decay_down,
    decay_up,
    decay_log_bias,
    decay_shift,
    learn_rate,
    group_gain,
    initial_state,
    query_weight,
    att_key_weight,
    att_value_weight,
    gate_cache,
    att_gain,
    out_lin_weight,
    out_att_weight,
):
    rows = tokens.shape[0]
    nz, ny, nx = (lax.axis_size(axis) for axis in (KEYS, "near", "x"))
    model_width = norm_gain.shape[0]
    shape = jax.ShapeDtypeStruct
    place = jnp.stack([lax.axis_index(axis) for axis in SP + ("c",)]).astype(jnp.int32)
    gain = norm_gain.reshape(1, -1)

    copies = call(spread_kernel, "spread", shape((nx, *tokens.shape), BF16), 10**10, 1 << 24, 4)(
        place, tokens
    )
    own = lax.all_to_all(copies, "x", 0, 0, tiled=True)
    other = to_partner(own, "c")
    kv = call(
        kv_kernel, "kv", shape((2 * rows, WIDE), BF16), 2 * rows * model_width * 256, 1 << 21, 12
    )(place, own, other, gain, att_key_weight, att_value_weight)
    kv, own, other = lax.optimization_barrier((kv, own, other))
    keys = lax.all_gather(kv, KEYS)

    extra = 16
    send, gates, reach, local = call(
        lin_kernel,
        "lin",
        (
            shape((ny, rows + WIDE + extra, WIDE), BF16),
            shape((extra, WIDE), BF16),
            shape((rows, WIDE), F32),
            shape((rows, WIDE), F32),
        ),
        4 * 10**9,
        1 << 22,
        24,
        scratch=[pltpu.VMEM((2, 2, rows, 2 * rows), F32)],
    )(
        place,
        own,
        other,
        gain,
        recv_weight,
        lin_key_weight,
        lin_value_weight,
        query_weight,
        decay_down.T,
        decay_up,
        decay_log_bias.reshape(1, -1),
        decay_shift,
        learn_rate.reshape(1, -1),
        gate_cache.reshape(rows // WIDE, WIDE),
    )
    asked = lax.all_to_all(send, "near", 0, 0, tiled=True)
    row_send, before = call(
        functools.partial(row_kernel, rows=rows),
        "row",
        (shape((WIDE + extra, WIDE), BF16), shape((2, WIDE, WIDE), F32)),
        10**8,
        1 << 20,
        12,
    )(place, asked, gates)
    pair_send, before = call(
        pair_kernel,
        "pair",
        (shape((WIDE + 2 * extra, WIDE), BF16), shape((2, WIDE, WIDE), F32)),
        10**8,
        1 << 20,
        12,
    )(place, row_send, to_partner(row_send, "zl"), before)
    held = lax.all_gather(pair_send, "zh")
    lin_mixed = call(mix_kernel, "mix", shape((rows, WIDE), BF16), 10**9, 1 << 20, 12)(
        place, initial_state, held, before, reach, local, group_gain.reshape(1, -1)
    )
    found = call(
        functools.partial(att_kernel, rows=rows),
        "att",
        shape((ny, rows + extra, HEAD_ATT), BF16),
        ny * rows * nz * rows * 512,
        1 << 22,
        36,
        scratch=[
            pltpu.VMEM((nz, ny, rows, rows), F32),
            pltpu.VMEM((ny, rows, WIDE), F32),
            pltpu.VMEM((ny, rows, HEAD_ATT + WIDE), F32),
        ],
    )(place, asked, held, keys)
    parts = lax.all_to_all(found, "near", 0, 0, tiled=True)
    width = model_width // (2 * nx)
    tile = shape((nx, rows, width), BF16)
    mine, theirs = call(
        out_kernel, "out", (tile, tile), 2 * rows * 256 * model_width, 1 << 21, 12
    )(place, parts, lin_mixed, att_gain.reshape(1, -1), out_lin_weight, out_att_weight)
    pair = (mine.astype(F32) + to_partner(theirs, "c").astype(F32)).astype(BF16)
    tiles = lax.all_to_all(pair, "x", 0, 0, tiled=True)
    return jnp.sum(tiles.astype(F32), axis=0).astype(BF16)


def solution(mesh):
    sp, tp = mesh.shape["sp"], mesh.shape["tp"]
    cores = 2
    near = math.isqrt(sp) if sp > 16 else 2
    torus = Mesh(mesh.devices.reshape(sp // (2 * near), 2, near, tp // cores, cores), SP + TP)
    return jax.shard_map(
        body,
        mesh=torus,
        in_specs=(
            P(SP, TP),
            P(),
            P(None, TP),
            P(None, TP),
            P(None, TP),
            P(),
            P(None, TP),
            P(TP),
            P(SP, TP),
            P(TP),
            P(TP),
            P(TP, None, None),
            P(None, TP),
            P(None, TP),
            P(None, TP),
            P(SP, TP),
            P(TP),
            P(TP, None),
            P(TP, None),
        ),
        out_specs=P(SP, TP),
        check_vma=False,
    )
```

```python
import functools
import math

import jax
import jax.numpy as jnp
from jax import lax
from jax.experimental import pallas as pl
from jax.experimental.pallas import tpu as pltpu
from jax.sharding import Mesh
from jax.sharding import PartitionSpec as P

HEAD_LIN = 64
HEAD_ATT = 128
WIDE = 128
KEYS = ("zh", "zl")
SP = KEYS + ("near",)
TP = ("x", "c")
LOG2E = math.log2(math.e)
NEG = -1e30
F32 = jnp.float32
BF16 = jnp.bfloat16


def params(mib):
    return pltpu.CompilerParams(vmem_limit_bytes=mib * 1024 * 1024)


def cost(flops, size):
    return pl.CostEstimate(flops=flops, bytes_accessed=size, transcendentals=0)


def dot(a, b, dims=((1,), (0,))):
    return lax.dot_general(a, b, (dims, ((), ())), preferred_element_type=F32)


def parts_of(a):
    high = a.astype(BF16)
    return high, (a - high.astype(F32)).astype(BF16)


def dot3(a, b, dims=((1,), (0,))):
    ah, al = parts_of(a)
    bh, bl = parts_of(b)
    return dot(ah, bh, dims) + (dot(ah, bl, dims) + dot(al, bh, dims))


def dot2(a, b, dims=((1,), (0,))):
    ah, al = parts_of(a)
    return dot(ah, b, dims) + dot(al, b, dims)


def in_thirds(a):
    high, mid = parts_of(a)
    low = (a - high.astype(F32) - mid.astype(F32)).astype(BF16)
    return jnp.concatenate([high, mid, low, jnp.zeros((10, WIDE), BF16)], axis=0)


def iota(shape, dim):
    return lax.broadcasted_iota(jnp.int32, shape, dim)


def by_head(a):
    left = iota(a.shape, 1) < HEAD_LIN
    first = jnp.sum(jnp.where(left, a, 0.0), axis=1, keepdims=True)
    second = jnp.sum(jnp.where(left, 0.0, a), axis=1, keepdims=True)
    return jnp.where(left, first, second)


def scaled_pieces(place_ref, own_ref, other_ref, gain_ref):
    shards, rows, depth = own_ref.shape
    core = place_ref[3]
    scaled, squares = [], jnp.zeros((rows, depth), F32)
    for c, ref in enumerate((own_ref, other_ref)):
        for j in range(shards):
            start = pl.multiple_of((2 * j + (core if c == 0 else 1 - core)) * depth, depth)
            wide = ref[j].astype(F32)
            scaled.append(((wide * gain_ref[:, pl.ds(start, depth)]).astype(BF16), start))
            squares = squares + wide * wide
    mean = jnp.sum(squares, axis=1, keepdims=True) / (2 * shards * depth)
    return scaled, lax.rsqrt(mean + 1e-6)


def projected(scaled, inverse, *w_refs):
    total = 0.0
    for piece, start in scaled:
        weight = [w_ref[pl.ds(start, piece.shape[1])] for w_ref in w_refs]
        total = total + dot(piece, jnp.concatenate(weight, axis=1))
    return total * inverse


def spread_kernel(place_ref, tokens_ref, out_ref):
    tokens = tokens_ref[...]
    for j in range(out_ref.shape[0]):
        out_ref[j] = tokens


def kv_kernel(place_ref, own_ref, other_ref, gain_ref, wk_ref, wv_ref, out_ref):
    scaled, inverse = scaled_pieces(place_ref, own_ref, other_ref, gain_ref)
    rows = own_ref.shape[1]
    both = projected(scaled, inverse, wk_ref, wv_ref).astype(BF16)
    out_ref[0:rows] = both[:, :HEAD_ATT]
    out_ref[rows:] = both[:, HEAD_ATT:]


def spans(log_decay):
    rows = log_decay.shape[0]
    row = iota(log_decay.shape, 0)
    zero = jnp.zeros_like(log_decay)
    before = [None] + [pltpu.roll(log_decay, i, 0) for i in range(1, 8)]
    behind = [None] + [pltpu.roll(log_decay, rows - i, 0) for i in range(1, 8)]
    ahead, after = {1: zero}, {1: zero}
    for h in (2, 4, 8):
        place = row & (h - 1)
        a, b = zero, zero
        for i in range(1, h):
            a = a + jnp.where(place >= i, before[i], 0.0)
            b = b + jnp.where(place + i < h, behind[i], 0.0)
        ahead[h], after[h] = a, b
    h = 8
    while h < rows:
        shape = (rows // (2 * h), 2 * h, WIDE)
        a, b = ahead[h].reshape(shape), after[h].reshape(shape)
        step = log_decay.reshape(shape)
        left = a[:, h - 1 : h] + step[:, h - 1 : h]
        right = b[:, h : h + 1] + step[:, h : h + 1]
        a = jnp.concatenate([a[:, :h], a[:, h:] + left], axis=1)
        b = jnp.concatenate([b[:, :h] + right, b[:, h:]], axis=1)
        h *= 2
        ahead[h], after[h] = a.reshape(rows, WIDE), b.reshape(rows, WIDE)
    return ahead, after


def lin_kernel(
    place_ref,
    own_ref,
    other_ref,
    gain_ref,
    wr_ref,
    wk_ref,
    wv_ref,
    wq_ref,
    down_ref,
    up_ref,
    bias_ref,
    shift_ref,
    rate_ref,
    gate_ref,
    send_ref,
    gates_ref,
    reach_ref,
    local_ref,
    pairs_ref,
):
    scaled, inverse = scaled_pieces(place_ref, own_ref, other_ref, gain_ref)
    rows = shift_ref.shape[0]
    both = projected(scaled, inverse, wr_ref, wk_ref).astype(BF16)
    recv, key = both[:, :WIDE].astype(F32), both[:, WIDE:].astype(F32)
    both = projected(scaled, inverse, wv_ref, wq_ref).astype(BF16)
    value = both[:, :WIDE]
    send_ref[0, 0:rows] = both[:, WIDE:]
    low = 0.0
    for piece, start in scaled:
        low = low + dot(piece, down_ref[:, pl.ds(start, piece.shape[1])], ((1,), (1,)))
    low = (low * inverse).astype(BF16).astype(F32)
    exponent = bias_ref[...] + shift_ref[...] + dot(jnp.tanh(low).astype(BF16), up_ref[...])
    log_decay = -jnp.exp(exponent)
    unit = key * lax.rsqrt(by_head(key * key) + 1e-6)
    rate = unit * rate_ref[...]

    ahead, after = spans(log_decay)
    half = rows // 2
    lane = iota((rows, WIDE), 1)
    row = iota((rows, WIDE), 0)
    tall = iota((half, half), 0)
    flat = iota((half, half), 1)
    heads = [lane < HEAD_LIN, lane >= HEAD_LIN]
    eye = tall == flat
    blocks = slice(0, half), slice(half, rows)

    def of_heads(a):
        return [jnp.where(mine, a, 0.0).astype(BF16) for mine in heads]

    def below(h):
        level = h.bit_length()
        near = (tall >> level) == (flat >> level)
        return near & ((tall & h) != 0) & ((flat & h) == 0)

    for m, source in enumerate((key, rate)):
        now = by_head(recv * source)
        for n in range(2):
            for b in range(2):
                cols = slice(m * rows + b * half, m * rows + (b + 1) * half)
                same_row = now[blocks[b], n * HEAD_LIN : n * HEAD_LIN + 1]
                pairs_ref[n, 1, blocks[b], cols] = jnp.where(eye, same_row, 0.0)
                pairs_ref[n, 0, blocks[b], cols] = jnp.zeros((half, half), F32)
            cols = slice(m * rows + half, (m + 1) * rows)
            for k in range(2):
                pairs_ref[n, k, blocks[0], cols] = jnp.zeros((half, half), F32)
    h = 1
    while h < rows:
        late = (row & h) != 0
        to_u = jnp.where(late, jnp.exp(ahead[h]), 0.0)
        to_q = jnp.where(late, jnp.exp(ahead[h] + log_decay), 0.0)
        from_s = jnp.where(late, 0.0, jnp.exp(after[h]))
        right = (key * from_s).astype(BF16), (rate * from_s).astype(BF16)
        left = of_heads(unit * to_u) + of_heads(recv * to_q)
        for b in range(2) if h < half else (1,):
            c = b if h < half else 0
            product = dot(
                jnp.concatenate([a[blocks[b]] for a in left], axis=0),
                jnp.concatenate([a[blocks[c]] for a in right], axis=0),
                ((1,), (1,)),
            )
            for k in range(2):
                for n in range(2):
                    for m in range(2):
                        cols = slice(m * rows + c * half, m * rows + (c + 1) * half)
                        new = product[
                            (2 * k + n) * half : (2 * k + n + 1) * half,
                            m * half : (m + 1) * half,
                        ]
                        if h < half:
                            new = jnp.where(below(h), new, pairs_ref[n, k, blocks[b], cols])
                        pairs_ref[n, k, blocks[b], cols] = new
        h *= 2

    solved = {}
    h = 1
    while h < half:
        here = below(h)
        for n in range(2):
            for b in range(2):
                cols = slice(rows + b * half, rows + (b + 1) * half)
                links = jnp.where(here, pairs_ref[n, 0, blocks[b], cols], 0.0)
                if h == 1:
                    solved[n, b] = jnp.where(eye, 1.0, 0.0) - links
                else:
                    step = dot3(links, solved[n, b])
                    solved[n, b] = solved[n, b] - dot3(solved[n, b], step)
        h *= 2

    full_u = unit * jnp.exp(ahead[rows])
    full_q = recv * jnp.exp(ahead[rows] + log_decay)
    tail = jnp.exp(after[rows])
    full_k = key * tail
    full_r = rate * tail
    reach, local, moved = [], [], []
    for n in range(2):
        add = dot2(pairs_ref[n, 0, :, :rows], value)
        source = jnp.where(heads[n], full_u, pltpu.roll(add, HEAD_LIN, 1))
        first = dot3(solved[n, 0], source[:half])
        later = source[half:] - dot3(pairs_ref[n, 0, half:, rows : rows + half], first)
        along = jnp.concatenate([first, dot3(solved[n, 1], later)], axis=0)
        taken = dot3(pairs_ref[n, 1, :, rows:], along)
        reach.append(full_q - taken)
        local.append(dot2(pairs_ref[n, 1, :, :rows], value) - pltpu.roll(taken, HEAD_LIN, 1))
        moved.append(dot3(along, full_r, ((0,), (0,))))
    reach_ref[...] = jnp.where(heads[0], reach[0], reach[1])
    local_ref[...] = jnp.where(heads[0], local[0], local[1])

    lane = iota((WIDE, WIDE), 1)
    row = iota((WIDE, WIDE), 0)
    same = (lane < HEAD_LIN) == (row < HEAD_LIN)
    added = pltpu.roll(dot2(full_k, value, ((0,), (0,))).T, HEAD_LIN, 0)
    last = jnp.exp(ahead[rows][rows - 1 : rows] + log_decay[rows - 1 : rows]) - 1.0
    packed = jnp.where(same, jnp.where(lane == row, last, 0.0), added)
    packed = packed - jnp.where(lane < HEAD_LIN, moved[0], moved[1])
    send_ref[0, rows : rows + WIDE] = packed.astype(BF16)
    gates = in_thirds(gate_ref[...])
    send_ref[0, rows + WIDE :] = gates
    gates_ref[...] = gates
    whole = send_ref[0]
    for j in range(1, send_ref.shape[0]):
        send_ref[j] = whole


def unpacked(packed):
    packed = packed.astype(F32)
    lane = iota((WIDE, WIDE), 1)
    row = iota((WIDE, WIDE), 0)
    same = (lane < HEAD_LIN) == (row < HEAD_LIN)
    return jnp.where(same, packed, 0.0), jnp.where(same, pltpu.roll(packed, HEAD_LIN, 0), 0.0)


def repacked(total):
    lane = iota((WIDE, WIDE), 1)
    row = iota((WIDE, WIDE), 0)
    same = (lane < HEAD_LIN) == (row < HEAD_LIN)
    return jnp.where(same, total[0], pltpu.roll(total[1], HEAD_LIN, 0)).astype(BF16)


def chained(first, second):
    return (
        first[0] + second[0] + dot3(first[0], second[0]),
        first[1] + second[1] + dot3(first[1], second[0]),
    )


def row_kernel(place_ref, gathered_ref, gates_ref, send_ref, before_ref, *, rows):
    near = place_ref[2]
    count = gathered_ref.shape[0]
    total = mine = jnp.zeros((WIDE, WIDE), F32), jnp.zeros((WIDE, WIDE), F32)
    for j in range(count):
        mine = tuple(jnp.where(near == j, t, m) for t, m in zip(total, mine))
        here = unpacked(gathered_ref[j, rows : rows + WIDE])
        total = chained(total, here) if j else here
    before_ref[0], before_ref[1] = mine
    send_ref[0:WIDE] = repacked(total)
    send_ref[WIDE:] = gates_ref[...]


def mix_kernel(place_ref, state_ref, gathered_ref, before_ref, reach_ref, local_ref, gain_ref, out_ref):
    none = jnp.zeros((HEAD_LIN, HEAD_LIN), F32)
    state = jnp.concatenate(
        [
            jnp.concatenate([state_ref[0], none], axis=1),
            jnp.concatenate([none, state_ref[1]], axis=1),
        ],
        axis=0,
    )

    def step(k, state):
        packed = gathered_ref[k]
        moved, added = unpacked(packed[0:WIDE])
        return state + dot2(state, moved.astype(BF16)) + added

    state = lax.fori_loop(0, place_ref[0] * 2 + place_ref[1], step, state)
    state = state + dot3(state, before_ref[0]) + before_ref[1]
    raw = dot3(reach_ref[...], state, ((1,), (1,))) + local_ref[...]
    off = raw - by_head(raw) * (1.0 / HEAD_LIN)
    spread = by_head(off * off) * (1.0 / HEAD_LIN)
    out_ref[...] = (off * lax.rsqrt(spread + 0.00064) * gain_ref[...]).astype(BF16)


def joined(gates):
    gates = gates.astype(F32)
    return gates[0:2] + gates[2:4] + gates[4:6]


def att_kernel(
    place_ref, asked_ref, held_ref, keys_ref, out_ref, logit_ref, best_ref, sum_ref, *, rows
):
    z, y = place_ref[0] * 2 + place_ref[1], place_ref[2]
    count = asked_ref.shape[0]
    scale = HEAD_ATT ** (-0.5) * LOG2E
    best_ref[...] = jnp.full(best_ref.shape, NEG, F32)
    sum_ref[...] = jnp.zeros(sum_ref.shape, F32)
    ones = jnp.ones((rows, HEAD_ATT), BF16)
    base = joined(asked_ref[0, rows + WIDE : rows + WIDE + 16])[0:1, 0:1]

    def score(k, masked):
        key = keys_ref[k, 0:rows]
        drop = (base - joined(held_ref[k, WIDE : WIDE + 16])) * LOG2E
        drop = jnp.concatenate([drop[0:1], drop[1:2]], axis=1)
        for j in range(count):
            logits = dot(asked_ref[j, 0:rows], key, ((1,), (1,))) * scale + drop
            if masked:
                allowed = y * rows + iota(logits.shape, 1) <= j * rows + iota(logits.shape, 0)
                logits = jnp.where(allowed, logits, NEG)
            logit_ref[k, j] = logits
            top = functools.reduce(
                jnp.maximum, [logits[:, i : i + WIDE] for i in range(0, rows, WIDE)]
            )
            best_ref[j] = jnp.maximum(best_ref[j], top)

    def gather(*blocks):
        value = [jnp.concatenate([keys_ref[k, rows:], ones], axis=1) for k in blocks]
        for j in range(count):
            best = jnp.concatenate([best_ref[j]] * (rows // WIDE), axis=1)
            new = 0.0
            for k, v in zip(blocks, value):
                new = new + dot(jnp.exp2(logit_ref[k, j] - best).astype(BF16), v)
            sum_ref[j] = sum_ref[j] + new

    def score_many(i, carry):
        for k in range(3):
            score(3 * i + k, False)
        return carry

    def score_one(k, carry):
        score(k, False)
        return carry

    def gather_many(i, carry):
        gather(*(4 * i + k for k in range(4)))
        return carry

    def gather_one(k, carry):
        gather(k)
        return carry

    many = z // 3
    lax.fori_loop(0, many, score_many, 0)
    lax.fori_loop(3 * many, z, score_one, 0)
    score(z, True)
    for j in range(count):
        best = jnp.max(best_ref[j], axis=1, keepdims=True)
        best = jnp.where(best > 0.5 * NEG, best, 0.0)
        best_ref[j] = jnp.broadcast_to(best, best_ref.shape[1:])
    many = (z + 1) // 4
    lax.fori_loop(0, many, gather_many, 0)
    lax.fori_loop(4 * many, z + 1, gather_one, 0)
    eye = iota((WIDE, WIDE), 0) == iota((WIDE, WIDE), 1)
    for j in range(count):
        total = sum_ref[j, :, HEAD_ATT:]
        some = total > 0.0
        safe = jnp.where(some, total, 1.0)
        out_ref[j, 0:rows] = (sum_ref[j, :, 0:HEAD_ATT] / safe).astype(BF16)
        level = jnp.where(some, best_ref[j] + jnp.log(safe) * LOG2E, NEG)
        level = [
            jnp.sum(jnp.where(eye, level[i : i + WIDE], 0.0), axis=0, keepdims=True)
            for i in range(0, rows, WIDE)
        ]
        out_ref[j, rows:] = in_thirds(jnp.concatenate(level, axis=0))


def out_kernel(place_ref, parts_ref, lin_ref, gain_ref, wl_ref, wa_ref, own_ref, other_ref):
    count, rows = parts_ref.shape[0], lin_ref.shape[0]
    core = place_ref[3]
    levels = [joined(parts_ref[j, rows:]) for j in range(count)]
    top = functools.reduce(jnp.maximum, levels)
    shares = [jnp.exp2(level - top) for level in levels]
    total = functools.reduce(jnp.add, shares)
    shares = jnp.concatenate([share / total for share in shares], axis=0).T
    raw = []
    for i in range(rows // WIDE):
        mine = slice(i * WIDE, (i + 1) * WIDE)
        raw.append(
            functools.reduce(
                jnp.add,
                [
                    shares[:, 2 * j + i : 2 * j + i + 1] * parts_ref[j, mine].astype(F32)
                    for j in range(count)
                ],
            )
        )
    raw = jnp.concatenate(raw, axis=0)
    size = jnp.mean(raw * raw, axis=1, keepdims=True)
    att = (raw * lax.rsqrt(size + 1e-6) * gain_ref[...]).astype(BF16)
    lin = lin_ref[...]
    width = own_ref.shape[2]
    for c, ref in enumerate((own_ref, other_ref)):
        for j in range(ref.shape[0]):
            start = pl.multiple_of((2 * j + (core if c == 0 else 1 - core)) * width, width)
            mine = pl.ds(start, width)
            ref[j] = (dot(lin, wl_ref[:, mine]) + dot(att, wa_ref[:, mine])).astype(BF16)


def to_partner(a, axis):
    return lax.ppermute(a, axis, [(0, 1), (1, 0)])


def smem():
    return pl.BlockSpec(memory_space=pltpu.SMEM)


def vmem():
    return pl.BlockSpec(memory_space=pltpu.VMEM)


def call(kernel, name, shapes, flops, size, mib, scratch=()):
    def run(*operands):
        many = isinstance(shapes, (list, tuple))
        return pl.pallas_call(
            kernel,
            name=name,
            out_shape=shapes,
            in_specs=[smem()] + [vmem()] * (len(operands) - 1),
            out_specs=[vmem()] * len(shapes) if many else vmem(),
            scratch_shapes=list(scratch),
            compiler_params=params(mib),
            cost_estimate=cost(flops, size),
        )(*operands)

    return run


def body(
    tokens,
    norm_gain,
    recv_weight,
    lin_key_weight,
    lin_value_weight,
    decay_down,
    decay_up,
    decay_log_bias,
    decay_shift,
    learn_rate,
    group_gain,
    initial_state,
    query_weight,
    att_key_weight,
    att_value_weight,
    gate_cache,
    att_gain,
    out_lin_weight,
    out_att_weight,
):
    rows = tokens.shape[0]
    nz, ny, nx = (lax.axis_size(axis) for axis in (KEYS, "near", "x"))
    model_width = norm_gain.shape[0]
    shape = jax.ShapeDtypeStruct
    place = jnp.stack([lax.axis_index(axis) for axis in SP + ("c",)]).astype(jnp.int32)
    gain = norm_gain.reshape(1, -1)

    copies = call(spread_kernel, "spread", shape((nx, *tokens.shape), BF16), 10**10, 1 << 24, 4)(
        place, tokens
    )
    own = lax.all_to_all(copies, "x", 0, 0, tiled=True)
    other = to_partner(own, "c")
    kv = call(
        kv_kernel, "kv", shape((2 * rows, WIDE), BF16), 2 * rows * model_width * 256, 1 << 21, 12
    )(place, own, other, gain, att_key_weight, att_value_weight)
    keys = lax.all_gather(kv, KEYS)

    extra = 16
    send, gates, reach, local = call(
        lin_kernel,
        "lin",
        (
            shape((ny, rows + WIDE + extra, WIDE), BF16),
            shape((extra, WIDE), BF16),
            shape((rows, WIDE), F32),
            shape((rows, WIDE), F32),
        ),
        4 * 10**9,
        1 << 22,
        24,
        scratch=[pltpu.VMEM((2, 2, rows, 2 * rows), F32)],
    )(
        place,
        own,
        other,
        gain,
        recv_weight,
        lin_key_weight,
        lin_value_weight,
        query_weight,
        decay_down.T,
        decay_up,
        decay_log_bias.reshape(1, -1),
        decay_shift,
        learn_rate.reshape(1, -1),
        gate_cache.reshape(rows // WIDE, WIDE),
    )
    asked = lax.all_to_all(send, "near", 0, 0, tiled=True)
    row_send, before = call(
        functools.partial(row_kernel, rows=rows),
        "row",
        (shape((WIDE + extra, WIDE), BF16), shape((2, WIDE, WIDE), F32)),
        10**8,
        1 << 20,
        12,
    )(place, asked, gates)
    held = lax.all_gather(row_send, KEYS)
    lin_mixed = call(mix_kernel, "mix", shape((rows, WIDE), BF16), 10**9, 1 << 20, 12)(
        place, initial_state, held, before, reach, local, group_gain.reshape(1, -1)
    )
    found = call(
        functools.partial(att_kernel, rows=rows),
        "att",
        shape((ny, rows + extra, HEAD_ATT), BF16),
        ny * rows * nz * rows * 512,
        1 << 22,
        36,
        scratch=[
            pltpu.VMEM((nz, ny, rows, rows), F32),
            pltpu.VMEM((ny, rows, WIDE), F32),
            pltpu.VMEM((ny, rows, HEAD_ATT + WIDE), F32),
        ],
    )(place, asked, held, keys)
    parts = lax.all_to_all(found, "near", 0, 0, tiled=True)
    width = model_width // (2 * nx)
    tile = shape((nx, rows, width), BF16)
    mine, theirs = call(
        out_kernel, "out", (tile, tile), 2 * rows * 256 * model_width, 1 << 21, 12
    )(place, parts, lin_mixed, att_gain.reshape(1, -1), out_lin_weight, out_att_weight)
    pair = (mine.astype(F32) + to_partner(theirs, "c").astype(F32)).astype(BF16)
    tiles = lax.all_to_all(pair, "x", 0, 0, tiled=True)
    return jnp.sum(tiles.astype(F32), axis=0).astype(BF16)


def solution(mesh):
    sp, tp = mesh.shape["sp"], mesh.shape["tp"]
    cores = 2
    near = math.isqrt(sp) if sp > 16 else 2
    torus = Mesh(mesh.devices.reshape(sp // (2 * near), 2, near, tp // cores, cores), SP + TP)
    return jax.shard_map(
        body,
        mesh=torus,
        in_specs=(
            P(SP, TP),
            P(),
            P(None, TP),
            P(None, TP),
            P(None, TP),
            P(),
            P(None, TP),
            P(TP),
            P(SP, TP),
            P(TP),
            P(TP),
            P(TP, None, None),
            P(None, TP),
            P(None, TP),
            P(None, TP),
            P(SP, TP),
            P(TP),
            P(TP, None),
            P(TP, None),
        ),
        out_specs=P(SP, TP),
        check_vma=False,
    )
```

```python
import functools
import math

import jax
import jax.numpy as jnp
from jax import lax
from jax.experimental import pallas as pl
from jax.experimental.pallas import tpu as pltpu
from jax.sharding import Mesh
from jax.sharding import PartitionSpec as P

HEAD_LIN = 64
HEAD_ATT = 128
WIDE = 128
KEYS = ("zh", "zl")
SP = KEYS + ("near",)
TP = ("x", "c")
LOG2E = math.log2(math.e)
NEG = -1e30
F32 = jnp.float32
BF16 = jnp.bfloat16


def params(mib):
    return pltpu.CompilerParams(vmem_limit_bytes=mib * 1024 * 1024)


def cost(flops, size):
    return pl.CostEstimate(flops=flops, bytes_accessed=size, transcendentals=0)


def dot(a, b, dims=((1,), (0,))):
    return lax.dot_general(a, b, (dims, ((), ())), preferred_element_type=F32)


def parts_of(a):
    high = a.astype(BF16)
    return high, (a - high.astype(F32)).astype(BF16)


def dot3(a, b, dims=((1,), (0,))):
    ah, al = parts_of(a)
    bh, bl = parts_of(b)
    return dot(ah, bh, dims) + (dot(ah, bl, dims) + dot(al, bh, dims))


def dot2(a, b, dims=((1,), (0,))):
    ah, al = parts_of(a)
    return dot(ah, b, dims) + dot(al, b, dims)


def in_thirds(a):
    high, mid = parts_of(a)
    low = (a - high.astype(F32) - mid.astype(F32)).astype(BF16)
    return jnp.concatenate([high, mid, low, jnp.zeros((10, WIDE), BF16)], axis=0)


def iota(shape, dim):
    return lax.broadcasted_iota(jnp.int32, shape, dim)


def by_head(a):
    left = iota(a.shape, 1) < HEAD_LIN
    first = jnp.sum(jnp.where(left, a, 0.0), axis=1, keepdims=True)
    second = jnp.sum(jnp.where(left, 0.0, a), axis=1, keepdims=True)
    return jnp.where(left, first, second)


def scaled_part(ref, gain_ref, core):
    shards, rows, depth = ref.shape
    scaled, squares = [], jnp.zeros((rows, depth), F32)
    for j in range(shards):
        start = pl.multiple_of((2 * j + core) * depth, depth)
        wide = ref[j].astype(F32)
        scaled.append(((wide * gain_ref[:, pl.ds(start, depth)]).astype(BF16), start))
        squares = squares + wide * wide
    return scaled, jnp.sum(squares, axis=1, keepdims=True)


def inverse_rms(squares, gain_ref):
    return lax.rsqrt(squares / gain_ref.shape[1] + 1e-6)


def scaled_pieces(place_ref, own_ref, other_ref, gain_ref):
    core = place_ref[3]
    own, own_squares = scaled_part(own_ref, gain_ref, core)
    other, other_squares = scaled_part(other_ref, gain_ref, 1 - core)
    return own + other, inverse_rms(own_squares + other_squares, gain_ref)


def projected(scaled, inverse, *w_refs):
    total = 0.0
    for piece, start in scaled:
        weight = [w_ref[pl.ds(start, piece.shape[1])] for w_ref in w_refs]
        total = total + dot(piece, jnp.concatenate(weight, axis=1))
    return total * inverse


def place_kernel(place_ref, out_ref):
    for i in range(out_ref.shape[0]):
        out_ref[i] = place_ref[i]


def kv_part_kernel(place_ref, own_ref, gain_ref, wk_ref, wv_ref, part_ref, squares_ref):
    scaled, squares = scaled_part(own_ref, gain_ref, place_ref[3])
    part_ref[...] = projected(scaled, 1.0, wk_ref, wv_ref)
    squares_ref[...] = jnp.broadcast_to(squares, squares_ref.shape)


def kv_kernel(place_ref, other_ref, gain_ref, wk_ref, wv_ref, part_ref, squares_ref, out_ref):
    scaled, squares = scaled_part(other_ref, gain_ref, 1 - place_ref[3])
    rows = other_ref.shape[1]
    inverse = inverse_rms(squares + squares_ref[:, 0:1], gain_ref)
    both = projected(scaled, 1.0, wk_ref, wv_ref) + part_ref[...]
    both = (both * inverse).astype(BF16)
    out_ref[0:rows] = both[:, :HEAD_ATT]
    out_ref[rows:] = both[:, HEAD_ATT:]


def spans(log_decay):
    rows = log_decay.shape[0]
    row = iota(log_decay.shape, 0)
    zero = jnp.zeros_like(log_decay)
    before = [None] + [pltpu.roll(log_decay, i, 0) for i in range(1, 8)]
    behind = [None] + [pltpu.roll(log_decay, rows - i, 0) for i in range(1, 8)]
    ahead, after = {1: zero}, {1: zero}
    for h in (2, 4, 8):
        place = row & (h - 1)
        a, b = zero, zero
        for i in range(1, h):
            a = a + jnp.where(place >= i, before[i], 0.0)
            b = b + jnp.where(place + i < h, behind[i], 0.0)
        ahead[h], after[h] = a, b
    h = 8
    while h < rows:
        shape = (rows // (2 * h), 2 * h, WIDE)
        a, b = ahead[h].reshape(shape), after[h].reshape(shape)
        step = log_decay.reshape(shape)
        left = a[:, h - 1 : h] + step[:, h - 1 : h]
        right = b[:, h : h + 1] + step[:, h : h + 1]
        a = jnp.concatenate([a[:, :h], a[:, h:] + left], axis=1)
        b = jnp.concatenate([b[:, :h] + right, b[:, h:]], axis=1)
        h *= 2
        ahead[h], after[h] = a.reshape(rows, WIDE), b.reshape(rows, WIDE)
    return ahead, after


def lin_kernel(
    place_ref,
    own_ref,
    other_ref,
    gain_ref,
    wr_ref,
    wk_ref,
    wv_ref,
    wq_ref,
    down_ref,
    up_ref,
    bias_ref,
    shift_ref,
    rate_ref,
    gate_ref,
    send_ref,
    gates_ref,
    reach_ref,
    local_ref,
    pairs_ref,
):
    scaled, inverse = scaled_pieces(place_ref, own_ref, other_ref, gain_ref)
    rows = shift_ref.shape[0]
    both = projected(scaled, inverse, wr_ref, wk_ref).astype(BF16)
    recv, key = both[:, :WIDE].astype(F32), both[:, WIDE:].astype(F32)
    both = projected(scaled, inverse, wv_ref, wq_ref).astype(BF16)
    value = both[:, :WIDE]
    send_ref[0, 0:rows] = both[:, WIDE:]
    low = 0.0
    for piece, start in scaled:
        low = low + dot(piece, down_ref[:, pl.ds(start, piece.shape[1])], ((1,), (1,)))
    low = (low * inverse).astype(BF16).astype(F32)
    exponent = bias_ref[...] + shift_ref[...] + dot(jnp.tanh(low).astype(BF16), up_ref[...])
    log_decay = -jnp.exp(exponent)
    unit = key * lax.rsqrt(by_head(key * key) + 1e-6)
    rate = unit * rate_ref[...]

    ahead, after = spans(log_decay)
    half = rows // 2
    lane = iota((rows, WIDE), 1)
    row = iota((rows, WIDE), 0)
    tall = iota((half, half), 0)
    flat = iota((half, half), 1)
    heads = [lane < HEAD_LIN, lane >= HEAD_LIN]
    eye = tall == flat
    blocks = slice(0, half), slice(half, rows)

    def of_heads(a):
        return [jnp.where(mine, a, 0.0).astype(BF16) for mine in heads]

    def below(h):
        level = h.bit_length()
        near = (tall >> level) == (flat >> level)
        return near & ((tall & h) != 0) & ((flat & h) == 0)

    for m, source in enumerate((key, rate)):
        now = by_head(recv * source)
        for n in range(2):
            for b in range(2):
                cols = slice(m * rows + b * half, m * rows + (b + 1) * half)
                same_row = now[blocks[b], n * HEAD_LIN : n * HEAD_LIN + 1]
                pairs_ref[n, 1, blocks[b], cols] = jnp.where(eye, same_row, 0.0)
                pairs_ref[n, 0, blocks[b], cols] = jnp.zeros((half, half), F32)
            cols = slice(m * rows + half, (m + 1) * rows)
            for k in range(2):
                pairs_ref[n, k, blocks[0], cols] = jnp.zeros((half, half), F32)
    h = 1
    while h < rows:
        late = (row & h) != 0
        to_u = jnp.where(late, jnp.exp(ahead[h]), 0.0)
        to_q = jnp.where(late, jnp.exp(ahead[h] + log_decay), 0.0)
        from_s = jnp.where(late, 0.0, jnp.exp(after[h]))
        right = (key * from_s).astype(BF16), (rate * from_s).astype(BF16)
        left = of_heads(unit * to_u) + of_heads(recv * to_q)
        for b in range(2) if h < half else (1,):
            c = b if h < half else 0
            product = dot(
                jnp.concatenate([a[blocks[b]] for a in left], axis=0),
                jnp.concatenate([a[blocks[c]] for a in right], axis=0),
                ((1,), (1,)),
            )
            for k in range(2):
                for n in range(2):
                    for m in range(2):
                        cols = slice(m * rows + c * half, m * rows + (c + 1) * half)
                        new = product[
                            (2 * k + n) * half : (2 * k + n + 1) * half,
                            m * half : (m + 1) * half,
                        ]
                        if h < half:
                            new = jnp.where(below(h), new, pairs_ref[n, k, blocks[b], cols])
                        pairs_ref[n, k, blocks[b], cols] = new
        h *= 2

    solved = {}
    h = 1
    while h < half:
        here = below(h)
        for n in range(2):
            for b in range(2):
                cols = slice(rows + b * half, rows + (b + 1) * half)
                links = jnp.where(here, pairs_ref[n, 0, blocks[b], cols], 0.0)
                if h == 1:
                    solved[n, b] = jnp.where(eye, 1.0, 0.0) - links
                else:
                    step = dot3(links, solved[n, b])
                    solved[n, b] = solved[n, b] - dot3(solved[n, b], step)
        h *= 2

    full_u = unit * jnp.exp(ahead[rows])
    full_q = recv * jnp.exp(ahead[rows] + log_decay)
    tail = jnp.exp(after[rows])
    full_k = key * tail
    full_r = rate * tail
    reach, local, moved = [], [], []
    for n in range(2):
        add = dot2(pairs_ref[n, 0, :, :rows], value)
        source = jnp.where(heads[n], full_u, pltpu.roll(add, HEAD_LIN, 1))
        first = dot3(solved[n, 0], source[:half])
        later = source[half:] - dot3(pairs_ref[n, 0, half:, rows : rows + half], first)
        along = jnp.concatenate([first, dot3(solved[n, 1], later)], axis=0)
        taken = dot3(pairs_ref[n, 1, :, rows:], along)
        reach.append(full_q - taken)
        local.append(dot2(pairs_ref[n, 1, :, :rows], value) - pltpu.roll(taken, HEAD_LIN, 1))
        moved.append(dot3(along, full_r, ((0,), (0,))))
    reach_ref[...] = jnp.where(heads[0], reach[0], reach[1])
    local_ref[...] = jnp.where(heads[0], local[0], local[1])

    lane = iota((WIDE, WIDE), 1)
    row = iota((WIDE, WIDE), 0)
    same = (lane < HEAD_LIN) == (row < HEAD_LIN)
    added = pltpu.roll(dot2(full_k, value, ((0,), (0,))).T, HEAD_LIN, 0)
    last = jnp.exp(ahead[rows][rows - 1 : rows] + log_decay[rows - 1 : rows]) - 1.0
    packed = jnp.where(same, jnp.where(lane == row, last, 0.0), added)
    packed = packed - jnp.where(lane < HEAD_LIN, moved[0], moved[1])
    send_ref[0, rows : rows + WIDE] = packed.astype(BF16)
    gates = in_thirds(gate_ref[...])
    send_ref[0, rows + WIDE :] = gates
    gates_ref[...] = gates
    whole = send_ref[0]
    for j in range(1, send_ref.shape[0]):
        send_ref[j] = whole


def unpacked(packed):
    packed = packed.astype(F32)
    lane = iota((WIDE, WIDE), 1)
    row = iota((WIDE, WIDE), 0)
    same = (lane < HEAD_LIN) == (row < HEAD_LIN)
    return jnp.where(same, packed, 0.0), jnp.where(same, pltpu.roll(packed, HEAD_LIN, 0), 0.0)


def repacked(total):
    lane = iota((WIDE, WIDE), 1)
    row = iota((WIDE, WIDE), 0)
    same = (lane < HEAD_LIN) == (row < HEAD_LIN)
    return jnp.where(same, total[0], pltpu.roll(total[1], HEAD_LIN, 0)).astype(BF16)


def chained(first, second):
    return (
        first[0] + second[0] + dot3(first[0], second[0]),
        first[1] + second[1] + dot3(first[1], second[0]),
    )


def row_kernel(place_ref, gathered_ref, gates_ref, send_ref, before_ref, *, rows):
    near = place_ref[2]
    count = gathered_ref.shape[0]
    total = mine = jnp.zeros((WIDE, WIDE), F32), jnp.zeros((WIDE, WIDE), F32)
    for j in range(count):
        mine = tuple(jnp.where(near == j, t, m) for t, m in zip(total, mine))
        here = unpacked(gathered_ref[j, rows : rows + WIDE])
        total = chained(total, here) if j else here
    before_ref[0], before_ref[1] = mine
    send_ref[0:WIDE] = repacked(total)
    send_ref[WIDE:] = gates_ref[...]


def mix_kernel(place_ref, state_ref, gathered_ref, before_ref, reach_ref, local_ref, gain_ref, out_ref):
    none = jnp.zeros((HEAD_LIN, HEAD_LIN), F32)
    state = jnp.concatenate(
        [
            jnp.concatenate([state_ref[0], none], axis=1),
            jnp.concatenate([none, state_ref[1]], axis=1),
        ],
        axis=0,
    )

    def step(k, state):
        packed = gathered_ref[k]
        moved, added = unpacked(packed[0:WIDE])
        return state + dot2(state, moved.astype(BF16)) + added

    state = lax.fori_loop(0, place_ref[0] * 2 + place_ref[1], step, state)
    state = state + dot3(state, before_ref[0]) + before_ref[1]
    raw = dot3(reach_ref[...], state, ((1,), (1,))) + local_ref[...]
    off = raw - by_head(raw) * (1.0 / HEAD_LIN)
    spread = by_head(off * off) * (1.0 / HEAD_LIN)
    out_ref[...] = (off * lax.rsqrt(spread + 0.00064) * gain_ref[...]).astype(BF16)


def joined(gates):
    gates = gates.astype(F32)
    return gates[0:2] + gates[2:4] + gates[4:6]


def att_kernel(
    place_ref, asked_ref, held_ref, keys_ref, out_ref, logit_ref, best_ref, sum_ref, *, rows
):
    z, y = place_ref[0] * 2 + place_ref[1], place_ref[2]
    count = asked_ref.shape[0]
    scale = HEAD_ATT ** (-0.5) * LOG2E
    best_ref[...] = jnp.full(best_ref.shape, NEG, F32)
    sum_ref[...] = jnp.zeros(sum_ref.shape, F32)
    ones = jnp.ones((rows, HEAD_ATT), BF16)
    base = joined(asked_ref[0, rows + WIDE : rows + WIDE + 16])[0:1, 0:1]

    def score(k, masked):
        key = keys_ref[k, 0:rows]
        drop = (base - joined(held_ref[k, WIDE : WIDE + 16])) * LOG2E
        drop = jnp.concatenate([drop[0:1], drop[1:2]], axis=1)
        for j in range(count):
            logits = dot(asked_ref[j, 0:rows], key, ((1,), (1,))) * scale + drop
            if masked:
                allowed = y * rows + iota(logits.shape, 1) <= j * rows + iota(logits.shape, 0)
                logits = jnp.where(allowed, logits, NEG)
            logit_ref[k, j] = logits
            top = functools.reduce(
                jnp.maximum, [logits[:, i : i + WIDE] for i in range(0, rows, WIDE)]
            )
            best_ref[j] = jnp.maximum(best_ref[j], top)

    def gather(*blocks):
        value = [jnp.concatenate([keys_ref[k, rows:], ones], axis=1) for k in blocks]
        for j in range(count):
            best = jnp.concatenate([best_ref[j]] * (rows // WIDE), axis=1)
            new = 0.0
            for k, v in zip(blocks, value):
                new = new + dot(jnp.exp2(logit_ref[k, j] - best).astype(BF16), v)
            sum_ref[j] = sum_ref[j] + new

    def score_many(i, carry):
        for k in range(5):
            score(5 * i + k, False)
        return carry

    def score_one(k, carry):
        score(k, False)
        return carry

    def gather_many(i, carry):
        gather(*(8 * i + k for k in range(8)))
        return carry

    def gather_one(k, carry):
        gather(k)
        return carry

    many = z // 5
    lax.fori_loop(0, many, score_many, 0)
    lax.fori_loop(5 * many, z, score_one, 0)
    score(z, True)
    for j in range(count):
        best = jnp.max(best_ref[j], axis=1, keepdims=True)
        best = jnp.where(best > 0.5 * NEG, best, 0.0)
        best_ref[j] = jnp.broadcast_to(best, best_ref.shape[1:])
    many = (z + 1) // 8
    lax.fori_loop(0, many, gather_many, 0)
    lax.fori_loop(8 * many, z + 1, gather_one, 0)
    eye = iota((WIDE, WIDE), 0) == iota((WIDE, WIDE), 1)
    for j in range(count):
        total = sum_ref[j, :, HEAD_ATT:]
        some = total > 0.0
        safe = jnp.where(some, total, 1.0)
        out_ref[j, 0:rows] = (sum_ref[j, :, 0:HEAD_ATT] / safe).astype(BF16)
        level = jnp.where(some, best_ref[j] + jnp.log(safe) * LOG2E, NEG)
        level = [
            jnp.sum(jnp.where(eye, level[i : i + WIDE], 0.0), axis=0, keepdims=True)
            for i in range(0, rows, WIDE)
        ]
        out_ref[j, rows:] = in_thirds(jnp.concatenate(level, axis=0))


def to_output(lin, att, wl_ref, wa_ref, core, out_ref):
    width = out_ref.shape[2]
    for j in range(out_ref.shape[0]):
        start = pl.multiple_of((2 * j + core) * width, width)
        mine = pl.ds(start, width)
        out_ref[j] = (dot(lin, wl_ref[:, mine]) + dot(att, wa_ref[:, mine])).astype(BF16)


def own_kernel(place_ref, att_ref, lin_ref, wl_ref, wa_ref, own_ref):
    to_output(lin_ref[...], att_ref[...], wl_ref, wa_ref, place_ref[3], own_ref)


def out_kernel(place_ref, parts_ref, lin_ref, gain_ref, wl_ref, wa_ref, other_ref, att_ref):
    count, rows = parts_ref.shape[0], lin_ref.shape[0]
    levels = [joined(parts_ref[j, rows:]) for j in range(count)]
    top = functools.reduce(jnp.maximum, levels)
    shares = [jnp.exp2(level - top) for level in levels]
    total = functools.reduce(jnp.add, shares)
    shares = jnp.concatenate([share / total for share in shares], axis=0).T
    raw = []
    for i in range(rows // WIDE):
        mine = slice(i * WIDE, (i + 1) * WIDE)
        raw.append(
            functools.reduce(
                jnp.add,
                [
                    shares[:, 2 * j + i : 2 * j + i + 1] * parts_ref[j, mine].astype(F32)
                    for j in range(count)
                ],
            )
        )
    raw = jnp.concatenate(raw, axis=0)
    size = jnp.mean(raw * raw, axis=1, keepdims=True)
    att = (raw * lax.rsqrt(size + 1e-6) * gain_ref[...]).astype(BF16)
    att_ref[...] = att
    to_output(lin_ref[...], att, wl_ref, wa_ref, 1 - place_ref[3], other_ref)


def to_partner(a, axis):
    return lax.ppermute(a, axis, [(0, 1), (1, 0)])


def smem():
    return pl.BlockSpec(memory_space=pltpu.SMEM)


def vmem():
    return pl.BlockSpec(memory_space=pltpu.VMEM)


def call(kernel, name, shapes, flops, size, mib, scratch=()):
    def run(*operands):
        many = isinstance(shapes, (list, tuple))
        return pl.pallas_call(
            kernel,
            name=name,
            out_shape=shapes,
            in_specs=[smem()] + [vmem()] * (len(operands) - 1),
            out_specs=[vmem()] * len(shapes) if many else vmem(),
            scratch_shapes=list(scratch),
            compiler_params=params(mib),
            cost_estimate=cost(flops, size),
        )(*operands)

    return run


def body(
    tokens,
    norm_gain,
    recv_weight,
    lin_key_weight,
    lin_value_weight,
    decay_down,
    decay_up,
    decay_log_bias,
    decay_shift,
    learn_rate,
    group_gain,
    initial_state,
    query_weight,
    att_key_weight,
    att_value_weight,
    gate_cache,
    att_gain,
    out_lin_weight,
    out_att_weight,
):
    rows = tokens.shape[0]
    nz, ny, nx = (lax.axis_size(axis) for axis in (KEYS, "near", "x"))
    model_width = norm_gain.shape[0]
    shape = jax.ShapeDtypeStruct
    place = jnp.stack([lax.axis_index(axis) for axis in SP + ("c",)]).astype(jnp.int32)
    gain = norm_gain.reshape(1, -1)

    place = pl.pallas_call(
        place_kernel,
        name="place",
        out_shape=shape(place.shape, jnp.int32),
        in_specs=[smem()],
        out_specs=smem(),
        cost_estimate=cost(10**10, 1 << 24),
    )(place)
    place, tokens = lax.optimization_barrier((place, tokens))
    own = lax.all_gather(tokens, "x")
    other = to_partner(own, "c")
    half = rows * model_width * 256
    part, squares = call(
        kv_part_kernel,
        "part",
        (shape((rows, 256), F32), shape((rows, WIDE), F32)),
        half,
        1 << 21,
        12,
    )(place, own, gain, att_key_weight, att_value_weight)
    kv = call(kv_kernel, "kv", shape((2 * rows, WIDE), BF16), half, 1 << 21, 12)(
        place, other, gain, att_key_weight, att_value_weight, part, squares
    )
    keys = lax.all_gather(kv, KEYS)

    extra = 16
    send, gates, reach, local = call(
        lin_kernel,
        "lin",
        (
            shape((ny, rows + WIDE + extra, WIDE), BF16),
            shape((extra, WIDE), BF16),
            shape((rows, WIDE), F32),
            shape((rows, WIDE), F32),
        ),
        4 * 10**9,
        1 << 22,
        24,
        scratch=[pltpu.VMEM((2, 2, rows, 2 * rows), F32)],
    )(
        place,
        own,
        other,
        gain,
        recv_weight,
        lin_key_weight,
        lin_value_weight,
        query_weight,
        decay_down.T,
        decay_up,
        decay_log_bias.reshape(1, -1),
        decay_shift,
        learn_rate.reshape(1, -1),
        gate_cache.reshape(rows // WIDE, WIDE),
    )
    asked = lax.all_to_all(send, "near", 0, 0, tiled=True)
    row_send, before = call(
        functools.partial(row_kernel, rows=rows),
        "row",
        (shape((WIDE + extra, WIDE), BF16), shape((2, WIDE, WIDE), F32)),
        10**8,
        1 << 20,
        12,
    )(place, asked, gates)
    held = lax.all_gather(row_send, KEYS)
    lin_mixed = call(mix_kernel, "mix", shape((rows, WIDE), BF16), 10**9, 1 << 20, 12)(
        place, initial_state, held, before, reach, local, group_gain.reshape(1, -1)
    )
    asked, lin_mixed = lax.optimization_barrier((asked, lin_mixed))
    found = call(
        functools.partial(att_kernel, rows=rows),
        "att",
        shape((ny, rows + extra, HEAD_ATT), BF16),
        ny * rows * nz * rows * 512,
        1 << 22,
        36,
        scratch=[
            pltpu.VMEM((nz, ny, rows, rows), F32),
            pltpu.VMEM((ny, rows, WIDE), F32),
            pltpu.VMEM((ny, rows, HEAD_ATT + WIDE), F32),
        ],
    )(place, asked, held, keys)
    parts = lax.all_to_all(found, "near", 0, 0, tiled=True)
    width = model_width // (2 * nx)
    tile = shape((nx, rows, width), BF16)
    theirs, att = call(
        out_kernel,
        "out",
        (tile, shape((rows, WIDE), BF16)),
        rows * 256 * model_width,
        1 << 21,
        12,
    )(place, parts, lin_mixed, att_gain.reshape(1, -1), out_lin_weight, out_att_weight)
    theirs = to_partner(theirs, "c")
    mine = call(own_kernel, "own", tile, rows * 256 * model_width, 1 << 21, 12)(
        place, att, lin_mixed, out_lin_weight, out_att_weight
    )
    pair = (mine.astype(F32) + theirs.astype(F32)).astype(BF16)
    tiles = lax.all_to_all(pair, "x", 0, 0, tiled=True)
    return jnp.sum(tiles.astype(F32), axis=0).astype(BF16)


def solution(mesh):
    sp, tp = mesh.shape["sp"], mesh.shape["tp"]
    cores = 2
    near = math.isqrt(sp) // 2 if sp > 16 else 2
    torus = Mesh(mesh.devices.reshape(sp // (2 * near), 2, near, tp // cores, cores), SP + TP)
    return jax.shard_map(
        body,
        mesh=torus,
        in_specs=(
            P(SP, TP),
            P(),
            P(None, TP),
            P(None, TP),
            P(None, TP),
            P(),
            P(None, TP),
            P(TP),
            P(SP, TP),
            P(TP),
            P(TP),
            P(TP, None, None),
            P(None, TP),
            P(None, TP),
            P(None, TP),
            P(SP, TP),
            P(TP),
            P(TP, None),
            P(TP, None),
        ),
        out_specs=P(SP, TP),
        check_vma=False,
    )
```

```python
import functools
import math

import jax
import jax.numpy as jnp
from jax import lax
from jax.experimental import pallas as pl
from jax.experimental.pallas import tpu as pltpu
from jax.sharding import Mesh
from jax.sharding import PartitionSpec as P

HEAD_LIN = 64
HEAD_ATT = 128
WIDE = 128
KEYS = ("zh", "zl")
SP = KEYS + ("near",)
TP = ("x", "c")
LOG2E = math.log2(math.e)
NEG = -1e30
F32 = jnp.float32
BF16 = jnp.bfloat16


def params(mib):
    return pltpu.CompilerParams(vmem_limit_bytes=mib * 1024 * 1024)


def cost(flops, size):
    return pl.CostEstimate(flops=flops, bytes_accessed=size, transcendentals=0)


def dot(a, b, dims=((1,), (0,))):
    return lax.dot_general(a, b, (dims, ((), ())), preferred_element_type=F32)


def parts_of(a):
    high = a.astype(BF16)
    return high, (a - high.astype(F32)).astype(BF16)


def dot3(a, b, dims=((1,), (0,))):
    ah, al = parts_of(a)
    bh, bl = parts_of(b)
    return dot(ah, bh, dims) + (dot(ah, bl, dims) + dot(al, bh, dims))


def dot2(a, b, dims=((1,), (0,))):
    ah, al = parts_of(a)
    return dot(ah, b, dims) + dot(al, b, dims)


def in_thirds(a):
    high, mid = parts_of(a)
    low = (a - high.astype(F32) - mid.astype(F32)).astype(BF16)
    return jnp.concatenate([high, mid, low, jnp.zeros((10, WIDE), BF16)], axis=0)


def iota(shape, dim):
    return lax.broadcasted_iota(jnp.int32, shape, dim)


def by_head(a):
    left = iota(a.shape, 1) < HEAD_LIN
    first = jnp.sum(jnp.where(left, a, 0.0), axis=1, keepdims=True)
    second = jnp.sum(jnp.where(left, 0.0, a), axis=1, keepdims=True)
    return jnp.where(left, first, second)


def scaled_pieces(place_ref, own_ref, other_ref, gain_ref):
    shards, rows, depth = own_ref.shape
    core = place_ref[3]
    scaled, squares = [], jnp.zeros((rows, depth), F32)
    for c, ref in enumerate((own_ref, other_ref)):
        for j in range(shards):
            start = pl.multiple_of((2 * j + (core if c == 0 else 1 - core)) * depth, depth)
            wide = ref[j].astype(F32)
            scaled.append(((wide * gain_ref[:, pl.ds(start, depth)]).astype(BF16), start))
            squares = squares + wide * wide
    mean = jnp.sum(squares, axis=1, keepdims=True) / (2 * shards * depth)
    return scaled, lax.rsqrt(mean + 1e-6)


def projected(scaled, inverse, *w_refs):
    total = 0.0
    for piece, start in scaled:
        weight = [w_ref[pl.ds(start, piece.shape[1])] for w_ref in w_refs]
        total = total + dot(piece, jnp.concatenate(weight, axis=1))
    return total * inverse


def spread_kernel(place_ref, tokens_ref, out_ref):
    tokens = tokens_ref[...]
    for j in range(out_ref.shape[0]):
        out_ref[j] = tokens


def kv_kernel(place_ref, own_ref, other_ref, gain_ref, wk_ref, wv_ref, out_ref):
    scaled, inverse = scaled_pieces(place_ref, own_ref, other_ref, gain_ref)
    rows = own_ref.shape[1]
    both = projected(scaled, inverse, wk_ref, wv_ref).astype(BF16)
    out_ref[0:rows] = both[:, :HEAD_ATT]
    out_ref[rows:] = both[:, HEAD_ATT:]


def spans(log_decay):
    rows = log_decay.shape[0]
    row = iota(log_decay.shape, 0)
    zero = jnp.zeros_like(log_decay)
    before = [None] + [pltpu.roll(log_decay, i, 0) for i in range(1, 8)]
    behind = [None] + [pltpu.roll(log_decay, rows - i, 0) for i in range(1, 8)]
    ahead, after = {1: zero}, {1: zero}
    for h in (2, 4, 8):
        place = row & (h - 1)
        a, b = zero, zero
        for i in range(1, h):
            a = a + jnp.where(place >= i, before[i], 0.0)
            b = b + jnp.where(place + i < h, behind[i], 0.0)
        ahead[h], after[h] = a, b
    h = 8
    while h < rows:
        shape = (rows // (2 * h), 2 * h, WIDE)
        a, b = ahead[h].reshape(shape), after[h].reshape(shape)
        step = log_decay.reshape(shape)
        left = a[:, h - 1 : h] + step[:, h - 1 : h]
        right = b[:, h : h + 1] + step[:, h : h + 1]
        a = jnp.concatenate([a[:, :h], a[:, h:] + left], axis=1)
        b = jnp.concatenate([b[:, :h] + right, b[:, h:]], axis=1)
        h *= 2
        ahead[h], after[h] = a.reshape(rows, WIDE), b.reshape(rows, WIDE)
    return ahead, after


def head_lanes(rows):
    lane = iota((rows, WIDE), 1)
    return [lane < HEAD_LIN, lane >= HEAD_LIN]


def below(h, half):
    tall = iota((half, half), 0)
    flat = iota((half, half), 1)
    level = h.bit_length()
    near = (tall >> level) == (flat >> level)
    return near & ((tall & h) != 0) & ((flat & h) == 0)


def fill_pairs(pairs_ref, asking, now, key, rate, ahead, after, step):
    rows = asking.shape[0]
    half = rows // 2
    row = iota((rows, WIDE), 0)
    heads = head_lanes(rows)
    eye = iota((half, half), 0) == iota((half, half), 1)
    blocks = slice(0, half), slice(half, rows)
    for m, source in enumerate((key, rate)):
        same = by_head(asking * source) if now else None
        for n in range(2):
            for b in range(2):
                cols = slice(m * rows + b * half, m * rows + (b + 1) * half)
                start = jnp.zeros((half, half), F32)
                if now:
                    column = same[blocks[b], n * HEAD_LIN : n * HEAD_LIN + 1]
                    start = jnp.where(eye, column, 0.0)
                pairs_ref[n, blocks[b], cols] = start
            cols = slice(m * rows + half, (m + 1) * rows)
            pairs_ref[n, blocks[0], cols] = jnp.zeros((half, half), F32)
    h = 1
    while h < rows:
        late = (row & h) != 0
        reach = ahead[h] if step is None else ahead[h] + step
        left = asking * jnp.where(late, jnp.exp(reach), 0.0)
        left = [jnp.where(mine, left, 0.0).astype(BF16) for mine in heads]
        from_s = jnp.where(late, 0.0, jnp.exp(after[h]))
        right = (key * from_s).astype(BF16), (rate * from_s).astype(BF16)
        for b in range(2) if h < half else (1,):
            c = b if h < half else 0
            product = dot(
                jnp.concatenate([a[blocks[b]] for a in left], axis=0),
                jnp.concatenate([a[blocks[c]] for a in right], axis=0),
                ((1,), (1,)),
            )
            for n in range(2):
                for m in range(2):
                    cols = slice(m * rows + c * half, m * rows + (c + 1) * half)
                    new = product[n * half : (n + 1) * half, m * half : (m + 1) * half]
                    if h < half:
                        new = jnp.where(below(h, half), new, pairs_ref[n, blocks[b], cols])
                    pairs_ref[n, blocks[b], cols] = new
        h *= 2


def lin_kernel(
    place_ref,
    own_ref,
    other_ref,
    gain_ref,
    wr_ref,
    wk_ref,
    wv_ref,
    wq_ref,
    down_ref,
    up_ref,
    bias_ref,
    shift_ref,
    rate_ref,
    gate_ref,
    send_ref,
    gates_ref,
    rows_ref,
    value_ref,
    pairs_ref,
):
    scaled, inverse = scaled_pieces(place_ref, own_ref, other_ref, gain_ref)
    rows = shift_ref.shape[0]
    both = projected(scaled, inverse, wr_ref, wk_ref).astype(BF16)
    recv, key = both[:, :WIDE].astype(F32), both[:, WIDE:].astype(F32)
    both = projected(scaled, inverse, wv_ref, wq_ref).astype(BF16)
    value = both[:, :WIDE]
    send_ref[0, 0:rows] = both[:, WIDE:]
    low = 0.0
    for piece, start in scaled:
        low = low + dot(piece, down_ref[:, pl.ds(start, piece.shape[1])], ((1,), (1,)))
    low = (low * inverse).astype(BF16).astype(F32)
    exponent = bias_ref[...] + shift_ref[...] + dot(jnp.tanh(low).astype(BF16), up_ref[...])
    log_decay = -jnp.exp(exponent)
    unit = key * lax.rsqrt(by_head(key * key) + 1e-6)
    rate = unit * rate_ref[...]

    ahead, after = spans(log_decay)
    half = rows // 2
    heads = head_lanes(rows)
    blocks = slice(0, half), slice(half, rows)
    eye = iota((half, half), 0) == iota((half, half), 1)
    fill_pairs(pairs_ref, unit, None, key, rate, ahead, after, None)

    solved = {}
    h = 1
    while h < half:
        here = below(h, half)
        for n in range(2):
            for b in range(2):
                cols = slice(rows + b * half, rows + (b + 1) * half)
                links = jnp.where(here, pairs_ref[n, blocks[b], cols], 0.0)
                if h == 1:
                    solved[n, b] = jnp.where(eye, 1.0, 0.0) - links
                else:
                    step = dot3(links, solved[n, b])
                    solved[n, b] = solved[n, b] - dot3(solved[n, b], step)
        h *= 2

    full_u = unit * jnp.exp(ahead[rows])
    tail = jnp.exp(after[rows])
    full_k = key * tail
    full_r = rate * tail
    moved = []
    for n in range(2):
        add = dot2(pairs_ref[n, :, :rows], value)
        source = jnp.where(heads[n], full_u, pltpu.roll(add, HEAD_LIN, 1))
        first = dot3(solved[n, 0], source[:half])
        later = source[half:] - dot3(pairs_ref[n, half:, rows : rows + half], first)
        along = jnp.concatenate([first, dot3(solved[n, 1], later)], axis=0)
        rows_ref[n] = along
        moved.append(dot3(along, full_r, ((0,), (0,))))
    for i, kept in enumerate((recv, key, rate, log_decay)):
        rows_ref[2 + i] = kept
    value_ref[...] = value

    lane = iota((WIDE, WIDE), 1)
    row = iota((WIDE, WIDE), 0)
    same = (lane < HEAD_LIN) == (row < HEAD_LIN)
    added = pltpu.roll(dot2(full_k, value, ((0,), (0,))).T, HEAD_LIN, 0)
    last = jnp.exp(ahead[rows][rows - 1 : rows] + log_decay[rows - 1 : rows]) - 1.0
    packed = jnp.where(same, jnp.where(lane == row, last, 0.0), added)
    packed = packed - jnp.where(lane < HEAD_LIN, moved[0], moved[1])
    send_ref[0, rows : rows + WIDE] = packed.astype(BF16)
    gates = in_thirds(gate_ref[...])
    send_ref[0, rows + WIDE :] = gates
    gates_ref[...] = gates
    whole = send_ref[0]
    for j in range(1, send_ref.shape[0]):
        send_ref[j] = whole


def reach_kernel(place_ref, rows_ref, value_ref, reach_ref, local_ref, pairs_ref):
    recv, key, rate, log_decay = (rows_ref[2 + i] for i in range(4))
    rows = recv.shape[0]
    ahead, after = spans(log_decay)
    heads = head_lanes(rows)
    fill_pairs(pairs_ref, recv, True, key, rate, ahead, after, log_decay)
    full_q = recv * jnp.exp(ahead[rows] + log_decay)
    value = value_ref[...]
    reach, local = [], []
    for n in range(2):
        taken = dot3(pairs_ref[n, :, rows:], rows_ref[n])
        reach.append(full_q - taken)
        local.append(dot2(pairs_ref[n, :, :rows], value) - pltpu.roll(taken, HEAD_LIN, 1))
    reach_ref[...] = jnp.where(heads[0], reach[0], reach[1])
    local_ref[...] = jnp.where(heads[0], local[0], local[1])


def unpacked(packed):
    packed = packed.astype(F32)
    lane = iota((WIDE, WIDE), 1)
    row = iota((WIDE, WIDE), 0)
    same = (lane < HEAD_LIN) == (row < HEAD_LIN)
    return jnp.where(same, packed, 0.0), jnp.where(same, pltpu.roll(packed, HEAD_LIN, 0), 0.0)


def repacked(total):
    lane = iota((WIDE, WIDE), 1)
    row = iota((WIDE, WIDE), 0)
    same = (lane < HEAD_LIN) == (row < HEAD_LIN)
    return jnp.where(same, total[0], pltpu.roll(total[1], HEAD_LIN, 0)).astype(BF16)


def chained(first, second):
    return (
        first[0] + second[0] + dot3(first[0], second[0]),
        first[1] + second[1] + dot3(first[1], second[0]),
    )


def row_kernel(place_ref, gathered_ref, gates_ref, send_ref, before_ref, *, rows):
    near = place_ref[2]
    count = gathered_ref.shape[0]
    total = mine = jnp.zeros((WIDE, WIDE), F32), jnp.zeros((WIDE, WIDE), F32)
    for j in range(count):
        mine = tuple(jnp.where(near == j, t, m) for t, m in zip(total, mine))
        here = unpacked(gathered_ref[j, rows : rows + WIDE])
        total = chained(total, here) if j else here
    before_ref[0], before_ref[1] = mine
    send_ref[0:WIDE] = repacked(total)
    send_ref[WIDE:] = gates_ref[...]


def mix_kernel(place_ref, state_ref, gathered_ref, before_ref, reach_ref, local_ref, gain_ref, out_ref):
    none = jnp.zeros((HEAD_LIN, HEAD_LIN), F32)
    state = jnp.concatenate(
        [
            jnp.concatenate([state_ref[0], none], axis=1),
            jnp.concatenate([none, state_ref[1]], axis=1),
        ],
        axis=0,
    )

    def step(k, state):
        packed = gathered_ref[k]
        moved, added = unpacked(packed[0:WIDE])
        return state + dot2(state, moved.astype(BF16)) + added

    state = lax.fori_loop(0, place_ref[0] * 2 + place_ref[1], step, state)
    state = state + dot3(state, before_ref[0]) + before_ref[1]
    raw = dot3(reach_ref[...], state, ((1,), (1,))) + local_ref[...]
    off = raw - by_head(raw) * (1.0 / HEAD_LIN)
    spread = by_head(off * off) * (1.0 / HEAD_LIN)
    out_ref[...] = (off * lax.rsqrt(spread + 0.00064) * gain_ref[...]).astype(BF16)


def joined(gates):
    gates = gates.astype(F32)
    return gates[0:2] + gates[2:4] + gates[4:6]


def att_kernel(
    place_ref, asked_ref, held_ref, keys_ref, out_ref, logit_ref, best_ref, sum_ref, *, rows
):
    z, y = place_ref[0] * 2 + place_ref[1], place_ref[2]
    count = asked_ref.shape[0]
    scale = HEAD_ATT ** (-0.5) * LOG2E
    best_ref[...] = jnp.full(best_ref.shape, NEG, F32)
    sum_ref[...] = jnp.zeros(sum_ref.shape, F32)
    ones = jnp.ones((rows, HEAD_ATT), BF16)
    base = joined(asked_ref[0, rows + WIDE : rows + WIDE + 16])[0:1, 0:1]

    def score(k, masked):
        key = keys_ref[k, 0:rows]
        drop = (base - joined(held_ref[k, WIDE : WIDE + 16])) * LOG2E
        drop = jnp.concatenate([drop[0:1], drop[1:2]], axis=1)
        for j in range(count):
            logits = dot(asked_ref[j, 0:rows], key, ((1,), (1,))) * scale + drop
            if masked:
                allowed = y * rows + iota(logits.shape, 1) <= j * rows + iota(logits.shape, 0)
                logits = jnp.where(allowed, logits, NEG)
            logit_ref[k, j] = logits
            top = functools.reduce(
                jnp.maximum, [logits[:, i : i + WIDE] for i in range(0, rows, WIDE)]
            )
            best_ref[j] = jnp.maximum(best_ref[j], top)

    def gather(*blocks):
        value = [jnp.concatenate([keys_ref[k, rows:], ones], axis=1) for k in blocks]
        for j in range(count):
            best = jnp.concatenate([best_ref[j]] * (rows // WIDE), axis=1)
            new = 0.0
            for k, v in zip(blocks, value):
                new = new + dot(jnp.exp2(logit_ref[k, j] - best).astype(BF16), v)
            sum_ref[j] = sum_ref[j] + new

    def score_many(i, carry):
        for k in range(3):
            score(3 * i + k, False)
        return carry

    def score_one(k, carry):
        score(k, False)
        return carry

    def gather_many(i, carry):
        gather(*(4 * i + k for k in range(4)))
        return carry

    def gather_one(k, carry):
        gather(k)
        return carry

    many = z // 3
    lax.fori_loop(0, many, score_many, 0)
    lax.fori_loop(3 * many, z, score_one, 0)
    score(z, True)
    for j in range(count):
        best = jnp.max(best_ref[j], axis=1, keepdims=True)
        best = jnp.where(best > 0.5 * NEG, best, 0.0)
        best_ref[j] = jnp.broadcast_to(best, best_ref.shape[1:])
    many = (z + 1) // 4
    lax.fori_loop(0, many, gather_many, 0)
    lax.fori_loop(4 * many, z + 1, gather_one, 0)
    eye = iota((WIDE, WIDE), 0) == iota((WIDE, WIDE), 1)
    for j in range(count):
        total = sum_ref[j, :, HEAD_ATT:]
        some = total > 0.0
        safe = jnp.where(some, total, 1.0)
        out_ref[j, 0:rows] = (sum_ref[j, :, 0:HEAD_ATT] / safe).astype(BF16)
        level = jnp.where(some, best_ref[j] + jnp.log(safe) * LOG2E, NEG)
        level = [
            jnp.sum(jnp.where(eye, level[i : i + WIDE], 0.0), axis=0, keepdims=True)
            for i in range(0, rows, WIDE)
        ]
        out_ref[j, rows:] = in_thirds(jnp.concatenate(level, axis=0))


def out_kernel(place_ref, parts_ref, lin_ref, gain_ref, wl_ref, wa_ref, own_ref, other_ref):
    count, rows = parts_ref.shape[0], lin_ref.shape[0]
    core = place_ref[3]
    levels = [joined(parts_ref[j, rows:]) for j in range(count)]
    top = functools.reduce(jnp.maximum, levels)
    shares = [jnp.exp2(level - top) for level in levels]
    total = functools.reduce(jnp.add, shares)
    shares = jnp.concatenate([share / total for share in shares], axis=0).T
    raw = []
    for i in range(rows // WIDE):
        mine = slice(i * WIDE, (i + 1) * WIDE)
        raw.append(
            functools.reduce(
                jnp.add,
                [
                    shares[:, 2 * j + i : 2 * j + i + 1] * parts_ref[j, mine].astype(F32)
                    for j in range(count)
                ],
            )
        )
    raw = jnp.concatenate(raw, axis=0)
    size = jnp.mean(raw * raw, axis=1, keepdims=True)
    att = (raw * lax.rsqrt(size + 1e-6) * gain_ref[...]).astype(BF16)
    lin = lin_ref[...]
    width = own_ref.shape[2]
    for c, ref in enumerate((own_ref, other_ref)):
        for j in range(ref.shape[0]):
            start = pl.multiple_of((2 * j + (core if c == 0 else 1 - core)) * width, width)
            mine = pl.ds(start, width)
            ref[j] = (dot(lin, wl_ref[:, mine]) + dot(att, wa_ref[:, mine])).astype(BF16)


def to_partner(a, axis):
    return lax.ppermute(a, axis, [(0, 1), (1, 0)])


def smem():
    return pl.BlockSpec(memory_space=pltpu.SMEM)


def vmem():
    return pl.BlockSpec(memory_space=pltpu.VMEM)


def call(kernel, name, shapes, flops, size, mib, scratch=()):
    def run(*operands):
        many = isinstance(shapes, (list, tuple))
        return pl.pallas_call(
            kernel,
            name=name,
            out_shape=shapes,
            in_specs=[smem()] + [vmem()] * (len(operands) - 1),
            out_specs=[vmem()] * len(shapes) if many else vmem(),
            scratch_shapes=list(scratch),
            compiler_params=params(mib),
            cost_estimate=cost(flops, size),
        )(*operands)

    return run


def body(
    tokens,
    norm_gain,
    recv_weight,
    lin_key_weight,
    lin_value_weight,
    decay_down,
    decay_up,
    decay_log_bias,
    decay_shift,
    learn_rate,
    group_gain,
    initial_state,
    query_weight,
    att_key_weight,
    att_value_weight,
    gate_cache,
    att_gain,
    out_lin_weight,
    out_att_weight,
):
    rows = tokens.shape[0]
    nz, ny, nx = (lax.axis_size(axis) for axis in (KEYS, "near", "x"))
    model_width = norm_gain.shape[0]
    shape = jax.ShapeDtypeStruct
    place = jnp.stack([lax.axis_index(axis) for axis in SP + ("c",)]).astype(jnp.int32)
    gain = norm_gain.reshape(1, -1)

    copies = call(spread_kernel, "spread", shape((nx, *tokens.shape), BF16), 10**10, 1 << 24, 4)(
        place, tokens
    )
    own = lax.all_to_all(copies, "x", 0, 0, tiled=True)
    other = to_partner(own, "c")
    extra = 16
    send, gates, kept, value = call(
        lin_kernel,
        "lin",
        (
            shape((ny, rows + WIDE + extra, WIDE), BF16),
            shape((extra, WIDE), BF16),
            shape((6, rows, WIDE), F32),
            shape((rows, WIDE), BF16),
        ),
        4 * 10**9,
        1 << 22,
        24,
        scratch=[pltpu.VMEM((2, rows, 2 * rows), F32)],
    )(
        place,
        own,
        other,
        gain,
        recv_weight,
        lin_key_weight,
        lin_value_weight,
        query_weight,
        decay_down.T,
        decay_up,
        decay_log_bias.reshape(1, -1),
        decay_shift,
        learn_rate.reshape(1, -1),
        gate_cache.reshape(rows // WIDE, WIDE),
    )
    send, own, other = lax.optimization_barrier((send, own, other))
    asked = lax.all_to_all(send, "near", 0, 0, tiled=True)
    kv = call(
        kv_kernel, "kv", shape((2 * rows, WIDE), BF16), 2 * rows * model_width * 256, 1 << 21, 12
    )(place, own, other, gain, att_key_weight, att_value_weight)
    kv, kept = lax.optimization_barrier((kv, kept))
    keys = lax.all_gather(kv, KEYS)
    reach, local = call(
        reach_kernel,
        "reach",
        (shape((rows, WIDE), F32), shape((rows, WIDE), F32)),
        2 * 10**9,
        1 << 21,
        16,
        scratch=[pltpu.VMEM((2, rows, 2 * rows), F32)],
    )(place, kept, value)
    row_send, before = call(
        functools.partial(row_kernel, rows=rows),
        "row",
        (shape((WIDE + extra, WIDE), BF16), shape((2, WIDE, WIDE), F32)),
        10**8,
        1 << 20,
        12,
    )(place, asked, gates)
    held = lax.all_gather(row_send, KEYS)
    lin_mixed = call(mix_kernel, "mix", shape((rows, WIDE), BF16), 10**9, 1 << 20, 12)(
        place, initial_state, held, before, reach, local, group_gain.reshape(1, -1)
    )
    asked, lin_mixed = lax.optimization_barrier((asked, lin_mixed))
    found = call(
        functools.partial(att_kernel, rows=rows),
        "att",
        shape((ny, rows + extra, HEAD_ATT), BF16),
        ny * rows * nz * rows * 512,
        1 << 22,
        36,
        scratch=[
            pltpu.VMEM((nz, ny, rows, rows), F32),
            pltpu.VMEM((ny, rows, WIDE), F32),
            pltpu.VMEM((ny, rows, HEAD_ATT + WIDE), F32),
        ],
    )(place, asked, held, keys)
    parts = lax.all_to_all(found, "near", 0, 0, tiled=True)
    width = model_width // (2 * nx)
    tile = shape((nx, rows, width), BF16)
    mine, theirs = call(
        out_kernel, "out", (tile, tile), 2 * rows * 256 * model_width, 1 << 21, 12
    )(place, parts, lin_mixed, att_gain.reshape(1, -1), out_lin_weight, out_att_weight)
    pair = (mine.astype(F32) + to_partner(theirs, "c").astype(F32)).astype(BF16)
    tiles = lax.all_to_all(pair, "x", 0, 0, tiled=True)
    return jnp.sum(tiles.astype(F32), axis=0).astype(BF16)


def solution(mesh):
    sp, tp = mesh.shape["sp"], mesh.shape["tp"]
    cores = 2
    near = math.isqrt(sp) if sp > 16 else 2
    torus = Mesh(mesh.devices.reshape(sp // (2 * near), 2, near, tp // cores, cores), SP + TP)
    return jax.shard_map(
        body,
        mesh=torus,
        in_specs=(
            P(SP, TP),
            P(),
            P(None, TP),
            P(None, TP),
            P(None, TP),
            P(),
            P(None, TP),
            P(TP),
            P(SP, TP),
            P(TP),
            P(TP),
            P(TP, None, None),
            P(None, TP),
            P(None, TP),
            P(None, TP),
            P(SP, TP),
            P(TP),
            P(TP, None),
            P(TP, None),
        ),
        out_specs=P(SP, TP),
        check_vma=False,
    )
```

```python
import functools
import math

import jax
import jax.numpy as jnp
from jax import lax
from jax.experimental import pallas as pl
from jax.experimental.pallas import tpu as pltpu
from jax.sharding import Mesh
from jax.sharding import PartitionSpec as P

HEAD_LIN = 64
HEAD_ATT = 128
WIDE = 128
KEYS = ("zh", "zl")
SP = KEYS + ("near",)
TP = ("x", "c")
LOG2E = math.log2(math.e)
NEG = -1e30
F32 = jnp.float32
BF16 = jnp.bfloat16


def params(mib):
    return pltpu.CompilerParams(vmem_limit_bytes=mib * 1024 * 1024)


def cost(flops, size):
    return pl.CostEstimate(flops=flops, bytes_accessed=size, transcendentals=0)


def dot(a, b, dims=((1,), (0,))):
    return lax.dot_general(a, b, (dims, ((), ())), preferred_element_type=F32)


def parts_of(a):
    high = a.astype(BF16)
    return high, (a - high.astype(F32)).astype(BF16)


def dot3(a, b, dims=((1,), (0,))):
    ah, al = parts_of(a)
    bh, bl = parts_of(b)
    return dot(ah, bh, dims) + (dot(ah, bl, dims) + dot(al, bh, dims))


def dot2(a, b, dims=((1,), (0,))):
    ah, al = parts_of(a)
    return dot(ah, b, dims) + dot(al, b, dims)


def in_thirds(a):
    high, mid = parts_of(a)
    low = (a - high.astype(F32) - mid.astype(F32)).astype(BF16)
    return jnp.concatenate([high, mid, low, jnp.zeros((10, WIDE), BF16)], axis=0)


def iota(shape, dim):
    return lax.broadcasted_iota(jnp.int32, shape, dim)


def by_head(a):
    left = iota(a.shape, 1) < HEAD_LIN
    first = jnp.sum(jnp.where(left, a, 0.0), axis=1, keepdims=True)
    second = jnp.sum(jnp.where(left, 0.0, a), axis=1, keepdims=True)
    return jnp.where(left, first, second)


def scaled_part(ref, gain_ref, core):
    shards, rows, depth = ref.shape
    scaled, squares = [], jnp.zeros((rows, depth), F32)
    for j in range(shards):
        start = pl.multiple_of((2 * j + core) * depth, depth)
        wide = ref[j].astype(F32)
        scaled.append(((wide * gain_ref[:, pl.ds(start, depth)]).astype(BF16), start))
        squares = squares + wide * wide
    return scaled, jnp.sum(squares, axis=1, keepdims=True)


def inverse_rms(squares, gain_ref):
    return lax.rsqrt(squares / gain_ref.shape[1] + 1e-6)


def scaled_pieces(place_ref, own_ref, other_ref, gain_ref):
    core = place_ref[3]
    own, own_squares = scaled_part(own_ref, gain_ref, core)
    other, other_squares = scaled_part(other_ref, gain_ref, 1 - core)
    return own + other, inverse_rms(own_squares + other_squares, gain_ref)


def projected(scaled, inverse, *w_refs):
    total = 0.0
    for piece, start in scaled:
        weight = [w_ref[pl.ds(start, piece.shape[1])] for w_ref in w_refs]
        total = total + dot(piece, jnp.concatenate(weight, axis=1))
    return total * inverse


def spread_kernel(place_ref, tokens_ref, out_ref):
    tokens = tokens_ref[...]
    for j in range(out_ref.shape[0]):
        out_ref[j] = tokens


def kv_part_kernel(place_ref, own_ref, gain_ref, wk_ref, wv_ref, part_ref, squares_ref):
    scaled, squares = scaled_part(own_ref, gain_ref, place_ref[3])
    part_ref[...] = projected(scaled, 1.0, wk_ref, wv_ref)
    squares_ref[...] = jnp.broadcast_to(squares, squares_ref.shape)


def kv_kernel(place_ref, other_ref, gain_ref, wk_ref, wv_ref, part_ref, squares_ref, out_ref):
    scaled, squares = scaled_part(other_ref, gain_ref, 1 - place_ref[3])
    rows = other_ref.shape[1]
    inverse = inverse_rms(squares + squares_ref[:, 0:1], gain_ref)
    both = projected(scaled, 1.0, wk_ref, wv_ref) + part_ref[...]
    both = (both * inverse).astype(BF16)
    out_ref[0:rows] = both[:, :HEAD_ATT]
    out_ref[rows:] = both[:, HEAD_ATT:]


def spans(log_decay):
    rows = log_decay.shape[0]
    row = iota(log_decay.shape, 0)
    zero = jnp.zeros_like(log_decay)
    before = [None] + [pltpu.roll(log_decay, i, 0) for i in range(1, 8)]
    behind = [None] + [pltpu.roll(log_decay, rows - i, 0) for i in range(1, 8)]
    ahead, after = {1: zero}, {1: zero}
    for h in (2, 4, 8):
        place = row & (h - 1)
        a, b = zero, zero
        for i in range(1, h):
            a = a + jnp.where(place >= i, before[i], 0.0)
            b = b + jnp.where(place + i < h, behind[i], 0.0)
        ahead[h], after[h] = a, b
    h = 8
    while h < rows:
        shape = (rows // (2 * h), 2 * h, WIDE)
        a, b = ahead[h].reshape(shape), after[h].reshape(shape)
        step = log_decay.reshape(shape)
        left = a[:, h - 1 : h] + step[:, h - 1 : h]
        right = b[:, h : h + 1] + step[:, h : h + 1]
        a = jnp.concatenate([a[:, :h], a[:, h:] + left], axis=1)
        b = jnp.concatenate([b[:, :h] + right, b[:, h:]], axis=1)
        h *= 2
        ahead[h], after[h] = a.reshape(rows, WIDE), b.reshape(rows, WIDE)
    return ahead, after


def lin_kernel(
    place_ref,
    own_ref,
    other_ref,
    gain_ref,
    wr_ref,
    wk_ref,
    wv_ref,
    wq_ref,
    down_ref,
    up_ref,
    bias_ref,
    shift_ref,
    rate_ref,
    gate_ref,
    send_ref,
    gates_ref,
    reach_ref,
    local_ref,
    pairs_ref,
):
    scaled, inverse = scaled_pieces(place_ref, own_ref, other_ref, gain_ref)
    rows = shift_ref.shape[0]
    both = projected(scaled, inverse, wr_ref, wk_ref).astype(BF16)
    recv, key = both[:, :WIDE].astype(F32), both[:, WIDE:].astype(F32)
    both = projected(scaled, inverse, wv_ref, wq_ref).astype(BF16)
    value = both[:, :WIDE]
    send_ref[0, 0:rows] = both[:, WIDE:]
    low = 0.0
    for piece, start in scaled:
        low = low + dot(piece, down_ref[:, pl.ds(start, piece.shape[1])], ((1,), (1,)))
    low = (low * inverse).astype(BF16).astype(F32)
    exponent = bias_ref[...] + shift_ref[...] + dot(jnp.tanh(low).astype(BF16), up_ref[...])
    log_decay = -jnp.exp(exponent)
    unit = key * lax.rsqrt(by_head(key * key) + 1e-6)
    rate = unit * rate_ref[...]

    ahead, after = spans(log_decay)
    half = rows // 2
    lane = iota((rows, WIDE), 1)
    row = iota((rows, WIDE), 0)
    tall = iota((half, half), 0)
    flat = iota((half, half), 1)
    heads = [lane < HEAD_LIN, lane >= HEAD_LIN]
    eye = tall == flat
    blocks = slice(0, half), slice(half, rows)

    def of_heads(a):
        return [jnp.where(mine, a, 0.0).astype(BF16) for mine in heads]

    def below(h):
        level = h.bit_length()
        near = (tall >> level) == (flat >> level)
        return near & ((tall & h) != 0) & ((flat & h) == 0)

    for m, source in enumerate((key, rate)):
        now = by_head(recv * source)
        for n in range(2):
            for b in range(2):
                cols = slice(m * rows + b * half, m * rows + (b + 1) * half)
                same_row = now[blocks[b], n * HEAD_LIN : n * HEAD_LIN + 1]
                pairs_ref[n, 1, blocks[b], cols] = jnp.where(eye, same_row, 0.0)
                pairs_ref[n, 0, blocks[b], cols] = jnp.zeros((half, half), F32)
            cols = slice(m * rows + half, (m + 1) * rows)
            for k in range(2):
                pairs_ref[n, k, blocks[0], cols] = jnp.zeros((half, half), F32)
    h = 1
    while h < rows:
        late = (row & h) != 0
        to_u = jnp.where(late, jnp.exp(ahead[h]), 0.0)
        to_q = jnp.where(late, jnp.exp(ahead[h] + log_decay), 0.0)
        from_s = jnp.where(late, 0.0, jnp.exp(after[h]))
        right = (key * from_s).astype(BF16), (rate * from_s).astype(BF16)
        left = of_heads(unit * to_u) + of_heads(recv * to_q)
        for b in range(2) if h < half else (1,):
            c = b if h < half else 0
            product = dot(
                jnp.concatenate([a[blocks[b]] for a in left], axis=0),
                jnp.concatenate([a[blocks[c]] for a in right], axis=0),
                ((1,), (1,)),
            )
            for k in range(2):
                for n in range(2):
                    for m in range(2):
                        cols = slice(m * rows + c * half, m * rows + (c + 1) * half)
                        new = product[
                            (2 * k + n) * half : (2 * k + n + 1) * half,
                            m * half : (m + 1) * half,
                        ]
                        if h < half:
                            new = jnp.where(below(h), new, pairs_ref[n, k, blocks[b], cols])
                        pairs_ref[n, k, blocks[b], cols] = new
        h *= 2

    solved = {}
    h = 1
    while h < half:
        here = below(h)
        for n in range(2):
            for b in range(2):
                cols = slice(rows + b * half, rows + (b + 1) * half)
                links = jnp.where(here, pairs_ref[n, 0, blocks[b], cols], 0.0)
                if h == 1:
                    solved[n, b] = jnp.where(eye, 1.0, 0.0) - links
                else:
                    step = dot3(links, solved[n, b])
                    solved[n, b] = solved[n, b] - dot3(solved[n, b], step)
        h *= 2

    full_u = unit * jnp.exp(ahead[rows])
    full_q = recv * jnp.exp(ahead[rows] + log_decay)
    tail = jnp.exp(after[rows])
    full_k = key * tail
    full_r = rate * tail
    reach, local, moved = [], [], []
    for n in range(2):
        add = dot2(pairs_ref[n, 0, :, :rows], value)
        source = jnp.where(heads[n], full_u, pltpu.roll(add, HEAD_LIN, 1))
        first = dot3(solved[n, 0], source[:half])
        later = source[half:] - dot3(pairs_ref[n, 0, half:, rows : rows + half], first)
        along = jnp.concatenate([first, dot3(solved[n, 1], later)], axis=0)
        taken = dot3(pairs_ref[n, 1, :, rows:], along)
        reach.append(full_q - taken)
        local.append(dot2(pairs_ref[n, 1, :, :rows], value) - pltpu.roll(taken, HEAD_LIN, 1))
        moved.append(dot3(along, full_r, ((0,), (0,))))
    reach_ref[...] = jnp.where(heads[0], reach[0], reach[1])
    local_ref[...] = jnp.where(heads[0], local[0], local[1])

    lane = iota((WIDE, WIDE), 1)
    row = iota((WIDE, WIDE), 0)
    same = (lane < HEAD_LIN) == (row < HEAD_LIN)
    added = pltpu.roll(dot2(full_k, value, ((0,), (0,))).T, HEAD_LIN, 0)
    last = jnp.exp(ahead[rows][rows - 1 : rows] + log_decay[rows - 1 : rows]) - 1.0
    packed = jnp.where(same, jnp.where(lane == row, last, 0.0), added)
    packed = packed - jnp.where(lane < HEAD_LIN, moved[0], moved[1])
    send_ref[0, rows : rows + WIDE] = packed.astype(BF16)
    gates = in_thirds(gate_ref[...])
    send_ref[0, rows + WIDE :] = gates
    gates_ref[...] = gates
    whole = send_ref[0]
    for j in range(1, send_ref.shape[0]):
        send_ref[j] = whole


def unpacked(packed):
    packed = packed.astype(F32)
    lane = iota((WIDE, WIDE), 1)
    row = iota((WIDE, WIDE), 0)
    same = (lane < HEAD_LIN) == (row < HEAD_LIN)
    return jnp.where(same, packed, 0.0), jnp.where(same, pltpu.roll(packed, HEAD_LIN, 0), 0.0)


def repacked(total):
    lane = iota((WIDE, WIDE), 1)
    row = iota((WIDE, WIDE), 0)
    same = (lane < HEAD_LIN) == (row < HEAD_LIN)
    return jnp.where(same, total[0], pltpu.roll(total[1], HEAD_LIN, 0)).astype(BF16)


def chained(first, second):
    return (
        first[0] + second[0] + dot3(first[0], second[0]),
        first[1] + second[1] + dot3(first[1], second[0]),
    )


def row_kernel(place_ref, gathered_ref, gates_ref, send_ref, before_ref, *, rows):
    near = place_ref[2]
    count = gathered_ref.shape[0]
    total = mine = jnp.zeros((WIDE, WIDE), F32), jnp.zeros((WIDE, WIDE), F32)
    for j in range(count):
        mine = tuple(jnp.where(near == j, t, m) for t, m in zip(total, mine))
        here = unpacked(gathered_ref[j, rows : rows + WIDE])
        total = chained(total, here) if j else here
    before_ref[0], before_ref[1] = mine
    send_ref[0:WIDE] = repacked(total)
    send_ref[WIDE:] = gates_ref[...]


def mix_kernel(place_ref, state_ref, gathered_ref, before_ref, reach_ref, local_ref, gain_ref, out_ref):
    none = jnp.zeros((HEAD_LIN, HEAD_LIN), F32)
    state = jnp.concatenate(
        [
            jnp.concatenate([state_ref[0], none], axis=1),
            jnp.concatenate([none, state_ref[1]], axis=1),
        ],
        axis=0,
    )

    def step(k, state):
        packed = gathered_ref[k]
        moved, added = unpacked(packed[0:WIDE])
        return state + dot2(state, moved.astype(BF16)) + added

    state = lax.fori_loop(0, place_ref[0] * 2 + place_ref[1], step, state)
    state = state + dot3(state, before_ref[0]) + before_ref[1]
    raw = dot3(reach_ref[...], state, ((1,), (1,))) + local_ref[...]
    off = raw - by_head(raw) * (1.0 / HEAD_LIN)
    spread = by_head(off * off) * (1.0 / HEAD_LIN)
    out_ref[...] = (off * lax.rsqrt(spread + 0.00064) * gain_ref[...]).astype(BF16)


def joined(gates):
    gates = gates.astype(F32)
    return gates[0:2] + gates[2:4] + gates[4:6]


def att_kernel(
    place_ref, asked_ref, held_ref, keys_ref, out_ref, logit_ref, best_ref, sum_ref, *, rows
):
    z, y = place_ref[0] * 2 + place_ref[1], place_ref[2]
    count = asked_ref.shape[0]
    scale = HEAD_ATT ** (-0.5) * LOG2E
    best_ref[...] = jnp.full(best_ref.shape, NEG, F32)
    sum_ref[...] = jnp.zeros(sum_ref.shape, F32)
    ones = jnp.ones((rows, HEAD_ATT), BF16)
    base = joined(asked_ref[0, rows + WIDE : rows + WIDE + 16])[0:1, 0:1]

    def score(k, masked):
        key = keys_ref[k, 0:rows]
        drop = (base - joined(held_ref[k, WIDE : WIDE + 16])) * LOG2E
        drop = jnp.concatenate([drop[0:1], drop[1:2]], axis=1)
        for j in range(count):
            logits = dot(asked_ref[j, 0:rows], key, ((1,), (1,))) * scale + drop
            if masked:
                allowed = y * rows + iota(logits.shape, 1) <= j * rows + iota(logits.shape, 0)
                logits = jnp.where(allowed, logits, NEG)
            logit_ref[k, j] = logits
            top = functools.reduce(
                jnp.maximum, [logits[:, i : i + WIDE] for i in range(0, rows, WIDE)]
            )
            best_ref[j] = jnp.maximum(best_ref[j], top)

    def gather(*blocks):
        value = [jnp.concatenate([keys_ref[k, rows:], ones], axis=1) for k in blocks]
        for j in range(count):
            best = jnp.concatenate([best_ref[j]] * (rows // WIDE), axis=1)
            new = 0.0
            for k, v in zip(blocks, value):
                new = new + dot(jnp.exp2(logit_ref[k, j] - best).astype(BF16), v)
            sum_ref[j] = sum_ref[j] + new

    def score_many(i, carry):
        for k in range(5):
            score(5 * i + k, False)
        return carry

    def score_one(k, carry):
        score(k, False)
        return carry

    def gather_many(i, carry):
        gather(*(8 * i + k for k in range(8)))
        return carry

    def gather_one(k, carry):
        gather(k)
        return carry

    many = z // 5
    lax.fori_loop(0, many, score_many, 0)
    lax.fori_loop(5 * many, z, score_one, 0)
    score(z, True)
    for j in range(count):
        best = jnp.max(best_ref[j], axis=1, keepdims=True)
        best = jnp.where(best > 0.5 * NEG, best, 0.0)
        best_ref[j] = jnp.broadcast_to(best, best_ref.shape[1:])
    many = (z + 1) // 8
    lax.fori_loop(0, many, gather_many, 0)
    lax.fori_loop(8 * many, z + 1, gather_one, 0)
    eye = iota((WIDE, WIDE), 0) == iota((WIDE, WIDE), 1)
    for j in range(count):
        total = sum_ref[j, :, HEAD_ATT:]
        some = total > 0.0
        safe = jnp.where(some, total, 1.0)
        out_ref[j, 0:rows] = (sum_ref[j, :, 0:HEAD_ATT] / safe).astype(BF16)
        level = jnp.where(some, best_ref[j] + jnp.log(safe) * LOG2E, NEG)
        level = [
            jnp.sum(jnp.where(eye, level[i : i + WIDE], 0.0), axis=0, keepdims=True)
            for i in range(0, rows, WIDE)
        ]
        out_ref[j, rows:] = in_thirds(jnp.concatenate(level, axis=0))


def to_output(lin, att, wl_ref, wa_ref, core, out_ref):
    width = out_ref.shape[2]
    for j in range(out_ref.shape[0]):
        start = pl.multiple_of((2 * j + core) * width, width)
        mine = pl.ds(start, width)
        out_ref[j] = (dot(lin, wl_ref[:, mine]) + dot(att, wa_ref[:, mine])).astype(BF16)


def own_kernel(place_ref, att_ref, lin_ref, wl_ref, wa_ref, own_ref):
    to_output(lin_ref[...], att_ref[...], wl_ref, wa_ref, place_ref[3], own_ref)


def out_kernel(place_ref, parts_ref, lin_ref, gain_ref, wl_ref, wa_ref, other_ref, att_ref):
    count, rows = parts_ref.shape[0], lin_ref.shape[0]
    levels = [joined(parts_ref[j, rows:]) for j in range(count)]
    top = functools.reduce(jnp.maximum, levels)
    shares = [jnp.exp2(level - top) for level in levels]
    total = functools.reduce(jnp.add, shares)
    shares = jnp.concatenate([share / total for share in shares], axis=0).T
    raw = []
    for i in range(rows // WIDE):
        mine = slice(i * WIDE, (i + 1) * WIDE)
        raw.append(
            functools.reduce(
                jnp.add,
                [
                    shares[:, 2 * j + i : 2 * j + i + 1] * parts_ref[j, mine].astype(F32)
                    for j in range(count)
                ],
            )
        )
    raw = jnp.concatenate(raw, axis=0)
    size = jnp.mean(raw * raw, axis=1, keepdims=True)
    att = (raw * lax.rsqrt(size + 1e-6) * gain_ref[...]).astype(BF16)
    att_ref[...] = att
    to_output(lin_ref[...], att, wl_ref, wa_ref, 1 - place_ref[3], other_ref)


def to_partner(a, axis):
    return lax.ppermute(a, axis, [(0, 1), (1, 0)])


def smem():
    return pl.BlockSpec(memory_space=pltpu.SMEM)


def vmem():
    return pl.BlockSpec(memory_space=pltpu.VMEM)


def call(kernel, name, shapes, flops, size, mib, scratch=()):
    def run(*operands):
        many = isinstance(shapes, (list, tuple))
        return pl.pallas_call(
            kernel,
            name=name,
            out_shape=shapes,
            in_specs=[smem()] + [vmem()] * (len(operands) - 1),
            out_specs=[vmem()] * len(shapes) if many else vmem(),
            scratch_shapes=list(scratch),
            compiler_params=params(mib),
            cost_estimate=cost(flops, size),
        )(*operands)

    return run


def body(
    tokens,
    norm_gain,
    recv_weight,
    lin_key_weight,
    lin_value_weight,
    decay_down,
    decay_up,
    decay_log_bias,
    decay_shift,
    learn_rate,
    group_gain,
    initial_state,
    query_weight,
    att_key_weight,
    att_value_weight,
    gate_cache,
    att_gain,
    out_lin_weight,
    out_att_weight,
):
    rows = tokens.shape[0]
    nz, ny, nx = (lax.axis_size(axis) for axis in (KEYS, "near", "x"))
    model_width = norm_gain.shape[0]
    shape = jax.ShapeDtypeStruct
    place = jnp.stack([lax.axis_index(axis) for axis in SP + ("c",)]).astype(jnp.int32)
    gain = norm_gain.reshape(1, -1)

    copies = call(spread_kernel, "spread", shape((nx, *tokens.shape), BF16), 10**10, 1 << 24, 4)(
        place, tokens
    )
    own = lax.all_to_all(copies, "x", 0, 0, tiled=True)
    other = to_partner(own, "c")
    half = rows * model_width * 256
    part, squares = call(
        kv_part_kernel,
        "part",
        (shape((rows, 256), F32), shape((rows, WIDE), F32)),
        half,
        1 << 21,
        12,
    )(place, own, gain, att_key_weight, att_value_weight)
    kv = call(kv_kernel, "kv", shape((2 * rows, WIDE), BF16), half, 1 << 21, 12)(
        place, other, gain, att_key_weight, att_value_weight, part, squares
    )
    keys = lax.all_gather(kv, KEYS)

    extra = 16
    send, gates, reach, local = call(
        lin_kernel,
        "lin",
        (
            shape((ny, rows + WIDE + extra, WIDE), BF16),
            shape((extra, WIDE), BF16),
            shape((rows, WIDE), F32),
            shape((rows, WIDE), F32),
        ),
        4 * 10**9,
        1 << 22,
        24,
        scratch=[pltpu.VMEM((2, 2, rows, 2 * rows), F32)],
    )(
        place,
        own,
        other,
        gain,
        recv_weight,
        lin_key_weight,
        lin_value_weight,
        query_weight,
        decay_down.T,
        decay_up,
        decay_log_bias.reshape(1, -1),
        decay_shift,
        learn_rate.reshape(1, -1),
        gate_cache.reshape(rows // WIDE, WIDE),
    )
    asked = lax.all_to_all(send, "near", 0, 0, tiled=True)
    row_send, before = call(
        functools.partial(row_kernel, rows=rows),
        "row",
        (shape((WIDE + extra, WIDE), BF16), shape((2, WIDE, WIDE), F32)),
        10**8,
        1 << 20,
        12,
    )(place, asked, gates)
    held = lax.all_gather(row_send, KEYS)
    lin_mixed = call(mix_kernel, "mix", shape((rows, WIDE), BF16), 10**9, 1 << 20, 12)(
        place, initial_state, held, before, reach, local, group_gain.reshape(1, -1)
    )
    asked, lin_mixed = lax.optimization_barrier((asked, lin_mixed))
    found = call(
        functools.partial(att_kernel, rows=rows),
        "att",
        shape((ny, rows + extra, HEAD_ATT), BF16),
        ny * rows * nz * rows * 512,
        1 << 22,
        36,
        scratch=[
            pltpu.VMEM((nz, ny, rows, rows), F32),
            pltpu.VMEM((ny, rows, WIDE), F32),
            pltpu.VMEM((ny, rows, HEAD_ATT + WIDE), F32),
        ],
    )(place, asked, held, keys)
    parts = lax.all_to_all(found, "near", 0, 0, tiled=True)
    width = model_width // (2 * nx)
    tile = shape((nx, rows, width), BF16)
    theirs, att = call(
        out_kernel,
        "out",
        (tile, shape((rows, WIDE), BF16)),
        rows * 256 * model_width,
        1 << 21,
        12,
    )(place, parts, lin_mixed, att_gain.reshape(1, -1), out_lin_weight, out_att_weight)
    theirs = to_partner(theirs, "c")
    mine = call(own_kernel, "own", tile, rows * 256 * model_width, 1 << 21, 12)(
        place, att, lin_mixed, out_lin_weight, out_att_weight
    )
    pair = (mine.astype(F32) + theirs.astype(F32)).astype(BF16)
    tiles = lax.all_to_all(pair, "x", 0, 0, tiled=True)
    return jnp.sum(tiles.astype(F32), axis=0).astype(BF16)


def solution(mesh):
    sp, tp = mesh.shape["sp"], mesh.shape["tp"]
    cores = 2
    near = math.isqrt(sp) // 2 if sp > 16 else 2
    torus = Mesh(mesh.devices.reshape(sp // (2 * near), 2, near, tp // cores, cores), SP + TP)
    return jax.shard_map(
        body,
        mesh=torus,
        in_specs=(
            P(SP, TP),
            P(),
            P(None, TP),
            P(None, TP),
            P(None, TP),
            P(),
            P(None, TP),
            P(TP),
            P(SP, TP),
            P(TP),
            P(TP),
            P(TP, None, None),
            P(None, TP),
            P(None, TP),
            P(None, TP),
            P(SP, TP),
            P(TP),
            P(TP, None),
            P(TP, None),
        ),
        out_specs=P(SP, TP),
        check_vma=False,
    )
```
